512 devices in a mesh: sp: 64 (over z, y), fs: 4 (over x), tp: 2 (over core).
Axes of the slice: x: 4, y: 8, z: 8, core: 2. Of those that a mesh axis runs over, the one named last changes fastest.
Arguments:
- tokens: bfloat16 [16384, 2048], P('sp'), may hold values from -6 to 6
- norm_gain: float32 [2048], replicated, may hold values from 0.1 to 1.9
- conv_value: bfloat16 [2048, 1024], P('sp', ('fs', 'tp')), may hold values from -0.125 to 0.125
- conv_gate: bfloat16 [2048, 1024], P('sp', ('fs', 'tp')), may hold values from -0.125 to 0.125
- mixer_gate: bfloat16 [2048, 1024], P('sp', ('fs', 'tp')), may hold values from -0.125 to 0.125
- state_input: bfloat16 [2048, 1024], P('sp', ('fs', 'tp')), may hold values from -0.125 to 0.125
- write_projection: bfloat16 [2048, 1024], P('sp', ('fs', 'tp')), may hold values from -0.125 to 0.125
- state_read: bfloat16 [2048, 1024], P('sp', ('fs', 'tp')), may hold values from -0.125 to 0.125
- step_proj: bfloat16 [2048, 16], replicated, may hold values from -0.125 to 0.125
- step_bias: float32 [16], P(('fs', 'tp')), may hold values from -6 to -0.5
- decay_log: float32 [16], P(('fs', 'tp')), may hold values from -9 to -1.5
- decay_extra: float32 [16, 16384], P(('fs', 'tp'), 'sp'), may hold values from -0.8 to 0
- input_taps: float32 [4, 1024], P(None, ('fs', 'tp')), may hold values from -3 to 3
- write_taps: float32 [4, 1024], P(None, ('fs', 'tp')), may hold values from -3 to 3
- fetch_kernel_coefficients: float32 [4, 1024], P(None, ('fs', 'tp')), may hold values from -3 to 3
- long_taps: float32 [31, 1024], P(None, ('fs', 'tp')), may hold values from -5 to 5
- conv_gain: float32 [1024], P(('fs', 'tp')), may hold values from 0.1 to 1.9
- state_gain: float32 [1024], P(('fs', 'tp')), may hold values from 0.1 to 1.9
- conv_output: bfloat16 [2048, 1024], P('sp', ('fs', 'tp')), may hold values from -0.125 to 0.125
- state_output: bfloat16 [2048, 1024], P('sp', ('fs', 'tp')), may hold values from -0.125 to 0.125
- initial_state: float32 [16, 64, 128], P(('fs', 'tp')), may hold values from -12 to 12
Outputs:
- mixed: bfloat16 [16384, 2048], P(('sp', 'fs', 'tp'))
The draws below stay inside these ranges and needn't reach their ends.
All inputs are finite; a program needn't handle non-finite values.
Results may differ from the reference program's by a relative error of at most 0.017.
Values may be sent and summed in bfloat16 or wider, within the bound.
No kernel may reach another device: no remote copies, remote signals or barrier semaphores. Data moves between devices by JAX's collectives and lax.ppermute only.
A program may use at most 64 MiB of HBM per device.

```python
import math
import jax
import jax.numpy as jnp
from jax import lax

D = 2048
C_CH = 1024
HEADS = 16
HEAD_P = 64
GROUPS = 8
STATE = 128
WIDE_TAPS = 31
SHORT_TAPS = 4
SPAN = 64
TOK_DEV = 256
D_INNER = 1024
SEQ = 16384
N_FS = 4
N_TP = 2


def head_kinds(key):
    draw = jax.random.uniform(jax.random.fold_in(key, 101), (HEADS,))
    return draw < 0.5


def draw_step_bias(key, part):
    fast = head_kinds(key)
    jitter = jax.random.uniform(jax.random.fold_in(key, 102), (HEADS,), minval=-0.5, maxval=0.5)
    slow_level = math.log(1.75) - 0.5 * math.log(SEQ)
    return (jnp.where(fast, -1.0, slow_level) + jitter).astype(jnp.float32)


def draw_decay_log(key, part):
    fast = head_kinds(key)
    jitter = jax.random.uniform(jax.random.fold_in(key, 103), (HEADS,), minval=-0.5, maxval=0.5)
    slow_level = math.log(0.114) - 0.5 * math.log(SEQ)
    return (jnp.where(fast, -2.2, slow_level) + jitter).astype(jnp.float32)


def draw_decay_extra(key, part):
    blocks = SEQ // TOK_DEV
    low, high = (math.log(0.5), math.log(2.0))
    level = jnp.exp(jax.random.uniform(jax.random.fold_in(key, 104), (HEADS, blocks), minval=low, maxval=high))
    gradual_fraction = -0.5 / SEQ * jnp.repeat(level, TOK_DEV, axis=1)
    point_locations = jax.random.randint(jax.random.fold_in(key, 105), (HEADS, 3), 0, SEQ)
    discarded_entries = jnp.log(jax.random.uniform(jax.random.fold_in(key, 106), (HEADS, 3), minval=0.5, maxval=0.8))
    location_numbers = jnp.arange(SEQ, dtype=jnp.int32)
    cluster_sets = jnp.sum(jnp.where(location_numbers[None, None, :] == point_locations[:, :, None], discarded_entries[:, :, None], 0.0), axis=1)
    return (gradual_fraction + cluster_sets).astype(jnp.float32)


def draw_long_taps(key, part):
    base = jax.random.truncated_normal(jax.random.fold_in(key, 107), -3.0, 3.0, (WIDE_TAPS, C_CH))
    ramp = math.log(3.0) * jnp.arange(C_CH, dtype=jnp.float32) / C_CH
    ramp = ramp + jax.random.uniform(jax.random.fold_in(key, 108), (C_CH,), minval=-0.35, maxval=0.35)
    return (base * jnp.exp(ramp)[None, :] / math.sqrt(WIDE_TAPS)).astype(jnp.float32)


def levels(stream_key, shape, cuts, least, top_value):
    loudness = 1.0
    for axis_at, blocks in cuts:
        heights = jax.random.uniform(jax.random.fold_in(jax.random.fold_in(stream_key, 6), axis_at), (blocks,), jnp.float32, least / len(cuts), top_value / len(cuts))
        loudness = loudness * jnp.repeat(jnp.exp(heights), shape[axis_at] // blocks).reshape((-1,) + (1,) * (len(shape) - 1 - axis_at))
    return loudness


def noise(own_key, shape, scale, most, shards=(), held_as=jnp.bfloat16):
    drawn = scale * jax.random.normal(own_key, shape, jnp.float32)
    if shards:
        drawn = drawn * levels(own_key, shape, shards, -0.22, 0.18)
    return jnp.clip(drawn, -most, most).astype(held_as)


def setup_inputs(seed: int = 0) -> dict:
    keys = jax.random.split(jax.random.key(seed), 22)
    return {
        "tokens": noise(keys[0], (SEQ, D), 1.0, 6.0, ((0, 64),)),
        "norm_gain": jnp.clip(1.0 + 0.18 * jax.random.normal(keys[1], (D,), jnp.float32), 0.1, 1.9),
        "conv_value": noise(keys[2], (D, C_CH), D ** -0.5, 0.125, ((0, 64), (1, 8))),
        "conv_gate": noise(keys[3], (D, C_CH), D ** -0.5, 0.125, ((0, 64), (1, 8))),
        "mixer_gate": noise(keys[4], (D, D_INNER), D ** -0.5, 0.125, ((0, 64), (1, 8))),
        "state_input": noise(keys[5], (D, D_INNER), D ** -0.5, 0.125, ((0, 64), (1, 8))),
        "write_projection": noise(keys[6], (D, GROUPS * STATE), D ** -0.5, 0.125, ((0, 64), (1, 8))),
        "state_read": noise(keys[7], (D, GROUPS * STATE), D ** -0.5, 0.125, ((0, 64), (1, 8))),
        "step_proj": noise(keys[8], (D, HEADS), D ** -0.5, 0.125),
        "step_bias": draw_step_bias(jax.random.fold_in(keys[21], 71), 0),
        "decay_log": draw_decay_log(jax.random.fold_in(keys[21], 71), 0),
        "decay_extra": draw_decay_extra(jax.random.fold_in(keys[21], 71), 0),
        "input_taps": noise(keys[12], (SHORT_TAPS, D_INNER), SHORT_TAPS ** -0.5, 3.0, ((1, 8),), jnp.float32),
        "write_taps": noise(keys[13], (SHORT_TAPS, GROUPS * STATE), SHORT_TAPS ** -0.5, 3.0, ((1, 8),), jnp.float32),
        "fetch_kernel_coefficients": noise(keys[14], (SHORT_TAPS, GROUPS * STATE), SHORT_TAPS ** -0.5, 3.0, ((1, 8),), jnp.float32),
        "long_taps": draw_long_taps(jax.random.fold_in(keys[21], 71), 0),
        "conv_gain": jnp.clip(1.0 + 0.18 * jax.random.normal(keys[16], (C_CH,), jnp.float32), 0.1, 1.9),
        "state_gain": jnp.clip(1.0 + 0.18 * jax.random.normal(keys[17], (D_INNER,), jnp.float32), 0.1, 1.9),
        "conv_output": noise(keys[18], (D, C_CH), (C_CH + D_INNER) ** -0.5, 0.125, ((0, 64), (1, 8))),
        "state_output": noise(keys[19], (D, D_INNER), (C_CH + D_INNER) ** -0.5, 0.125, ((0, 64), (1, 8))),
        "initial_state": noise(keys[20], (HEADS, HEAD_P, STATE), 2.0, 12.0, ((0, 8),), jnp.float32),
    }


eps_norm = 1e-06

def causal_valid(padded, taps):
    result = lax.conv_general_dilated(padded[None], taps[:, None, :], window_strides=(1,), padding='VALID', dimension_numbers=('NWC', 'WIO', 'NWC'), feature_group_count=taps.shape[1], precision=lax.Precision.HIGHEST)
    return result[0]

def causal_conv(signal, taps):
    padded = jnp.pad(signal, ((taps.shape[0] - 1, 0), (0, 0)))
    return causal_valid(padded, taps)

def project(normed, weight):
    return jnp.dot(normed, weight, preferred_element_type=jnp.float32).astype(jnp.bfloat16)

def span_step(state, inputs):
    x_span, write_span, read_span, log_span = inputs
    cumul = jnp.cumsum(log_span, axis=0)
    length = cumul.shape[0]
    lower = jnp.tril(jnp.ones((length, length), dtype=bool))
    gaps = cumul.T[:, :, None] - cumul.T[:, None, :]
    weights = jnp.where(lower, jnp.exp(jnp.where(lower, gaps, 0.0)), 0.0)
    scores = jnp.einsum('thn,shn->hts', read_span, write_span, precision=lax.Precision.HIGHEST)
    inner = jnp.einsum('hts,shp->thp', scores * weights, x_span, precision=lax.Precision.HIGHEST)
    carried = jnp.einsum('thn,hpn->thp', read_span, state, precision=lax.Precision.HIGHEST) * jnp.exp(cumul)[:, :, None]
    last = cumul[-1]
    fresh = jnp.einsum('shn,shp->hpn', write_span * jnp.exp(last[None, :] - cumul)[:, :, None], x_span, precision=lax.Precision.HIGHEST)
    return (state * jnp.exp(last)[:, None, None] + fresh, inner + carried)

def reference(tokens, norm_gain, conv_value, conv_gate, mixer_gate, state_input, write_projection, state_read, step_proj, step_bias, decay_log, decay_extra, input_taps, write_taps, fetch_kernel_coefficients, long_taps, conv_gain, state_gain, conv_output, state_output, initial_state):
    length = tokens.shape[0]
    values = tokens.astype(jnp.float32)
    normed = (values * lax.rsqrt(lax.optimization_barrier(jnp.mean(values * values, axis=1, keepdims=True)) + eps_norm) * norm_gain).astype(jnp.bfloat16)
    value_rows = project(normed, conv_value)
    gate_rows = project(normed, conv_gate)
    gate_z = project(normed, mixer_gate)
    input_rows = project(normed, state_input)
    write_rows = project(normed, write_projection)
    read_rows = project(normed, state_read)
    step_size = jax.nn.softplus(jnp.dot(normed, step_proj, preferred_element_type=jnp.float32) + step_bias)
    log_step = -jnp.exp(decay_log) * step_size + decay_extra.T
    glu = value_rows.astype(jnp.float32) * jax.nn.sigmoid(gate_rows.astype(jnp.float32))
    long_mix = causal_conv(glu, long_taps)
    mean = lax.optimization_barrier(jnp.mean(long_mix, axis=1, keepdims=True))
    spread = lax.optimization_barrier(jnp.mean(long_mix * long_mix, axis=1, keepdims=True)) - mean * mean
    conv_out = jax.nn.silu((long_mix - mean) * lax.rsqrt(spread + eps_norm) * conv_gain).astype(jnp.bfloat16)
    input_act = jax.nn.silu(causal_conv(input_rows.astype(jnp.float32), input_taps))
    write_activation = jax.nn.silu(causal_conv(write_rows.astype(jnp.float32), write_taps))
    read_act = jax.nn.silu(causal_conv(read_rows.astype(jnp.float32), fetch_kernel_coefficients))
    per_group = HEADS // GROUPS
    blocks = length // SPAN
    x_heads = (input_act.reshape(length, HEADS, HEAD_P) * step_size[:, :, None]).reshape(blocks, SPAN, HEADS, HEAD_P)
    write_heads = jnp.repeat(write_activation.reshape(length, GROUPS, STATE), per_group, axis=1).reshape(blocks, SPAN, HEADS, STATE)
    read_heads = jnp.repeat(read_act.reshape(length, GROUPS, STATE), per_group, axis=1).reshape(blocks, SPAN, HEADS, STATE)
    log_blocks = log_step.reshape(blocks, SPAN, HEADS)
    ending, outputs = lax.scan(span_step, initial_state, (x_heads, write_heads, read_heads, log_blocks))
    gated = outputs.reshape(length, D_INNER) * jax.nn.silu(gate_z.astype(jnp.float32))
    state_out = (gated * lax.rsqrt(lax.optimization_barrier(jnp.mean(gated * gated, axis=1, keepdims=True)) + eps_norm) * state_gain).astype(jnp.bfloat16)
    pieces = N_FS * N_TP
    conv_width = C_CH // pieces
    state_width = D_INNER // pieces
    contract = (((1,), (1,)), ((), ()))

    def summand_term(total, index):
        conv_part = lax.dynamic_slice_in_dim(conv_out, (index * conv_width).astype(jnp.int32), conv_width, 1)
        conv_back = lax.dynamic_slice_in_dim(conv_output, (index * conv_width).astype(jnp.int32), conv_width, 1)
        state_part = lax.dynamic_slice_in_dim(state_out, (index * state_width).astype(jnp.int32), state_width, 1)
        state_back = lax.dynamic_slice_in_dim(state_output, (index * state_width).astype(jnp.int32), state_width, 1)
        term = lax.dot_general(conv_part, conv_back, contract, preferred_element_type=jnp.float32)
        term = term + lax.dot_general(state_part, state_back, contract, preferred_element_type=jnp.float32)
        rounded = lax.optimization_barrier(term.astype(jnp.bfloat16))
        return (total + rounded.astype(jnp.float32), None)
    total, ignored = lax.scan(summand_term, jnp.zeros((length, D), jnp.float32), jnp.arange(pieces, dtype=jnp.int32))
    return total.astype(jnp.bfloat16)
```

```python
import jax
import jax.numpy as jnp
from jax import lax
from jax.sharding import Mesh
from jax.sharding import PartitionSpec as P

C_CH = 1024
STATE = 128
D_INNER = 1024
WIDE = 31
SHORT = 4
HALO = 32
EPS = 1e-06
SP = ("sp_0", "sp_1")
FT = ("fs", "tp")
f32 = jnp.float32
bf16 = jnp.bfloat16


def spread(shard, axis):
    n = lax.axis_size(axis)
    return lax.all_to_all(jnp.broadcast_to(shard[None], (n, *shard.shape)), axis, 0, 0, tiled=True)


def previous(block):
    n = lax.axis_size(SP)
    return lax.ppermute(block, SP, [(i, i + 1) for i in range(n - 1)])


def dot(a, b, ca, cb):
    return lax.dot_general(a, b, (((ca,), (cb,)), ((), ())), preferred_element_type=f32)


def unit_rows(tokens, gain):
    v = tokens.astype(f32)
    return (v * lax.rsqrt(jnp.mean(v * v, axis=1, keepdims=True) + EPS) * gain).astype(bf16)


def causal(rows, taps, at, n):
    k = taps.shape[0]
    return sum(rows[at + i : at + i + n] * taps[i] for i in range(k))


def split3(x):
    hi = x.astype(bf16)
    rest = x - hi.astype(f32)
    mid = rest.astype(bf16)
    return hi, mid, (rest - mid.astype(f32)).astype(bf16)


def per_device(
    tokens, norm_gain, conv_value, conv_gate, mixer_gate, state_input, write_projection, state_read,
    step_proj, step_bias, decay_log, decay_extra, input_taps, write_taps, fetch_taps, long_taps,
    conv_gain, state_gain, conv_output, state_output, initial_state,
):
    rows = tokens.shape[0]
    ch = conv_value.shape[1]
    heads = step_bias.shape[0]
    p = ch // heads
    nf, nt = lax.axis_size("fs"), lax.axis_size("tp")
    shard = jnp.concatenate(
        [state_input, write_projection, state_read, mixer_gate, conv_value, conv_gate, conv_output, state_output], 1
    )
    near = spread(shard, "sp_1").reshape(-1, 8 * ch)
    rest = lax.all_gather(near[:, 2 * ch :], "sp_0", axis=0, tiled=True)
    first = spread(near[:, : 2 * ch], "sp_0").reshape(-1, 2 * ch)
    halo = previous(tokens[rows - HALO :])
    normed = unit_rows(jnp.concatenate([halo, tokens], 0), norm_gain)
    own = normed[HALO:]
    step_all = jnp.dot(own, step_proj, preferred_element_type=f32)
    me = lax.axis_index("fs") * nt + lax.axis_index("tp")
    step = jax.nn.softplus(lax.dynamic_slice_in_dim(step_all, me * heads, heads, 1) + step_bias)
    log_step = (-jnp.exp(decay_log) * step + decay_extra.T).T
    cumul = jnp.cumsum(log_step, axis=1)
    total = cumul[:, -1]
    xw = dot(normed, first, 1, 0).astype(bf16).astype(f32)
    x_act = jax.nn.silu(causal(xw[:, :ch], input_taps, HALO - SHORT + 1, rows))
    w_act = jax.nn.silu(causal(xw[:, ch:], write_taps, HALO - SHORT + 1, rows))
    xs = [(x_act[:, h * p : (h + 1) * p] * step[:, h : h + 1]).astype(bf16) for h in range(heads)]
    w16 = w_act.astype(bf16)
    left = jnp.exp(total[:, None] - cumul).T
    ends = jnp.concatenate(
        [dot(xs[h], (w_act * left[:, h : h + 1]).astype(bf16), 0, 0) for h in range(heads)], 0
    ).astype(bf16)
    hi, mid, lo = split3(total)
    logs = jnp.zeros((16, STATE), bf16)
    logs = logs.at[0, :heads].set(hi).at[1, :heads].set(mid).at[2, :heads].set(lo)
    got = spread(jnp.concatenate([ends, logs], 0), "sp_1")
    logs_y = jnp.sum(got[:, heads * p : heads * p + 3, :heads].astype(f32), 1)
    iy, ny = lax.axis_index("sp_1"), lax.axis_size("sp_1")
    k = jnp.arange(ny)
    after = lambda last: jnp.sum(
        jnp.where((k[None, :, None] > k[:, None, None]) & (k[None, :, None] < last), logs_y[None], 0.0), 1
    )
    c_in = jnp.where(k[:, None] < iy, jnp.exp(after(iy)), 0.0)
    c_all = jnp.exp(after(ny))
    pieces = got[:, : heads * p].astype(f32).reshape(ny, heads, p, STATE)
    enter_y = jnp.sum(pieces * c_in[:, :, None, None], 0)
    line = jnp.sum(pieces * c_all[:, :, None, None], 0).reshape(heads * p, STATE).astype(bf16)
    line_log = jnp.sum(logs_y, 0)
    before_log = jnp.sum(jnp.where(k[:, None] < iy, logs_y, 0.0), 0)
    hi, mid, lo = split3(line_log)
    logs = jnp.zeros((16, STATE), bf16)
    logs = logs.at[0, :heads].set(hi).at[1, :heads].set(mid).at[2, :heads].set(lo)
    got = spread(jnp.concatenate([line, logs], 0), "sp_0")
    logs_z = jnp.sum(got[:, heads * p : heads * p + 3, :heads].astype(f32), 1)
    iz, nz = lax.axis_index("sp_0"), lax.axis_size("sp_0")
    k = jnp.arange(nz)
    between = jnp.sum(
        jnp.where((k[None, :, None] > k[:, None, None]) & (k[None, :, None] < iz), logs_z[None], 0.0), 1
    )
    c_in = jnp.where(k[:, None] < iz, jnp.exp(between + before_log), 0.0)
    c_init = jnp.exp(jnp.sum(jnp.where(k[:, None] < iz, logs_z, 0.0), 0) + before_log)
    pieces = got[:, : heads * p].astype(f32).reshape(nz, heads, p, STATE)
    start = enter_y + jnp.sum(pieces * c_in[:, :, None, None], 0) + c_init[:, None, None] * initial_state
    start = start.astype(bf16)
    proj = dot(normed, rest[:, : 4 * ch], 1, 0).astype(bf16).astype(f32)
    r_act = jax.nn.silu(causal(proj[:, :ch], fetch_taps, HALO - SHORT + 1, rows)).astype(bf16)
    z_gate = jax.nn.silu(proj[HALO:, ch : 2 * ch])
    glu = proj[:, 2 * ch : 3 * ch] * jax.nn.sigmoid(proj[:, 3 * ch :])
    mix = causal(glu, long_taps, HALO - WIDE + 1, rows)
    sums = jnp.stack([jnp.sum(mix, 1), jnp.sum(mix * mix, 1)])
    sums = jnp.sum(spread(sums, FT), 0)
    mean = sums[0] / C_CH
    var = sums[1] / C_CH - mean * mean
    conv_out = jax.nn.silu((mix - mean[:, None]) * lax.rsqrt(var + EPS)[:, None] * conv_gain).astype(bf16)
    scores = dot(r_act, w16, 1, 1)
    lower = jnp.tril(jnp.ones((rows, rows), bool))
    ys = []
    for h in range(heads):
        gap = jnp.where(lower, cumul[h][:, None] - cumul[h][None, :], 0.0)
        m = jnp.where(lower, jnp.exp(gap) * scores, 0.0).astype(bf16)
        ys.append(dot(m, xs[h], 1, 0) + dot(r_act, start[h], 1, 1) * jnp.exp(cumul[h])[:, None])
    gated = jnp.concatenate(ys, 1) * z_gate
    square = jnp.sum(spread(jnp.sum(gated * gated, 1)[None], FT), (0, 1))
    state_pre = (gated * state_gain).astype(bf16)
    tp = lax.axis_index("tp")

    def half(a):
        a = a.reshape(nf, nt, rows // (nf * nt), *a.shape[1:])
        return lax.dynamic_index_in_dim(a, tp, 1, keepdims=False).reshape(rows // nt, *a.shape[3:])

    def pair(a):
        both = lax.all_gather(a, "tp", axis=0)
        return jnp.concatenate([both[i] for i in range(nt)], 1)

    conv_in = half(pair(conv_out))
    state_in = half(pair(state_pre))
    back_c = pair(rest[:, 4 * ch : 5 * ch])
    back_s = pair(rest[:, 5 * ch :])
    scale = lax.rsqrt(half(square) / D_INNER + EPS)[:, None]
    part = (dot(conv_in, back_c, 1, 1) + scale * dot(state_in, back_s, 1, 1)).astype(bf16)
    pieces = lax.all_to_all(part.reshape(nf, -1, part.shape[1]), "fs", 0, 0, tiled=True)
    return jnp.sum(pieces.astype(f32), 0).astype(bf16)


def solution(mesh):
    torus = Mesh(
        mesh.devices.reshape(8, 8, mesh.shape["fs"], mesh.shape["tp"]), ("sp_0", "sp_1", "fs", "tp")
    )
    w = P(SP, FT)
    in_specs = (
        P(SP, None), P(), w, w, w, w, w, w, P(), P(FT), P(FT), P(FT, SP), P(None, FT), P(None, FT), P(None, FT),
        P(None, FT), P(FT), P(FT), w, w, P(FT, None, None),
    )
    return jax.shard_map(
        per_device, mesh=torus, in_specs=in_specs, out_specs=P((*SP, *FT), None), check_vma=False
    )
```

```python
import jax
import jax.numpy as jnp
from jax import lax
from jax.experimental import pallas as pl
from jax.experimental.pallas import tpu as pltpu
from jax.sharding import Mesh
from jax.sharding import PartitionSpec as P

C_CH = 1024
STATE = 128
D_INNER = 1024
WIDE = 31
SHORT = 4
HALO = 32
EPS = 1e-06
SP = ("sp_0", "sp_1")
FT = ("fs", "tp")
f32 = jnp.float32
bf16 = jnp.bfloat16


def spread(shard, axis):
    n = lax.axis_size(axis)
    return lax.all_to_all(jnp.broadcast_to(shard[None], (n, *shard.shape)), axis, 0, 0, tiled=True)


def previous(block):
    n = lax.axis_size(SP)
    return lax.ppermute(block, SP, [(i, i + 1) for i in range(n - 1)])


def dot(a, b, ca, cb):
    return lax.dot_general(a, b, (((ca,), (cb,)), ((), ())), preferred_element_type=f32)


def unit_rows(tokens, gain):
    v = tokens.astype(f32)
    return (v * lax.rsqrt(jnp.mean(v * v, axis=1, keepdims=True) + EPS) * gain).astype(bf16)


def causal(rows, taps, at, n):
    k = taps.shape[0]
    return sum(rows[at + i : at + i + n] * taps[i] for i in range(k))


def split3(x):
    hi = x.astype(bf16)
    rest = x - hi.astype(f32)
    mid = rest.astype(bf16)
    return hi, mid, (rest - mid.astype(f32)).astype(bf16)


def lay_out(early, late, n_all, n_y):
    rows, ch = early[0].shape
    ne, nl = len(early), len(late)

    def body(*refs):
        ins, (first, rest) = refs[: ne + nl], refs[ne + nl :]
        for i in range(nl):
            w = ins[ne + i][...]
            for k in range(n_y):
                rest[k, :, i * ch : (i + 1) * ch] = w
        for i in range(ne):
            w = ins[i][...]
            for k in range(n_all):
                first[k, :, i * ch : (i + 1) * ch] = w

    return pl.pallas_call(
        body,
        out_shape=(
            jax.ShapeDtypeStruct((n_all, rows, ne * ch), bf16),
            jax.ShapeDtypeStruct((n_y, rows, nl * ch), bf16),
        ),
        in_specs=[pl.BlockSpec(memory_space=pltpu.VMEM)] * (ne + nl),
        out_specs=(pl.BlockSpec(memory_space=pltpu.VMEM),) * 2,
        name="lay_out",
    )(*early, *late)


def log_rows(logs):
    hi, mid, lo = split3(logs)
    rows = jnp.stack([hi, mid, lo])
    return jnp.pad(rows, ((0, 13), (0, STATE - logs.shape[0])))


def per_device(
    tokens, norm_gain, conv_value, conv_gate, mixer_gate, state_input, write_projection, state_read,
    step_proj, step_bias, decay_log, decay_extra, input_taps, write_taps, fetch_taps, long_taps,
    conv_gain, state_gain, conv_output, state_output, initial_state,
):
    rows = tokens.shape[0]
    ch = conv_value.shape[1]
    heads = step_bias.shape[0]
    p = ch // heads
    nf, nt = lax.axis_size("fs"), lax.axis_size("tp")
    first, rest = lay_out(
        (state_input, write_projection),
        (state_read, mixer_gate, conv_value, conv_gate, conv_output, state_output),
        lax.axis_size(SP),
        lax.axis_size("sp_1"),
    )
    rest = lax.all_to_all(rest, "sp_1", 0, 0, tiled=True).reshape(-1, 6 * ch)
    rest = lax.all_gather(rest, "sp_0", axis=0, tiled=True)
    first = lax.all_to_all(first, SP, 0, 0, tiled=True).reshape(-1, 2 * ch)
    halo = previous(tokens[rows - HALO :])
    normed = unit_rows(jnp.concatenate([halo, tokens], 0), norm_gain)
    own = normed[HALO:]
    step_all = jnp.dot(own, step_proj, preferred_element_type=f32)
    tp = lax.axis_index("tp")
    me = lax.axis_index("fs") * nt + tp
    step = jax.nn.softplus(lax.dynamic_slice_in_dim(step_all, me * heads, heads, 1) + step_bias)
    log_step = (-jnp.exp(decay_log) * step + decay_extra.T).T
    cumul = jnp.cumsum(log_step, axis=1)
    total = cumul[:, -1]
    xw = dot(normed, first, 1, 0).astype(bf16).astype(f32)
    x_act = jax.nn.silu(causal(xw[:, :ch], input_taps, HALO - SHORT + 1, rows))
    w_act = jax.nn.silu(causal(xw[:, ch:], write_taps, HALO - SHORT + 1, rows))
    xs = [(x_act[:, h * p : (h + 1) * p] * step[:, h : h + 1]).astype(bf16) for h in range(heads)]
    w16 = w_act.astype(bf16)
    left = jnp.exp(total[:, None] - cumul).T
    ends = jnp.concatenate(
        [dot(xs[h], (w_act * left[:, h : h + 1]).astype(bf16), 0, 0) for h in range(heads)], 0
    ).astype(bf16)
    got = spread(jnp.concatenate([ends, log_rows(total)], 0), "sp_1")
    logs_y = jnp.sum(got[:, heads * p : heads * p + 3, :heads].astype(f32), 1)
    iy, ny = lax.axis_index("sp_1"), lax.axis_size("sp_1")
    k = jnp.arange(ny)
    after = lambda last: jnp.sum(
        jnp.where((k[None, :, None] > k[:, None, None]) & (k[None, :, None] < last), logs_y[None], 0.0), 1
    )
    c_in = jnp.where(k[:, None] < iy, jnp.exp(after(iy)), 0.0)
    c_all = jnp.exp(after(ny))
    pieces = got[:, : heads * p].astype(f32).reshape(ny, heads, p, STATE)
    enter_y = jnp.sum(pieces * c_in[:, :, None, None], 0)
    line = jnp.sum(pieces * c_all[:, :, None, None], 0).reshape(heads * p, STATE).astype(bf16)
    line_log = jnp.sum(logs_y, 0)
    before_log = jnp.sum(jnp.where(k[:, None] < iy, logs_y, 0.0), 0)
    got = spread(jnp.concatenate([line, log_rows(line_log)], 0), "sp_0")
    logs_z = jnp.sum(got[:, heads * p : heads * p + 3, :heads].astype(f32), 1)
    iz, nz = lax.axis_index("sp_0"), lax.axis_size("sp_0")
    k = jnp.arange(nz)
    between = jnp.sum(
        jnp.where((k[None, :, None] > k[:, None, None]) & (k[None, :, None] < iz), logs_z[None], 0.0), 1
    )
    c_in = jnp.where(k[:, None] < iz, jnp.exp(between + before_log), 0.0)
    c_init = jnp.exp(jnp.sum(jnp.where(k[:, None] < iz, logs_z, 0.0), 0) + before_log)
    pieces = got[:, : heads * p].astype(f32).reshape(nz, heads, p, STATE)
    start = enter_y + jnp.sum(pieces * c_in[:, :, None, None], 0) + c_init[:, None, None] * initial_state
    start = start.astype(bf16)
    back = rest[:, 4 * ch :]
    back_other = lax.ppermute(back, "tp", [(i, nt - 1 - i) for i in range(nt)])
    gain_both = lax.all_gather(conv_gain, "tp")
    proj = dot(normed, rest[:, : 4 * ch], 1, 0).astype(bf16).astype(f32)
    r_act = jax.nn.silu(causal(proj[:, :ch], fetch_taps, HALO - SHORT + 1, rows)).astype(bf16)
    z_gate = jax.nn.silu(proj[HALO:, ch : 2 * ch])
    glu = proj[:, 2 * ch : 3 * ch] * jax.nn.sigmoid(proj[:, 3 * ch :])
    mix = causal(glu, long_taps, HALO - WIDE + 1, rows)
    scores = dot(r_act, w16, 1, 1)
    lower = jnp.tril(jnp.ones((rows, rows), bool))
    inner = []
    for h in range(heads):
        gap = jnp.where(lower, cumul[h][:, None] - cumul[h][None, :], 0.0)
        m = jnp.where(lower, jnp.exp(gap) * scores, 0.0).astype(bf16)
        inner.append(dot(m, xs[h], 1, 0))
    ys = [inner[h] + dot(r_act, start[h], 1, 1) * jnp.exp(cumul[h])[:, None] for h in range(heads)]
    gated = jnp.concatenate(ys, 1) * z_gate
    sums = jnp.stack([jnp.sum(mix, 1), jnp.sum(mix * mix, 1), jnp.sum(gated * gated, 1)])
    sums = jnp.sum(spread(sums, FT), 0)

    def half(a):
        a = a.reshape(nf, nt, rows // (nf * nt), *a.shape[1:])
        return lax.dynamic_index_in_dim(a, tp, 1, keepdims=False).reshape(rows // nt, *a.shape[3:])

    pre = jnp.concatenate([mix.astype(bf16), (gated * state_gain).astype(bf16)], 1)
    both = lax.all_gather(pre, "tp", axis=0)
    sums = half(sums.T)
    mean = sums[:, 0:1] / C_CH
    rstd = lax.rsqrt(sums[:, 1:2] / C_CH - mean * mean + EPS)
    scale = lax.rsqrt(sums[:, 2:3] / D_INNER + EPS)
    part = 0.0
    for i, w in ((tp, back), (1 - tp, back_other)):
        a = half(lax.dynamic_index_in_dim(both, i, 0, keepdims=False)).astype(f32)
        g = lax.dynamic_index_in_dim(gain_both, i, 0, keepdims=False)
        conv = jax.nn.silu((a[:, :ch] - mean) * rstd * g)
        part = part + dot(jnp.concatenate([conv, a[:, ch:] * scale], 1).astype(bf16), w, 1, 1)
    pieces = lax.all_to_all(part.astype(bf16).reshape(nf, -1, part.shape[1]), "fs", 0, 0, tiled=True)
    return jnp.sum(pieces.astype(f32), 0).astype(bf16)


def solution(mesh):
    torus = Mesh(
        mesh.devices.reshape(8, 8, mesh.shape["fs"], mesh.shape["tp"]), ("sp_0", "sp_1", "fs", "tp")
    )
    w = P(SP, FT)
    in_specs = (
        P(SP, None), P(), w, w, w, w, w, w, P(), P(FT), P(FT), P(FT, SP), P(None, FT), P(None, FT), P(None, FT),
        P(None, FT), P(FT), P(FT), w, w, P(FT, None, None),
    )
    return jax.shard_map(
        per_device, mesh=torus, in_specs=in_specs, out_specs=P((*SP, *FT), None), check_vma=False
    )
```

```python
import jax
import jax.numpy as jnp
from jax import lax
from jax.experimental import pallas as pl
from jax.experimental.pallas import tpu as pltpu
from jax.sharding import Mesh
from jax.sharding import PartitionSpec as P

C_CH = 1024
STATE = 128
D_INNER = 1024
WIDE = 31
SHORT = 4
HALO = 32
EPS = 1e-06
SP = ("sp_0", "sp_1")
FT = ("fs", "tp")
f32 = jnp.float32
bf16 = jnp.bfloat16


def spread(shard, axis):
    n = lax.axis_size(axis)
    return lax.all_to_all(jnp.broadcast_to(shard[None], (n, *shard.shape)), axis, 0, 0, tiled=True)


def previous(block):
    n = lax.axis_size(SP)
    return lax.ppermute(block, SP, [(i, i + 1) for i in range(n - 1)])


def dot(a, b, ca, cb):
    return lax.dot_general(a, b, (((ca,), (cb,)), ((), ())), preferred_element_type=f32)


def unit_rows(tokens, gain):
    v = tokens.astype(f32)
    return (v * lax.rsqrt(jnp.mean(v * v, axis=1, keepdims=True) + EPS) * gain).astype(bf16)


def causal(rows, taps, at, n):
    k = taps.shape[0]
    return sum(rows[at + i : at + i + n] * taps[i] for i in range(k))


def split3(x):
    hi = x.astype(bf16)
    rest = x - hi.astype(f32)
    mid = rest.astype(bf16)
    return hi, mid, (rest - mid.astype(f32)).astype(bf16)


VMEM = pl.BlockSpec(memory_space=pltpu.VMEM)


def lay_out(shards, copies):
    rows, ch = shards[0].shape
    n = len(shards)

    def body(*refs):
        for i in range(n):
            w = refs[i][...]
            for k in range(copies):
                refs[n][k, :, i * ch : (i + 1) * ch] = w

    return pl.pallas_call(
        body, out_shape=jax.ShapeDtypeStruct((copies, rows, n * ch), bf16), in_specs=[VMEM] * n, out_specs=VMEM
    )(*shards)


def log_rows(logs):
    hi, mid, lo = split3(logs)
    rows = jnp.stack([hi, mid, lo])
    return jnp.pad(rows, ((0, 13), (0, STATE - logs.shape[0])))


def per_device(
    tokens, norm_gain, conv_value, conv_gate, mixer_gate, state_input, write_projection, state_read,
    step_proj, step_bias, decay_log, decay_extra, input_taps, write_taps, fetch_taps, long_taps,
    conv_gain, state_gain, conv_output, state_output, initial_state,
):
    rows = tokens.shape[0]
    ch = conv_value.shape[1]
    heads = step_bias.shape[0]
    p = ch // heads
    nf, nt = lax.axis_size("fs"), lax.axis_size("tp")
    rest = lay_out((state_read, mixer_gate, conv_value, conv_gate, conv_output, state_output), 1)
    rest = lax.all_gather(rest[0], SP, axis=0, tiled=True)
    first = lay_out((state_input, write_projection), lax.axis_size(SP))
    first = lax.all_to_all(first, SP, 0, 0, tiled=True).reshape(-1, 2 * ch)
    halo = previous(tokens[rows - HALO :])
    normed = unit_rows(jnp.concatenate([halo, tokens], 0), norm_gain)
    own = normed[HALO:]
    step_all = jnp.dot(own, step_proj, preferred_element_type=f32)
    tp = lax.axis_index("tp")
    me = lax.axis_index("fs") * nt + tp
    step = jax.nn.softplus(lax.dynamic_slice_in_dim(step_all, me * heads, heads, 1) + step_bias)
    log_step = (-jnp.exp(decay_log) * step + decay_extra.T).T
    cumul = jnp.cumsum(log_step, axis=1)
    total = cumul[:, -1]
    xw = dot(normed, first, 1, 0).astype(bf16).astype(f32)
    x_act = jax.nn.silu(causal(xw[:, :ch], input_taps, HALO - SHORT + 1, rows))
    w_act = jax.nn.silu(causal(xw[:, ch:], write_taps, HALO - SHORT + 1, rows))
    xs = [(x_act[:, h * p : (h + 1) * p] * step[:, h : h + 1]).astype(bf16) for h in range(heads)]
    w16 = w_act.astype(bf16)
    left = jnp.exp(total[:, None] - cumul).T
    ends = jnp.concatenate(
        [dot(xs[h], (w_act * left[:, h : h + 1]).astype(bf16), 0, 0) for h in range(heads)], 0
    ).astype(bf16)
    got = spread(jnp.concatenate([ends, log_rows(total)], 0), "sp_1")
    logs_y = jnp.sum(got[:, heads * p : heads * p + 3, :heads].astype(f32), 1)
    iy, ny = lax.axis_index("sp_1"), lax.axis_size("sp_1")
    k = jnp.arange(ny)
    after = lambda last: jnp.sum(
        jnp.where((k[None, :, None] > k[:, None, None]) & (k[None, :, None] < last), logs_y[None], 0.0), 1
    )
    c_in = jnp.where(k[:, None] < iy, jnp.exp(after(iy)), 0.0)
    c_all = jnp.exp(after(ny))
    pieces = got[:, : heads * p].astype(f32).reshape(ny, heads, p, STATE)
    enter_y = jnp.sum(pieces * c_in[:, :, None, None], 0)
    line = jnp.sum(pieces * c_all[:, :, None, None], 0).reshape(heads * p, STATE).astype(bf16)
    line_log = jnp.sum(logs_y, 0)
    before_log = jnp.sum(jnp.where(k[:, None] < iy, logs_y, 0.0), 0)
    got = spread(jnp.concatenate([line, log_rows(line_log)], 0), "sp_0")
    logs_z = jnp.sum(got[:, heads * p : heads * p + 3, :heads].astype(f32), 1)
    iz, nz = lax.axis_index("sp_0"), lax.axis_size("sp_0")
    k = jnp.arange(nz)
    between = jnp.sum(
        jnp.where((k[None, :, None] > k[:, None, None]) & (k[None, :, None] < iz), logs_z[None], 0.0), 1
    )
    c_in = jnp.where(k[:, None] < iz, jnp.exp(between + before_log), 0.0)
    c_init = jnp.exp(jnp.sum(jnp.where(k[:, None] < iz, logs_z, 0.0), 0) + before_log)
    pieces = got[:, : heads * p].astype(f32).reshape(nz, heads, p, STATE)
    start = enter_y + jnp.sum(pieces * c_in[:, :, None, None], 0) + c_init[:, None, None] * initial_state
    start = start.astype(bf16)
    back = rest[:, 4 * ch :]
    back_other = lax.ppermute(back, "tp", [(i, nt - 1 - i) for i in range(nt)])
    gain_both = lax.all_gather(conv_gain, "tp")
    proj = dot(normed, rest[:, : 4 * ch], 1, 0).astype(bf16).astype(f32)
    r_act = jax.nn.silu(causal(proj[:, :ch], fetch_taps, HALO - SHORT + 1, rows)).astype(bf16)
    z_gate = jax.nn.silu(proj[HALO:, ch : 2 * ch])
    glu = proj[:, 2 * ch : 3 * ch] * jax.nn.sigmoid(proj[:, 3 * ch :])
    mix = causal(glu, long_taps, HALO - WIDE + 1, rows)
    scores = dot(r_act, w16, 1, 1)
    lower = jnp.tril(jnp.ones((rows, rows), bool))
    inner = []
    for h in range(heads):
        gap = jnp.where(lower, cumul[h][:, None] - cumul[h][None, :], 0.0)
        m = jnp.where(lower, jnp.exp(gap) * scores, 0.0).astype(bf16)
        inner.append(dot(m, xs[h], 1, 0))
    ys = [inner[h] + dot(r_act, start[h], 1, 1) * jnp.exp(cumul[h])[:, None] for h in range(heads)]
    gated = jnp.concatenate(ys, 1) * z_gate
    sums = jnp.stack([jnp.sum(mix, 1), jnp.sum(mix * mix, 1), jnp.sum(gated * gated, 1)])
    sums = jnp.sum(spread(sums, FT), 0)

    def half(a):
        a = a.reshape(nf, nt, rows // (nf * nt), *a.shape[1:])
        return lax.dynamic_index_in_dim(a, tp, 1, keepdims=False).reshape(rows // nt, *a.shape[3:])

    pre = jnp.concatenate([mix.astype(bf16), (gated * state_gain).astype(bf16)], 1)
    both = lax.all_gather(pre, "tp", axis=0)
    sums = half(sums.T)
    mean = sums[:, 0:1] / C_CH
    rstd = lax.rsqrt(sums[:, 1:2] / C_CH - mean * mean + EPS)
    scale = lax.rsqrt(sums[:, 2:3] / D_INNER + EPS)
    part = 0.0
    for i, w in ((tp, back), (1 - tp, back_other)):
        a = half(lax.dynamic_index_in_dim(both, i, 0, keepdims=False)).astype(f32)
        g = lax.dynamic_index_in_dim(gain_both, i, 0, keepdims=False)
        conv = jax.nn.silu((a[:, :ch] - mean) * rstd * g)
        part = part + dot(jnp.concatenate([conv, a[:, ch:] * scale], 1).astype(bf16), w, 1, 1)
    pieces = lax.all_to_all(part.astype(bf16).reshape(nf, -1, part.shape[1]), "fs", 0, 0, tiled=True)
    return jnp.sum(pieces.astype(f32), 0).astype(bf16)


def solution(mesh):
    torus = Mesh(
        mesh.devices.reshape(8, 8, mesh.shape["fs"], mesh.shape["tp"]), ("sp_0", "sp_1", "fs", "tp")
    )
    w = P(SP, FT)
    in_specs = (
        P(SP, None), P(), w, w, w, w, w, w, P(), P(FT), P(FT), P(FT, SP), P(None, FT), P(None, FT), P(None, FT),
        P(None, FT), P(FT), P(FT), w, w, P(FT, None, None),
    )

    return jax.shard_map(per_device, mesh=torus, in_specs=in_specs, out_specs=P((*SP, *FT), None), check_vma=False)
```

```python
import jax
import jax.numpy as jnp
from jax import lax
from jax.experimental import pallas as pl
from jax.experimental.pallas import tpu as pltpu
from jax.sharding import Mesh
from jax.sharding import PartitionSpec as P


C_CH = 1024
STATE = 128
D_INNER = 1024
WIDE = 31
SHORT = 4
HALO = 32
EPS = 1e-06
LOGS = 16
SP = ("sp_0", "sp_1")
FT = ("fs", "tp")
f32 = jnp.float32
bf16 = jnp.bfloat16
VMEM = pl.BlockSpec(memory_space=pltpu.VMEM)
SMEM = pl.BlockSpec(memory_space=pltpu.SMEM)
HIGHEST = lax.Precision.HIGHEST
SMALL = pltpu.CompilerParams(vmem_limit_bytes=12 * 2**20)


def dot(a, b, ca, cb, precision=None):
    return lax.dot_general(a, b, (((ca,), (cb,)), ((), ())), precision=precision, preferred_element_type=f32)


def sds(shape, dtype):
    return jax.ShapeDtypeStruct(shape, dtype)


def held(*arrays):
    return tuple(pltpu.with_memory_space_constraint(a, pltpu.VMEM) for a in arrays)


def fetched(*arrays):
    return tuple(pltpu.with_memory_space_constraint(a, pltpu.HBM) for a in arrays)


def lay_out(shards, copies):
    rows, ch = shards[0].shape
    n = len(shards)

    def body(*refs):
        for i in range(n):
            w = refs[i][...]
            for k in range(copies):
                refs[n][k, :, i * ch : (i + 1) * ch] = w

    return pl.pallas_call(
        body, out_shape=sds((copies, rows, n * ch), bf16), in_specs=[VMEM] * n, out_specs=VMEM, compiler_params=SMALL
    )(*fetched(*shards))


def in_line(mine, other, index):
    n = 2 * mine.shape[0]

    def body(at, a, b, out):
        for j, off in enumerate((0, 4, 2, 6)):
            out[pl.ds(at[0] ^ off, 1)] = a[j : j + 1]
            out[pl.ds(at[0] ^ (off + 1), 1)] = b[j : j + 1]

    return pl.pallas_call(
        body, out_shape=sds((n, *mine.shape[1:]), bf16), in_specs=[SMEM, VMEM, VMEM], out_specs=VMEM, compiler_params=SMALL, name="in_line"
    )(index, *held(mine, other))


def log_rows(logs):
    hi = logs.astype(bf16).astype(f32)
    mid = (logs - hi).astype(bf16).astype(f32)
    lo = logs - hi - mid
    row = lax.broadcasted_iota(jnp.int32, (LOGS, STATE), 0)
    return jnp.where(row == 0, hi, jnp.where(row == 1, mid, jnp.where(row == 2, lo, 0.0))).astype(bf16)


def local_states(normed, first, taps, step, left, total, copies):
    ext, _ = normed.shape
    rows, ch = step.shape

    def body(nref, wref, tref, sref, lref, logs, send, xs, w16, buf):
        buf[...] = dot(nref[...], wref[...], 1, 0).astype(bf16).astype(f32)
        at = HALO - SHORT + 1
        mix = sum(buf[at + i : at + i + rows, :] * tref[i : i + 1, :] for i in range(SHORT))
        act = jax.nn.silu(mix)
        x = act[:, :ch] * sref[...]
        w = act[:, ch:].astype(bf16)
        xs[...] = x.astype(bf16)
        w16[...] = w
        ends = dot((x * lref[...]).astype(bf16), w, 0, 0).astype(bf16)
        tail = log_rows(logs[...])
        for k in range(copies):
            send[k, :ch, :] = ends
            send[k, ch:, :] = tail

    return pl.pallas_call(
        body,
        out_shape=(sds((copies, ch + LOGS, STATE), bf16), pltpu.VMEM((rows, ch), bf16), pltpu.VMEM((rows, STATE), bf16)),
        in_specs=[VMEM] * 6,
        out_specs=(VMEM,) * 3,
        scratch_shapes=[pltpu.VMEM((ext, 2 * ch), f32)],
        compiler_params=SMALL, name="local_states",
    )(*held(normed, first, taps, step, left, total))


def spread_heads(c, heads, p):
    return jnp.concatenate([jnp.broadcast_to(c[:, h : h + 1], (p, STATE)) for h in range(heads)], 0)


def line_states(got, index, heads, p, copies):
    n, size, _ = got.shape
    ch = heads * p

    def body(at, ref, enter, before, send):
        zero = jnp.zeros((1, STATE), f32)
        acc_in, acc_all = zero, zero
        ent = jnp.zeros((ch, STATE), f32)
        tot = jnp.zeros((ch, STATE), f32)
        for k in reversed(range(n)):
            logs = jnp.sum(ref[k, ch:, :].astype(f32), axis=0, keepdims=True)
            inside = (k < at[0]).astype(f32)
            piece = ref[k, :ch, :].astype(f32)
            ent = ent + piece * spread_heads(inside * jnp.exp(acc_in), heads, p)
            tot = tot + piece * spread_heads(jnp.exp(acc_all), heads, p)
            acc_in = acc_in + inside * logs
            acc_all = acc_all + logs
        enter[...] = ent
        before[...] = jnp.broadcast_to(acc_in, (8, STATE))
        line, tail = tot.astype(bf16), log_rows(acc_all)
        for k in range(copies):
            send[k, :ch, :] = line
            send[k, ch:, :] = tail

    return pl.pallas_call(
        body,
        out_shape=(pltpu.VMEM((ch, STATE), f32), pltpu.VMEM((8, STATE), f32), sds((copies, size, STATE), bf16)),
        in_specs=[SMEM, VMEM],
        out_specs=(VMEM,) * 3,
        compiler_params=SMALL, name="line_states",
    )(index, *held(got))


def rows_done(normed, rest, got, enter, before, init, index, ftaps, ltaps, xs, w16, cum, cum_t, gain, copies):
    ext, d = normed.shape
    rows, ch = xs.shape
    n, _, _ = got.shape
    heads = cum_t.shape[0]
    p = ch // heads
    steps = 4
    kb = d // steps
    part = 64

    def body(at, nref, wref, got, enter, before, init, ftaps, ltaps, xs, w16, cum, cum_t, gain, sums, pre, back, acc, glu):
        k = pl.program_id(0)
        at_k = pl.ds(pl.multiple_of(k * kb, kb), kb)
        term = dot(nref[:, at_k], wref[:, : 4 * ch], 1, 0)
        back[at_k, :] = wref[:, 4 * ch :]

        @pl.when(k == 0)
        def _():
            acc[...] = term

        @pl.when(k > 0)
        def _():
            acc[...] += term

        @pl.when(k == steps - 1)
        def _():
            glu[...] = acc[:, 2 * ch : 3 * ch].astype(bf16).astype(f32) * jax.nn.sigmoid(
                acc[:, 3 * ch :].astype(bf16).astype(f32)
            )
            acc[:, : 2 * ch] = acc[:, : 2 * ch].astype(bf16).astype(f32)
            s_at, l_at = HALO - SHORT + 1, HALO - WIDE + 1
            read = sum(acc[s_at + i : s_at + i + rows, :ch] * ftaps[i : i + 1, :] for i in range(SHORT))
            read = jax.nn.silu(read).astype(bf16)
            z = jax.nn.silu(acc[HALO:, ch : 2 * ch])
            acc_in = jnp.zeros((1, STATE), f32)
            start = enter[...]
            b = before[0:1, :]
            for j in reversed(range(n)):
                logs = jnp.sum(got[j, ch:, :].astype(f32), axis=0, keepdims=True)
                inside = (j < at[0]).astype(f32)
                start = start + got[j, :ch, :].astype(f32) * spread_heads(inside * jnp.exp(acc_in + b), heads, p)
                acc_in = acc_in + inside * logs
            start = start + init[...] * spread_heads(jnp.exp(acc_in + b), heads, p)
            y = dot(read, start.astype(bf16), 1, 1) * jnp.exp(cum[...])
            scores = dot(read, w16[...], 1, 1)
            lower = lax.broadcasted_iota(jnp.int32, (rows, rows), 0) >= lax.broadcasted_iota(jnp.int32, (rows, rows), 1)
            lane = lax.broadcasted_iota(jnp.int32, (rows, ch), 1)
            for h in range(heads):
                gap = jnp.where(lower, cum[:, h * p : h * p + 1] - cum_t[h : h + 1, :], 0.0)
                m = jnp.where(lower, jnp.exp(gap) * scores, 0.0).astype(bf16)
                x = jnp.where(lane // p == h, xs[...].astype(f32), 0.0).astype(bf16)
                y = y + dot(m, x, 1, 0)
            gated = y * z
            mix = jnp.concatenate(
                [
                    sum(glu[l_at + r + i : l_at + r + i + part, :] * ltaps[i : i + 1, :] for i in range(WIDE))
                    for r in range(0, rows, part)
                ],
                0,
            )
            squares = jnp.concatenate([mix, mix * mix, gated * gated], 1)
            pick = lax.broadcasted_iota(jnp.int32, (8, 3 * ch), 1) // ch == lax.broadcasted_iota(jnp.int32, (8, 3 * ch), 0)
            found = dot(jnp.where(pick, 1.0, 0.0), squares, 1, 1, HIGHEST)
            for j in range(copies):
                sums[j] = found[:3]
            pre[:, :ch] = mix.astype(bf16)
            pre[:, ch:] = (gated * gain[...]).astype(bf16)

    small = (got, enter, before, init, ftaps, ltaps, xs, w16, cum, cum_t, gain)
    return pl.pallas_call(
        body,
        grid=(steps,),
        out_shape=(sds((copies, 3, rows), f32), pltpu.VMEM((rows, 2 * ch), bf16), pltpu.VMEM((d, 2 * ch), bf16)),
        in_specs=[SMEM, VMEM, pl.BlockSpec((kb, 6 * ch), lambda k: (k, 0)), *[VMEM] * len(small)],
        out_specs=(pl.BlockSpec((copies, 3, rows), lambda k: (0, 0, 0)), VMEM, VMEM),
        scratch_shapes=[pltpu.VMEM((ext, 4 * ch), f32), pltpu.VMEM((ext, ch), f32)],
        compiler_params=SMALL, name="rows_done",
    )(index, *held(normed), *fetched(rest), *held(*small))


def output_rows(sums, both, gains, own, other, index, nf, nt):
    copies, _, rows = sums.shape
    ch = gains.shape[1]
    d = own.shape[0]
    piece = rows // (nf * nt)

    def body(at, sref, bref, gref, wa, wb, out, cols, act):
        tp = at[0]
        s = sref[0]
        for j in range(1, copies):
            s = s + sref[j]
        cols[...] = jnp.transpose(jnp.concatenate([s, jnp.zeros((5, rows), f32)], 0))
        for i in range(nf):
            at_row = pl.multiple_of(i * (nt * piece) + tp * piece, piece)
            here = slice(i * piece, (i + 1) * piece)
            t = cols[pl.ds(at_row, piece), :]
            mean = t[:, 0:1] / C_CH
            rstd = lax.rsqrt(t[:, 1:2] / C_CH - mean * mean + EPS)
            scale = lax.rsqrt(t[:, 2:3] / D_INNER + EPS)
            for j in range(nt):
                src = tp if j == 0 else 1 - tp
                a = bref[pl.ds(pl.multiple_of(src * rows + at_row, piece), piece), :].astype(f32)
                conv = jax.nn.silu((a[:, :ch] - mean) * rstd * gref[pl.ds(src, 1), :])
                act[here, 2 * j * ch : (2 * j + 1) * ch] = conv.astype(bf16)
                act[here, (2 * j + 1) * ch : (2 * j + 2) * ch] = (a[:, ch:] * scale).astype(bf16)
        term = dot(act[:, : 2 * ch], wa[...], 1, 1) + dot(act[:, 2 * ch :], wb[...], 1, 1)
        out[...] = term.astype(bf16).reshape(nf, piece, d)

    return pl.pallas_call(
        body,
        out_shape=sds((nf, piece, d), bf16),
        in_specs=[SMEM, *[VMEM] * 5],
        out_specs=VMEM,
        scratch_shapes=[pltpu.VMEM((rows, 8), f32), pltpu.VMEM((nf * piece, 4 * ch), bf16)],
        compiler_params=SMALL, name="output_rows",
    )(index, *held(sums, both, gains, own, other))


def per_device(
    tokens, norm_gain, conv_value, conv_gate, mixer_gate, state_input, write_projection, state_read,
    step_proj, step_bias, decay_log, decay_extra, input_taps, write_taps, fetch_taps, long_taps,
    conv_gain, state_gain, conv_output, state_output, initial_state,
):
    rows = tokens.shape[0]
    ch = conv_value.shape[1]
    heads = step_bias.shape[0]
    p = ch // heads
    nf, nt = lax.axis_size("fs"), lax.axis_size("tp")
    iz, iy, tp = (lax.axis_index(a).astype(jnp.int32).reshape(1) for a in ("sp_0", "sp_1", "tp"))
    ny = lax.axis_size("sp_1")
    block = lay_out((state_read, mixer_gate, conv_value, conv_gate, conv_output, state_output), 1)
    for bit in (4, 2):
        block = jnp.concatenate([block, lax.ppermute(block, "sp_1", [(i, i ^ bit) for i in range(ny)])], 0)
    other = lax.ppermute(block, "sp_1", [(i, i ^ 1) for i in range(ny)])
    rest = in_line(block, other, iy).reshape(-1, 6 * ch)
    rest = lax.all_gather(rest, "sp_0", axis=0, tiled=True)
    first = lay_out((state_input, write_projection), lax.axis_size(SP))
    first = lax.all_to_all(first, SP, 0, 0, tiled=True).reshape(-1, 2 * ch)
    n = lax.axis_size(SP)
    halo = lax.ppermute(tokens[rows - HALO :], SP, [(i, i + 1) for i in range(n - 1)])
    v = jnp.concatenate([halo, tokens], 0).astype(f32)
    normed = (v * lax.rsqrt(jnp.mean(v * v, axis=1, keepdims=True) + EPS) * norm_gain).astype(bf16)
    step_all = jnp.dot(normed[HALO:], step_proj, preferred_element_type=f32)
    me = lax.axis_index("fs") * nt + lax.axis_index("tp")
    step = jax.nn.softplus(lax.dynamic_slice_in_dim(step_all, me * heads, heads, 1) + step_bias)
    log_step = (-jnp.exp(decay_log) * step + decay_extra.T).T
    cum_t = jnp.cumsum(log_step, axis=1)
    total = cum_t[:, -1]
    cum = jnp.repeat(cum_t.T, p, axis=1)
    step = jnp.repeat(step, p, axis=1)
    left = jnp.repeat(jnp.exp(total[:, None] - cum_t).T, p, axis=1)
    total = jnp.pad(total[None], ((0, 0), (0, STATE - heads)))
    gains = lax.all_gather(conv_gain, "tp")
    taps = jnp.concatenate([input_taps, write_taps], 1)
    send, xs, w16 = local_states(normed, first, taps, step, left, total, ny)
    got = lax.all_to_all(send, "sp_1", 0, 0, tiled=True)
    enter, before, send = line_states(got, iy, heads, p, lax.axis_size("sp_0"))
    got = lax.all_to_all(send, "sp_0", 0, 0, tiled=True)
    sums, pre, back = rows_done(
        normed, rest, got, enter, before, initial_state.reshape(ch, STATE), iz, fetch_taps, long_taps, xs, w16,
        cum, cum_t, state_gain[None], nf * nt,
    )
    sums = lax.all_to_all(sums, FT, 0, 0, tiled=True)
    both = lax.all_gather(pre, "tp", axis=0, tiled=True)
    back_other = lax.ppermute(back, "tp", [(i, nt - 1 - i) for i in range(nt)])
    out = output_rows(sums, both, gains, back, back_other, tp, nf, nt)
    pieces = lax.all_to_all(out, "fs", 0, 0, tiled=True)
    return jnp.sum(pieces.astype(f32), 0).astype(bf16)


def solution(mesh):
    torus = Mesh(
        mesh.devices.reshape(8, 8, mesh.shape["fs"], mesh.shape["tp"]), ("sp_0", "sp_1", "fs", "tp")
    )
    w = P(SP, FT)
    in_specs = (
        P(SP, None), P(), w, w, w, w, w, w, P(), P(FT), P(FT), P(FT, SP), P(None, FT), P(None, FT), P(None, FT),
        P(None, FT), P(FT), P(FT), w, w, P(FT, None, None),
    )

    return jax.shard_map(per_device, mesh=torus, in_specs=in_specs, out_specs=P((*SP, *FT), None), check_vma=False)
```

```python
import jax
import jax.numpy as jnp
from jax import lax
from jax.experimental import pallas as pl
from jax.experimental.pallas import tpu as pltpu
from jax.sharding import Mesh
from jax.sharding import PartitionSpec as P


C_CH = 1024
STATE = 128
D_INNER = 1024
WIDE = 31
SHORT = 4
HALO = 32
EPS = 1e-06
LOGS = 16
SP = ("sp_0", "sp_1")
FT = ("fs", "tp")
f32 = jnp.float32
bf16 = jnp.bfloat16
VMEM = pl.BlockSpec(memory_space=pltpu.VMEM)
SMEM = pl.BlockSpec(memory_space=pltpu.SMEM)
HIGHEST = lax.Precision.HIGHEST
SMALL = pltpu.CompilerParams(vmem_limit_bytes=12 * 2**20)


def dot(a, b, ca, cb, precision=None):
    return lax.dot_general(a, b, (((ca,), (cb,)), ((), ())), precision=precision, preferred_element_type=f32)


def sds(shape, dtype):
    return jax.ShapeDtypeStruct(shape, dtype)


def held(*arrays):
    return tuple(pltpu.with_memory_space_constraint(a, pltpu.VMEM) for a in arrays)


def fetched(*arrays):
    return tuple(pltpu.with_memory_space_constraint(a, pltpu.HBM) for a in arrays)


def lay_out(shards, copies):
    rows, ch = shards[0].shape
    n = len(shards)

    def body(*refs):
        for i in range(n):
            w = refs[i][...]
            for k in range(copies):
                refs[n][k, :, i * ch : (i + 1) * ch] = w

    return pl.pallas_call(
        body, out_shape=sds((copies, rows, n * ch), bf16), in_specs=[VMEM] * n, out_specs=VMEM, compiler_params=SMALL
    )(*fetched(*shards))


def copies_of(block, copies):
    def body(ref, out):
        for k in range(copies):
            out[k] = ref[...]

    return pl.pallas_call(
        body, out_shape=sds((copies, *block.shape), bf16), in_specs=[VMEM], out_specs=VMEM, compiler_params=SMALL
    )(*held(block))


def log_rows(logs):
    hi = logs.astype(bf16).astype(f32)
    mid = (logs - hi).astype(bf16).astype(f32)
    lo = logs - hi - mid
    row = lax.broadcasted_iota(jnp.int32, (LOGS, STATE), 0)
    return jnp.where(row == 0, hi, jnp.where(row == 1, mid, jnp.where(row == 2, lo, 0.0))).astype(bf16)


def local_states(normed, first, taps, step, left, total, copies):
    ext, d = normed.shape
    rows, ch = step.shape
    ny, nz, piece, _ = first.shape

    def body(nref, wref, tref, sref, lref, logs, send, xs, w16, buf, wall):
        for y in range(ny):
            for z in range(nz):
                wall[(z * ny + y) * piece : (z * ny + y + 1) * piece, :] = wref[y, z]
        buf[...] = dot(nref[...], wall[...], 1, 0).astype(bf16).astype(f32)
        at = HALO - SHORT + 1
        mix = sum(buf[at + i : at + i + rows, :] * tref[i : i + 1, :] for i in range(SHORT))
        act = jax.nn.silu(mix)
        x = act[:, :ch] * sref[...]
        w = act[:, ch:].astype(bf16)
        xs[...] = x.astype(bf16)
        w16[...] = w
        ends = dot((x * lref[...]).astype(bf16), w, 0, 0).astype(bf16)
        tail = log_rows(logs[...])
        for k in range(copies):
            send[k, :ch, :] = ends
            send[k, ch:, :] = tail

    return pl.pallas_call(
        body,
        out_shape=(sds((copies, ch + LOGS, STATE), bf16), pltpu.VMEM((rows, ch), bf16), pltpu.VMEM((rows, STATE), bf16)),
        in_specs=[VMEM] * 6,
        out_specs=(VMEM,) * 3,
        scratch_shapes=[pltpu.VMEM((ext, 2 * ch), f32), pltpu.VMEM((d, 2 * ch), bf16)],
        compiler_params=SMALL, name="local_states",
    )(*held(normed, first, taps, step, left, total))


def spread_heads(c, heads, p):
    return jnp.concatenate([jnp.broadcast_to(c[:, h : h + 1], (p, STATE)) for h in range(heads)], 0)


def line_states(got, index, heads, p, copies):
    n, size, _ = got.shape
    ch = heads * p

    def body(at, ref, enter, before, send):
        zero = jnp.zeros((1, STATE), f32)
        acc_in, acc_all = zero, zero
        ent = jnp.zeros((ch, STATE), f32)
        tot = jnp.zeros((ch, STATE), f32)
        for k in reversed(range(n)):
            logs = jnp.sum(ref[k, ch:, :].astype(f32), axis=0, keepdims=True)
            inside = (k < at[0]).astype(f32)
            piece = ref[k, :ch, :].astype(f32)
            ent = ent + piece * spread_heads(inside * jnp.exp(acc_in), heads, p)
            tot = tot + piece * spread_heads(jnp.exp(acc_all), heads, p)
            acc_in = acc_in + inside * logs
            acc_all = acc_all + logs
        enter[...] = ent
        before[...] = jnp.broadcast_to(acc_in, (8, STATE))
        line, tail = tot.astype(bf16), log_rows(acc_all)
        for k in range(copies):
            send[k, :ch, :] = line
            send[k, ch:, :] = tail

    return pl.pallas_call(
        body,
        out_shape=(pltpu.VMEM((ch, STATE), f32), pltpu.VMEM((8, STATE), f32), sds((copies, size, STATE), bf16)),
        in_specs=[SMEM, VMEM],
        out_specs=(VMEM,) * 3,
        compiler_params=SMALL, name="line_states",
    )(index, *held(got))


def rows_local(normed, rest, ftaps, ltaps, xs, w16, cum, cum_t):
    ext, d = normed.shape
    rows, ch = xs.shape
    heads = cum_t.shape[0]
    p = ch // heads
    steps = 4
    kb = d // steps
    part = 64

    def body(nref, wref, ftaps, ltaps, xs, w16, cum, cum_t, read16, zgate, mixed, inner, back, acc, glu):
        k = pl.program_id(0)
        at_k = pl.ds(pl.multiple_of(k * kb, kb), kb)
        term = dot(nref[:, at_k], wref[:, : 4 * ch], 1, 0)
        back[at_k, :] = wref[:, 4 * ch :]

        @pl.when(k == 0)
        def _():
            acc[...] = term

        @pl.when(k > 0)
        def _():
            acc[...] += term

        @pl.when(k == steps - 1)
        def _():
            glu[...] = acc[:, 2 * ch : 3 * ch].astype(bf16).astype(f32) * jax.nn.sigmoid(
                acc[:, 3 * ch :].astype(bf16).astype(f32)
            )
            acc[:, : 2 * ch] = acc[:, : 2 * ch].astype(bf16).astype(f32)
            s_at, l_at = HALO - SHORT + 1, HALO - WIDE + 1
            read = sum(acc[s_at + i : s_at + i + rows, :ch] * ftaps[i : i + 1, :] for i in range(SHORT))
            read = jax.nn.silu(read).astype(bf16)
            read16[...] = read
            zgate[...] = jax.nn.silu(acc[HALO:, ch : 2 * ch])
            scores = dot(read, w16[...], 1, 1)
            lower = lax.broadcasted_iota(jnp.int32, (rows, rows), 0) >= lax.broadcasted_iota(jnp.int32, (rows, rows), 1)
            lane = lax.broadcasted_iota(jnp.int32, (rows, ch), 1)
            y = jnp.zeros((rows, ch), f32)
            for h in range(heads):
                gap = jnp.where(lower, cum[:, h * p : h * p + 1] - cum_t[h : h + 1, :], 0.0)
                m = jnp.where(lower, jnp.exp(gap) * scores, 0.0).astype(bf16)
                x = jnp.where(lane // p == h, xs[...].astype(f32), 0.0).astype(bf16)
                y = y + dot(m, x, 1, 0)
            inner[...] = y
            for r in range(0, rows, part):
                mixed[r : r + part, :] = sum(
                    glu[l_at + r + i : l_at + r + i + part, :] * ltaps[i : i + 1, :] for i in range(WIDE)
                )

    small = (ftaps, ltaps, xs, w16, cum, cum_t)
    return pl.pallas_call(
        body,
        grid=(steps,),
        out_shape=(
            pltpu.VMEM((rows, STATE), bf16), pltpu.VMEM((rows, ch), f32), pltpu.VMEM((rows, ch), f32),
            pltpu.VMEM((rows, ch), f32), pltpu.VMEM((d, 2 * ch), bf16),
        ),
        in_specs=[VMEM, pl.BlockSpec((kb, 6 * ch), lambda k: (k, 0)), *[VMEM] * len(small)],
        out_specs=(VMEM,) * 5,
        scratch_shapes=[pltpu.VMEM((ext, 4 * ch), f32), pltpu.VMEM((ext, ch), f32)],
        compiler_params=SMALL, name="rows_local",
    )(*held(normed), *fetched(rest), *held(*small))


def rows_done(got, enter, before, init, index, read16, zgate, mixed, inner, cum, gain, copies):
    rows, ch = mixed.shape
    n, _, _ = got.shape
    heads = init.shape[0]
    p = ch // heads

    def body(at, got, enter, before, init, read16, zgate, mixed, inner, cum, gain, sums, pre):
        acc_in = jnp.zeros((1, STATE), f32)
        start = enter[...]
        b = before[0:1, :]
        for j in reversed(range(n)):
            logs = jnp.sum(got[j, ch:, :].astype(f32), axis=0, keepdims=True)
            inside = (j < at[0]).astype(f32)
            start = start + got[j, :ch, :].astype(f32) * spread_heads(inside * jnp.exp(acc_in + b), heads, p)
            acc_in = acc_in + inside * logs
        start = start + init[...].reshape(ch, STATE) * spread_heads(jnp.exp(acc_in + b), heads, p)
        y = inner[...] + dot(read16[...], start.astype(bf16), 1, 1) * jnp.exp(cum[...])
        gated = y * zgate[...]
        mix = mixed[...]
        squares = jnp.concatenate([mix, mix * mix, gated * gated], 1)
        pick = lax.broadcasted_iota(jnp.int32, (8, 3 * ch), 1) // ch == lax.broadcasted_iota(jnp.int32, (8, 3 * ch), 0)
        found = dot(jnp.where(pick, 1.0, 0.0), squares, 1, 1, HIGHEST)
        for j in range(copies):
            sums[j] = found[:3]
        pre[:, :ch] = mix.astype(bf16)
        pre[:, ch:] = (gated * gain[...]).astype(bf16)

    return pl.pallas_call(
        body,
        out_shape=(sds((copies, 3, rows), f32), pltpu.VMEM((rows, 2 * ch), bf16)),
        in_specs=[SMEM, *[VMEM] * 10],
        out_specs=(VMEM, VMEM),
        compiler_params=SMALL, name="rows_done",
    )(index, *held(got, enter, before, init, read16, zgate, mixed, inner, cum, gain))


def output_rows(sums, both, gains, own, other, index, nf, nt):
    copies, _, rows = sums.shape
    ch = gains.shape[1]
    d = own.shape[0]
    piece = rows // (nf * nt)

    def body(at, sref, bref, gref, wa, wb, out, cols, act):
        tp = at[0]
        s = sref[0]
        for j in range(1, copies):
            s = s + sref[j]
        cols[...] = jnp.transpose(jnp.concatenate([s, jnp.zeros((5, rows), f32)], 0))
        for i in range(nf):
            at_row = pl.multiple_of(i * (nt * piece) + tp * piece, piece)
            here = slice(i * piece, (i + 1) * piece)
            t = cols[pl.ds(at_row, piece), :]
            mean = t[:, 0:1] / C_CH
            rstd = lax.rsqrt(t[:, 1:2] / C_CH - mean * mean + EPS)
            scale = lax.rsqrt(t[:, 2:3] / D_INNER + EPS)
            for j in range(nt):
                src = tp if j == 0 else 1 - tp
                a = bref[pl.ds(pl.multiple_of(src * rows + at_row, piece), piece), :].astype(f32)
                conv = jax.nn.silu((a[:, :ch] - mean) * rstd * gref[pl.ds(src, 1), :])
                act[here, 2 * j * ch : (2 * j + 1) * ch] = conv.astype(bf16)
                act[here, (2 * j + 1) * ch : (2 * j + 2) * ch] = (a[:, ch:] * scale).astype(bf16)
        term = dot(act[:, : 2 * ch], wa[...], 1, 1) + dot(act[:, 2 * ch :], wb[...], 1, 1)
        out[...] = term.astype(bf16).reshape(nf, piece, d)

    return pl.pallas_call(
        body,
        out_shape=sds((nf, piece, d), bf16),
        in_specs=[SMEM, *[VMEM] * 5],
        out_specs=VMEM,
        scratch_shapes=[pltpu.VMEM((rows, 8), f32), pltpu.VMEM((nf * piece, 4 * ch), bf16)],
        compiler_params=SMALL, name="output_rows",
    )(index, *held(sums, both, gains, own, other))


def per_device(
    tokens, norm_gain, conv_value, conv_gate, mixer_gate, state_input, write_projection, state_read,
    step_proj, step_bias, decay_log, decay_extra, input_taps, write_taps, fetch_taps, long_taps,
    conv_gain, state_gain, conv_output, state_output, initial_state,
):
    rows = tokens.shape[0]
    ch = conv_value.shape[1]
    heads = step_bias.shape[0]
    p = ch // heads
    nf, nt = lax.axis_size("fs"), lax.axis_size("tp")
    iz, iy, tp = (lax.axis_index(a).astype(jnp.int32).reshape(1) for a in ("sp_0", "sp_1", "tp"))
    ny = lax.axis_size("sp_1")
    first = lay_out((state_input, write_projection), lax.axis_size("sp_0"))
    first = lax.all_to_all(first, "sp_0", 0, 0, tiled=True)
    rest = lay_out((state_read, mixer_gate, conv_value, conv_gate, conv_output, state_output), ny)
    rest = lax.all_to_all(rest, "sp_1", 0, 0, tiled=True).reshape(-1, 6 * ch)
    rest = lax.all_gather(rest, "sp_0", axis=0, tiled=True)
    first = copies_of(first, ny)
    first = lax.all_to_all(first, "sp_1", 0, 0, tiled=True)
    n = lax.axis_size(SP)
    halo = lax.ppermute(tokens[rows - HALO :], SP, [(i, i + 1) for i in range(n - 1)])
    v = jnp.concatenate([halo, tokens], 0).astype(f32)
    normed = (v * lax.rsqrt(jnp.mean(v * v, axis=1, keepdims=True) + EPS) * norm_gain).astype(bf16)
    step_all = jnp.dot(normed[HALO:], step_proj, preferred_element_type=f32)
    me = lax.axis_index("fs") * nt + lax.axis_index("tp")
    step = jax.nn.softplus(lax.dynamic_slice_in_dim(step_all, me * heads, heads, 1) + step_bias)
    log_step = (-jnp.exp(decay_log) * step + decay_extra.T).T
    cum_t = jnp.cumsum(log_step, axis=1)
    total = cum_t[:, -1]
    cum = jnp.repeat(cum_t.T, p, axis=1)
    step = jnp.repeat(step, p, axis=1)
    left = jnp.repeat(jnp.exp(total[:, None] - cum_t).T, p, axis=1)
    total = jnp.pad(total[None], ((0, 0), (0, STATE - heads)))
    gains = lax.all_gather(conv_gain, "tp")
    taps = jnp.concatenate([input_taps, write_taps], 1)
    send, xs, w16 = local_states(normed, first, taps, step, left, total, ny)
    got = lax.all_to_all(send, "sp_1", 0, 0, tiled=True)
    enter, before, send = line_states(got, iy, heads, p, lax.axis_size("sp_0"))
    got = lax.all_to_all(send, "sp_0", 0, 0, tiled=True)
    read16, zgate, mixed, inner, back = rows_local(normed, rest, fetch_taps, long_taps, xs, w16, cum, cum_t)
    back_other = lax.ppermute(back, "tp", [(i, nt - 1 - i) for i in range(nt)])
    sums, pre = rows_done(
        got, enter, before, initial_state, iz, read16, zgate, mixed, inner, cum, state_gain[None], nf * nt
    )
    sums = lax.all_to_all(sums, FT, 0, 0, tiled=True)
    both = lax.all_gather(pre, "tp", axis=0, tiled=True)
    out = output_rows(sums, both, gains, back, back_other, tp, nf, nt)
    pieces = lax.all_to_all(out, "fs", 0, 0, tiled=True)
    return jnp.sum(pieces.astype(f32), 0).astype(bf16)


def solution(mesh):
    torus = Mesh(
        mesh.devices.reshape(8, 8, mesh.shape["fs"], mesh.shape["tp"]), ("sp_0", "sp_1", "fs", "tp")
    )
    w = P(SP, FT)
    in_specs = (
        P(SP, None), P(), w, w, w, w, w, w, P(), P(FT), P(FT), P(FT, SP), P(None, FT), P(None, FT), P(None, FT),
        P(None, FT), P(FT), P(FT), w, w, P(FT, None, None),
    )

    return jax.shard_map(per_device, mesh=torus, in_specs=in_specs, out_specs=P((*SP, *FT), None), check_vma=False)
```

```python
import jax
import jax.numpy as jnp
from jax import lax
from jax.experimental import pallas as pl
from jax.experimental.pallas import tpu as pltpu
from jax.sharding import Mesh
from jax.sharding import PartitionSpec as P


C_CH = 1024
STATE = 128
D_INNER = 1024
WIDE = 31
SHORT = 4
HALO = 32
EPS = 1e-06
LOGS = 16
SP = ("sp_0", "sp_1")
FT = ("fs", "tp")
f32 = jnp.float32
bf16 = jnp.bfloat16
VMEM = pl.BlockSpec(memory_space=pltpu.VMEM)
SMEM = pl.BlockSpec(memory_space=pltpu.SMEM)
HIGHEST = lax.Precision.HIGHEST
SMALL = pltpu.CompilerParams(vmem_limit_bytes=12 * 2**20)


def dot(a, b, ca, cb, precision=None):
    return lax.dot_general(a, b, (((ca,), (cb,)), ((), ())), precision=precision, preferred_element_type=f32)


def sds(shape, dtype):
    return jax.ShapeDtypeStruct(shape, dtype)


def held(*arrays):
    return tuple(pltpu.with_memory_space_constraint(a, pltpu.VMEM) for a in arrays)


def fetched(*arrays):
    return tuple(pltpu.with_memory_space_constraint(a, pltpu.HBM) for a in arrays)


def lay_out(shards, copies):
    rows, ch = shards[0].shape
    n = len(shards)

    def body(*refs):
        for i in range(n):
            w = refs[i][...]
            for k in range(copies):
                refs[n][k, :, i * ch : (i + 1) * ch] = w

    return pl.pallas_call(
        body, out_shape=sds((copies, rows, n * ch), bf16), in_specs=[VMEM] * n, out_specs=VMEM, compiler_params=SMALL
    )(*fetched(*shards))


def copies_of(block, copies):
    def body(ref, out):
        for k in range(copies):
            out[k] = ref[...]

    return pl.pallas_call(
        body, out_shape=sds((copies, *block.shape), bf16), in_specs=[VMEM], out_specs=VMEM, compiler_params=SMALL
    )(*held(block))


def log_rows(logs):
    hi = logs.astype(bf16).astype(f32)
    mid = (logs - hi).astype(bf16).astype(f32)
    lo = logs - hi - mid
    row = lax.broadcasted_iota(jnp.int32, (LOGS, STATE), 0)
    return jnp.where(row == 0, hi, jnp.where(row == 1, mid, jnp.where(row == 2, lo, 0.0))).astype(bf16)


def local_states(normed, first, taps, step, left, total, copies):
    ext, d = normed.shape
    rows, ch = step.shape
    ny, nz, piece, _ = first.shape

    def body(nref, wref, tref, sref, lref, logs, send, xs, w16, buf, wall):
        for y in range(ny):
            for z in range(nz):
                wall[(z * ny + y) * piece : (z * ny + y + 1) * piece, :] = wref[y, z]
        buf[...] = dot(nref[...], wall[...], 1, 0).astype(bf16).astype(f32)
        at = HALO - SHORT + 1
        mix = sum(buf[at + i : at + i + rows, :] * tref[i : i + 1, :] for i in range(SHORT))
        act = jax.nn.silu(mix)
        x = act[:, :ch] * sref[...]
        w = act[:, ch:].astype(bf16)
        xs[...] = x.astype(bf16)
        w16[...] = w
        ends = dot((x * lref[...]).astype(bf16), w, 0, 0).astype(bf16)
        tail = log_rows(logs[...])
        for k in range(copies):
            send[k, :ch, :] = ends
            send[k, ch:, :] = tail

    return pl.pallas_call(
        body,
        out_shape=(sds((copies, ch + LOGS, STATE), bf16), pltpu.VMEM((rows, ch), bf16), pltpu.VMEM((rows, STATE), bf16)),
        in_specs=[VMEM] * 6,
        out_specs=(VMEM,) * 3,
        scratch_shapes=[pltpu.VMEM((ext, 2 * ch), f32), pltpu.VMEM((d, 2 * ch), bf16)],
        compiler_params=SMALL, name="local_states",
    )(*held(normed, first, taps, step, left, total))


def spread_heads(c, heads, p):
    return jnp.concatenate([jnp.broadcast_to(c[:, h : h + 1], (p, STATE)) for h in range(heads)], 0)


def line_states(got, index, heads, p, copies):
    n, size, _ = got.shape
    ch = heads * p

    def body(at, ref, enter, before, send):
        zero = jnp.zeros((1, STATE), f32)
        acc_in, acc_all = zero, zero
        ent = jnp.zeros((ch, STATE), f32)
        tot = jnp.zeros((ch, STATE), f32)
        for k in reversed(range(n)):
            logs = jnp.sum(ref[k, ch:, :].astype(f32), axis=0, keepdims=True)
            inside = (k < at[0]).astype(f32)
            piece = ref[k, :ch, :].astype(f32)
            ent = ent + piece * spread_heads(inside * jnp.exp(acc_in), heads, p)
            tot = tot + piece * spread_heads(jnp.exp(acc_all), heads, p)
            acc_in = acc_in + inside * logs
            acc_all = acc_all + logs
        enter[...] = ent
        before[...] = jnp.broadcast_to(acc_in, (8, STATE))
        line, tail = tot.astype(bf16), log_rows(acc_all)
        for k in range(copies):
            send[k, :ch, :] = line
            send[k, ch:, :] = tail

    return pl.pallas_call(
        body,
        out_shape=(pltpu.VMEM((ch, STATE), f32), pltpu.VMEM((8, STATE), f32), sds((copies, size, STATE), bf16)),
        in_specs=[SMEM, VMEM],
        out_specs=(VMEM,) * 3,
        compiler_params=SMALL, name="line_states",
    )(index, *held(got))


def rows_local(normed, rest, ftaps, ltaps, xs, w16, cum, cum_t):
    ext, d = normed.shape
    rows, ch = xs.shape
    heads = cum_t.shape[0]
    p = ch // heads
    steps = 4
    kb = d // steps
    part = 64

    def body(nref, wref, ftaps, ltaps, xs, w16, cum, cum_t, read16, zgate, mixed, inner, back, acc, glu):
        k = pl.program_id(0)
        at_k = pl.ds(pl.multiple_of(k * kb, kb), kb)
        term = dot(nref[:, at_k], wref[:, : 4 * ch], 1, 0)
        back[at_k, :] = wref[:, 4 * ch :]

        @pl.when(k == 0)
        def _():
            acc[...] = term

        @pl.when(k > 0)
        def _():
            acc[...] += term

        @pl.when(k == steps - 1)
        def _():
            glu[...] = acc[:, 2 * ch : 3 * ch].astype(bf16).astype(f32) * jax.nn.sigmoid(
                acc[:, 3 * ch :].astype(bf16).astype(f32)
            )
            acc[:, : 2 * ch] = acc[:, : 2 * ch].astype(bf16).astype(f32)
            s_at, l_at = HALO - SHORT + 1, HALO - WIDE + 1
            read = sum(acc[s_at + i : s_at + i + rows, :ch] * ftaps[i : i + 1, :] for i in range(SHORT))
            read = jax.nn.silu(read).astype(bf16)
            read16[...] = read
            zgate[...] = jax.nn.silu(acc[HALO:, ch : 2 * ch])
            scores = dot(read, w16[...], 1, 1)
            lower = lax.broadcasted_iota(jnp.int32, (rows, rows), 0) >= lax.broadcasted_iota(jnp.int32, (rows, rows), 1)
            lane = lax.broadcasted_iota(jnp.int32, (rows, ch), 1)
            y = jnp.zeros((rows, ch), f32)
            for h in range(heads):
                gap = jnp.where(lower, cum[:, h * p : h * p + 1] - cum_t[h : h + 1, :], 0.0)
                m = jnp.where(lower, jnp.exp(gap) * scores, 0.0).astype(bf16)
                x = jnp.where(lane // p == h, xs[...].astype(f32), 0.0).astype(bf16)
                y = y + dot(m, x, 1, 0)
            inner[...] = y
            for r in range(0, rows, part):
                mixed[r : r + part, :] = sum(
                    glu[l_at + r + i : l_at + r + i + part, :] * ltaps[i : i + 1, :] for i in range(WIDE)
                )

    small = (ftaps, ltaps, xs, w16, cum, cum_t)
    return pl.pallas_call(
        body,
        grid=(steps,),
        out_shape=(
            pltpu.VMEM((rows, STATE), bf16), pltpu.VMEM((rows, ch), f32), pltpu.VMEM((rows, ch), f32),
            pltpu.VMEM((rows, ch), f32), pltpu.VMEM((d, 2 * ch), bf16),
        ),
        in_specs=[VMEM, pl.BlockSpec((kb, 6 * ch), lambda k: (k, 0)), *[VMEM] * len(small)],
        out_specs=(VMEM,) * 5,
        scratch_shapes=[pltpu.VMEM((ext, 4 * ch), f32), pltpu.VMEM((ext, ch), f32)],
        compiler_params=SMALL, name="rows_local",
    )(*held(normed), *fetched(rest), *held(*small))


def rows_done(got, enter, before, init, index, read16, zgate, mixed, inner, cum, gain, copies):
    rows, ch = mixed.shape
    n, _, _ = got.shape
    heads = init.shape[0]
    p = ch // heads

    def body(at, got, enter, before, init, read16, zgate, mixed, inner, cum, gain, sums, pre):
        acc_in = jnp.zeros((1, STATE), f32)
        start = enter[...]
        b = before[0:1, :]
        for j in reversed(range(n)):
            logs = jnp.sum(got[j, ch:, :].astype(f32), axis=0, keepdims=True)
            inside = (j < at[0]).astype(f32)
            start = start + got[j, :ch, :].astype(f32) * spread_heads(inside * jnp.exp(acc_in + b), heads, p)
            acc_in = acc_in + inside * logs
        start = start + init[...].reshape(ch, STATE) * spread_heads(jnp.exp(acc_in + b), heads, p)
        y = inner[...] + dot(read16[...], start.astype(bf16), 1, 1) * jnp.exp(cum[...])
        gated = y * zgate[...]
        mix = mixed[...]
        squares = jnp.concatenate([mix, mix * mix, gated * gated], 1)
        pick = lax.broadcasted_iota(jnp.int32, (8, 3 * ch), 1) // ch == lax.broadcasted_iota(jnp.int32, (8, 3 * ch), 0)
        found = dot(jnp.where(pick, 1.0, 0.0), squares, 1, 1, HIGHEST)
        for j in range(copies):
            sums[j] = found[:3]
        pre[:, :ch] = mix.astype(bf16)
        pre[:, ch:] = (gated * gain[...]).astype(bf16)

    return pl.pallas_call(
        body,
        out_shape=(sds((copies, 3, rows), f32), pltpu.VMEM((rows, 2 * ch), bf16)),
        in_specs=[SMEM, *[VMEM] * 10],
        out_specs=(VMEM, VMEM),
        compiler_params=SMALL, name="rows_done",
    )(index, *held(got, enter, before, init, read16, zgate, mixed, inner, cum, gain))


def output_rows(sums, both, gains, own, other, index, nf, nt):
    copies, _, rows = sums.shape
    ch = gains.shape[1]
    d = own.shape[0]
    piece = rows // (nf * nt)

    def body(at, sref, bref, gref, wa, wb, out, cols, act):
        tp = at[0]
        s = sref[0]
        for j in range(1, copies):
            s = s + sref[j]
        cols[...] = jnp.transpose(jnp.concatenate([s, jnp.zeros((5, rows), f32)], 0))
        for i in range(nf):
            at_row = pl.multiple_of(i * (nt * piece) + tp * piece, piece)
            here = slice(i * piece, (i + 1) * piece)
            t = cols[pl.ds(at_row, piece), :]
            mean = t[:, 0:1] / C_CH
            rstd = lax.rsqrt(t[:, 1:2] / C_CH - mean * mean + EPS)
            scale = lax.rsqrt(t[:, 2:3] / D_INNER + EPS)
            for j in range(nt):
                src = tp if j == 0 else 1 - tp
                a = bref[pl.ds(pl.multiple_of(src * rows + at_row, piece), piece), :].astype(f32)
                conv = jax.nn.silu((a[:, :ch] - mean) * rstd * gref[pl.ds(src, 1), :])
                act[here, 2 * j * ch : (2 * j + 1) * ch] = conv.astype(bf16)
                act[here, (2 * j + 1) * ch : (2 * j + 2) * ch] = (a[:, ch:] * scale).astype(bf16)
        term = dot(act[:, : 2 * ch], wa[...], 1, 1) + dot(act[:, 2 * ch :], wb[...], 1, 1)
        out[...] = term.astype(bf16).reshape(nf, piece, d)

    return pl.pallas_call(
        body,
        out_shape=sds((nf, piece, d), bf16),
        in_specs=[SMEM, *[VMEM] * 5],
        out_specs=VMEM,
        scratch_shapes=[pltpu.VMEM((rows, 8), f32), pltpu.VMEM((nf * piece, 4 * ch), bf16)],
        compiler_params=SMALL, name="output_rows",
    )(index, *held(sums, both, gains, own, other))


def per_device(
    tokens, norm_gain, conv_value, conv_gate, mixer_gate, state_input, write_projection, state_read,
    step_proj, step_bias, decay_log, decay_extra, input_taps, write_taps, fetch_taps, long_taps,
    conv_gain, state_gain, conv_output, state_output, initial_state,
):
    rows = tokens.shape[0]
    ch = conv_value.shape[1]
    heads = step_bias.shape[0]
    p = ch // heads
    nf, nt = lax.axis_size("fs"), lax.axis_size("tp")
    iz, iy, tp = (lax.axis_index(a).astype(jnp.int32).reshape(1) for a in ("sp_0", "sp_1", "tp"))
    ny = lax.axis_size("sp_1")
    rest = lay_out((state_read, mixer_gate, conv_value, conv_gate, conv_output, state_output), 1)
    rest = lax.all_gather(rest[0], SP, axis=0, tiled=True)
    first = lay_out((state_input, write_projection), lax.axis_size("sp_0"))
    first = lax.all_to_all(first, "sp_0", 0, 0, tiled=True)
    first = copies_of(first, ny)
    first = lax.all_to_all(first, "sp_1", 0, 0, tiled=True)
    n = lax.axis_size(SP)
    halo = lax.ppermute(tokens[rows - HALO :], SP, [(i, i + 1) for i in range(n - 1)])
    v = jnp.concatenate([halo, tokens], 0).astype(f32)
    normed = (v * lax.rsqrt(jnp.mean(v * v, axis=1, keepdims=True) + EPS) * norm_gain).astype(bf16)
    step_all = jnp.dot(normed[HALO:], step_proj, preferred_element_type=f32)
    me = lax.axis_index("fs") * nt + lax.axis_index("tp")
    step = jax.nn.softplus(lax.dynamic_slice_in_dim(step_all, me * heads, heads, 1) + step_bias)
    log_step = (-jnp.exp(decay_log) * step + decay_extra.T).T
    cum_t = jnp.cumsum(log_step, axis=1)
    total = cum_t[:, -1]
    cum = jnp.repeat(cum_t.T, p, axis=1)
    step = jnp.repeat(step, p, axis=1)
    left = jnp.repeat(jnp.exp(total[:, None] - cum_t).T, p, axis=1)
    total = jnp.pad(total[None], ((0, 0), (0, STATE - heads)))
    gains = lax.all_gather(conv_gain, "tp")
    taps = jnp.concatenate([input_taps, write_taps], 1)
    send, xs, w16 = local_states(normed, first, taps, step, left, total, ny)
    got = lax.all_to_all(send, "sp_1", 0, 0, tiled=True)
    enter, before, send = line_states(got, iy, heads, p, lax.axis_size("sp_0"))
    got = lax.all_to_all(send, "sp_0", 0, 0, tiled=True)
    read16, zgate, mixed, inner, back = rows_local(normed, rest, fetch_taps, long_taps, xs, w16, cum, cum_t)
    back_other = lax.ppermute(back, "tp", [(i, nt - 1 - i) for i in range(nt)])
    sums, pre = rows_done(
        got, enter, before, initial_state, iz, read16, zgate, mixed, inner, cum, state_gain[None], nf * nt
    )
    sums = lax.all_to_all(sums, FT, 0, 0, tiled=True)
    both = lax.all_gather(pre, "tp", axis=0, tiled=True)
    out = output_rows(sums, both, gains, back, back_other, tp, nf, nt)
    pieces = lax.all_to_all(out, "fs", 0, 0, tiled=True)
    return jnp.sum(pieces.astype(f32), 0).astype(bf16)


def solution(mesh):
    torus = Mesh(
        mesh.devices.reshape(8, 8, mesh.shape["fs"], mesh.shape["tp"]), ("sp_0", "sp_1", "fs", "tp")
    )
    w = P(SP, FT)
    in_specs = (
        P(SP, None), P(), w, w, w, w, w, w, P(), P(FT), P(FT), P(FT, SP), P(None, FT), P(None, FT), P(None, FT),
        P(None, FT), P(FT), P(FT), w, w, P(FT, None, None),
    )

    return jax.shard_map(per_device, mesh=torus, in_specs=in_specs, out_specs=P((*SP, *FT), None), check_vma=False)
```

```python
import jax
import jax.numpy as jnp
from jax import lax
from jax.experimental import pallas as pl
from jax.experimental.pallas import tpu as pltpu
from jax.sharding import Mesh
from jax.sharding import PartitionSpec as P


C_CH = 1024
STATE = 128
D_INNER = 1024
WIDE = 31
SHORT = 4
HALO = 32
EPS = 1e-06
LOGS = 16
SP = ("sp_0", "sp_1")
FT = ("fs", "tp")
f32 = jnp.float32
bf16 = jnp.bfloat16
VMEM = pl.BlockSpec(memory_space=pltpu.VMEM)
SMEM = pl.BlockSpec(memory_space=pltpu.SMEM)
HIGHEST = lax.Precision.HIGHEST
SMALL = pltpu.CompilerParams(vmem_limit_bytes=12 * 2**20)


def dot(a, b, ca, cb, precision=None):
    return lax.dot_general(a, b, (((ca,), (cb,)), ((), ())), precision=precision, preferred_element_type=f32)


def sds(shape, dtype):
    return jax.ShapeDtypeStruct(shape, dtype)


def held(*arrays):
    return tuple(pltpu.with_memory_space_constraint(a, pltpu.VMEM) for a in arrays)


def fetched(*arrays):
    return tuple(pltpu.with_memory_space_constraint(a, pltpu.HBM) for a in arrays)


def lay_out(shards, copies):
    rows, ch = shards[0].shape
    n = len(shards)

    def body(*refs):
        for i in range(n):
            w = refs[i][...]
            for k in range(copies):
                refs[n][k, :, i * ch : (i + 1) * ch] = w

    return pl.pallas_call(
        body, out_shape=sds((copies, rows, n * ch), bf16), in_specs=[VMEM] * n, out_specs=VMEM, compiler_params=SMALL
    )(*fetched(*shards))


def log_rows(logs):
    hi = logs.astype(bf16).astype(f32)
    mid = (logs - hi).astype(bf16).astype(f32)
    lo = logs - hi - mid
    row = lax.broadcasted_iota(jnp.int32, (LOGS, STATE), 0)
    return jnp.where(row == 0, hi, jnp.where(row == 1, mid, jnp.where(row == 2, lo, 0.0))).astype(bf16)


def local_states(normed, first, taps, step, left, total, copies):
    ext, _ = normed.shape
    rows, ch = step.shape

    def body(nref, wref, tref, sref, lref, logs, send, xs, w16, buf):
        buf[...] = dot(nref[...], wref[...], 1, 0).astype(bf16).astype(f32)
        at = HALO - SHORT + 1
        mix = sum(buf[at + i : at + i + rows, :] * tref[i : i + 1, :] for i in range(SHORT))
        act = jax.nn.silu(mix)
        x = act[:, :ch] * sref[...]
        w = act[:, ch:].astype(bf16)
        xs[...] = x.astype(bf16)
        w16[...] = w
        ends = dot((x * lref[...]).astype(bf16), w, 0, 0).astype(bf16)
        tail = log_rows(logs[...])
        for k in range(copies):
            send[k, :ch, :] = ends
            send[k, ch:, :] = tail

    return pl.pallas_call(
        body,
        out_shape=(sds((copies, ch + LOGS, STATE), bf16), pltpu.VMEM((rows, ch), bf16), pltpu.VMEM((rows, STATE), bf16)),
        in_specs=[VMEM] * 6,
        out_specs=(VMEM,) * 3,
        scratch_shapes=[pltpu.VMEM((ext, 2 * ch), f32)],
        compiler_params=SMALL, name="local_states",
    )(*held(normed, first, taps, step, left, total))


def spread_heads(c, heads, p):
    return jnp.concatenate([jnp.broadcast_to(c[:, h : h + 1], (p, STATE)) for h in range(heads)], 0)


def line_states(got, index, heads, p, copies):
    n, size, _ = got.shape
    ch = heads * p

    def body(at, ref, enter, before, send):
        zero = jnp.zeros((1, STATE), f32)
        acc_in, acc_all = zero, zero
        ent = jnp.zeros((ch, STATE), f32)
        tot = jnp.zeros((ch, STATE), f32)
        for k in reversed(range(n)):
            logs = jnp.sum(ref[k, ch:, :].astype(f32), axis=0, keepdims=True)
            inside = (k < at[0]).astype(f32)
            piece = ref[k, :ch, :].astype(f32)
            ent = ent + piece * spread_heads(inside * jnp.exp(acc_in), heads, p)
            tot = tot + piece * spread_heads(jnp.exp(acc_all), heads, p)
            acc_in = acc_in + inside * logs
            acc_all = acc_all + logs
        enter[...] = ent
        before[...] = jnp.broadcast_to(acc_in, (8, STATE))
        line, tail = tot.astype(bf16), log_rows(acc_all)
        for k in range(copies):
            send[k, :ch, :] = line
            send[k, ch:, :] = tail

    return pl.pallas_call(
        body,
        out_shape=(pltpu.VMEM((ch, STATE), f32), pltpu.VMEM((8, STATE), f32), sds((copies, size, STATE), bf16)),
        in_specs=[SMEM, VMEM],
        out_specs=(VMEM,) * 3,
        compiler_params=SMALL, name="line_states",
    )(index, *held(got))


def rows_local(normed, rest, ftaps, ltaps, xs, w16, cum, cum_t):
    ext, d = normed.shape
    rows, ch = xs.shape
    heads = cum_t.shape[0]
    p = ch // heads
    steps = 4
    kb = d // steps
    part = 64

    def body(nref, wref, ftaps, ltaps, xs, w16, cum, cum_t, read16, zgate, mixed, inner, back, acc, glu):
        k = pl.program_id(0)
        at_k = pl.ds(pl.multiple_of(k * kb, kb), kb)
        term = dot(nref[:, at_k], wref[:, : 4 * ch], 1, 0)
        back[at_k, :] = wref[:, 4 * ch :]

        @pl.when(k == 0)
        def _():
            acc[...] = term

        @pl.when(k > 0)
        def _():
            acc[...] += term

        @pl.when(k == steps - 1)
        def _():
            glu[...] = acc[:, 2 * ch : 3 * ch].astype(bf16).astype(f32) * jax.nn.sigmoid(
                acc[:, 3 * ch :].astype(bf16).astype(f32)
            )
            acc[:, : 2 * ch] = acc[:, : 2 * ch].astype(bf16).astype(f32)
            s_at, l_at = HALO - SHORT + 1, HALO - WIDE + 1
            read = sum(acc[s_at + i : s_at + i + rows, :ch] * ftaps[i : i + 1, :] for i in range(SHORT))
            read = jax.nn.silu(read).astype(bf16)
            read16[...] = read
            zgate[...] = jax.nn.silu(acc[HALO:, ch : 2 * ch])
            scores = dot(read, w16[...], 1, 1)
            lower = lax.broadcasted_iota(jnp.int32, (rows, rows), 0) >= lax.broadcasted_iota(jnp.int32, (rows, rows), 1)
            lane = lax.broadcasted_iota(jnp.int32, (rows, ch), 1)
            y = jnp.zeros((rows, ch), f32)
            for h in range(heads):
                gap = jnp.where(lower, cum[:, h * p : h * p + 1] - cum_t[h : h + 1, :], 0.0)
                m = jnp.where(lower, jnp.exp(gap) * scores, 0.0).astype(bf16)
                x = jnp.where(lane // p == h, xs[...].astype(f32), 0.0).astype(bf16)
                y = y + dot(m, x, 1, 0)
            inner[...] = y
            for r in range(0, rows, part):
                mixed[r : r + part, :] = sum(
                    glu[l_at + r + i : l_at + r + i + part, :] * ltaps[i : i + 1, :] for i in range(WIDE)
                )

    small = (ftaps, ltaps, xs, w16, cum, cum_t)
    return pl.pallas_call(
        body,
        grid=(steps,),
        out_shape=(
            pltpu.VMEM((rows, STATE), bf16), pltpu.VMEM((rows, ch), f32), pltpu.VMEM((rows, ch), f32),
            pltpu.VMEM((rows, ch), f32), pltpu.VMEM((d, 2 * ch), bf16),
        ),
        in_specs=[VMEM, pl.BlockSpec((kb, 6 * ch), lambda k: (k, 0)), *[VMEM] * len(small)],
        out_specs=(VMEM,) * 5,
        scratch_shapes=[pltpu.VMEM((ext, 4 * ch), f32), pltpu.VMEM((ext, ch), f32)],
        compiler_params=SMALL, name="rows_local",
    )(*held(normed), *fetched(rest), *held(*small))


def rows_done(got, enter, before, init, index, read16, zgate, mixed, inner, cum, gain, copies):
    rows, ch = mixed.shape
    n, _, _ = got.shape
    heads = init.shape[0]
    p = ch // heads

    def body(at, got, enter, before, init, read16, zgate, mixed, inner, cum, gain, sums, pre):
        acc_in = jnp.zeros((1, STATE), f32)
        start = enter[...]
        b = before[0:1, :]
        for j in reversed(range(n)):
            logs = jnp.sum(got[j, ch:, :].astype(f32), axis=0, keepdims=True)
            inside = (j < at[0]).astype(f32)
            start = start + got[j, :ch, :].astype(f32) * spread_heads(inside * jnp.exp(acc_in + b), heads, p)
            acc_in = acc_in + inside * logs
        start = start + init[...].reshape(ch, STATE) * spread_heads(jnp.exp(acc_in + b), heads, p)
        y = inner[...] + dot(read16[...], start.astype(bf16), 1, 1) * jnp.exp(cum[...])
        gated = y * zgate[...]
        mix = mixed[...]
        squares = jnp.concatenate([mix, mix * mix, gated * gated], 1)
        pick = lax.broadcasted_iota(jnp.int32, (8, 3 * ch), 1) // ch == lax.broadcasted_iota(jnp.int32, (8, 3 * ch), 0)
        found = dot(jnp.where(pick, 1.0, 0.0), squares, 1, 1, HIGHEST)
        for j in range(copies):
            sums[j] = found[:3]
        pre[:, :ch] = mix.astype(bf16)
        pre[:, ch:] = (gated * gain[...]).astype(bf16)

    return pl.pallas_call(
        body,
        out_shape=(sds((copies, 3, rows), f32), pltpu.VMEM((rows, 2 * ch), bf16)),
        in_specs=[SMEM, *[VMEM] * 10],
        out_specs=(VMEM, VMEM),
        compiler_params=SMALL, name="rows_done",
    )(index, *held(got, enter, before, init, read16, zgate, mixed, inner, cum, gain))


def output_rows(sums, both, gains, own, other, index, nf, nt):
    copies, _, rows = sums.shape
    ch = gains.shape[1]
    d = own.shape[0]
    piece = rows // (nf * nt)

    def body(at, sref, bref, gref, wa, wb, out, cols, act):
        tp = at[0]
        s = sref[0]
        for j in range(1, copies):
            s = s + sref[j]
        cols[...] = jnp.transpose(jnp.concatenate([s, jnp.zeros((5, rows), f32)], 0))
        for i in range(nf):
            at_row = pl.multiple_of(i * (nt * piece) + tp * piece, piece)
            here = slice(i * piece, (i + 1) * piece)
            t = cols[pl.ds(at_row, piece), :]
            mean = t[:, 0:1] / C_CH
            rstd = lax.rsqrt(t[:, 1:2] / C_CH - mean * mean + EPS)
            scale = lax.rsqrt(t[:, 2:3] / D_INNER + EPS)
            for j in range(nt):
                src = tp if j == 0 else 1 - tp
                a = bref[pl.ds(pl.multiple_of(src * rows + at_row, piece), piece), :].astype(f32)
                conv = jax.nn.silu((a[:, :ch] - mean) * rstd * gref[pl.ds(src, 1), :])
                act[here, 2 * j * ch : (2 * j + 1) * ch] = conv.astype(bf16)
                act[here, (2 * j + 1) * ch : (2 * j + 2) * ch] = (a[:, ch:] * scale).astype(bf16)
        term = dot(act[:, : 2 * ch], wa[...], 1, 1) + dot(act[:, 2 * ch :], wb[...], 1, 1)
        out[...] = term.astype(bf16).reshape(nf, piece, d)

    return pl.pallas_call(
        body,
        out_shape=sds((nf, piece, d), bf16),
        in_specs=[SMEM, *[VMEM] * 5],
        out_specs=VMEM,
        scratch_shapes=[pltpu.VMEM((rows, 8), f32), pltpu.VMEM((nf * piece, 4 * ch), bf16)],
        compiler_params=SMALL, name="output_rows",
    )(index, *held(sums, both, gains, own, other))


def per_device(
    tokens, norm_gain, conv_value, conv_gate, mixer_gate, state_input, write_projection, state_read,
    step_proj, step_bias, decay_log, decay_extra, input_taps, write_taps, fetch_taps, long_taps,
    conv_gain, state_gain, conv_output, state_output, initial_state,
):
    rows = tokens.shape[0]
    ch = conv_value.shape[1]
    heads = step_bias.shape[0]
    p = ch // heads
    nf, nt = lax.axis_size("fs"), lax.axis_size("tp")
    iz, iy, tp = (lax.axis_index(a).astype(jnp.int32).reshape(1) for a in ("sp_0", "sp_1", "tp"))
    ny = lax.axis_size("sp_1")
    rest = lay_out((state_read, mixer_gate, conv_value, conv_gate, conv_output, state_output), ny)
    rest = lax.all_to_all(rest, "sp_1", 0, 0, tiled=True).reshape(-1, 6 * ch)
    rest = lax.all_gather(rest, "sp_0", axis=0, tiled=True)
    first = lay_out((state_input, write_projection), lax.axis_size(SP))
    first = lax.all_to_all(first, SP, 0, 0, tiled=True).reshape(-1, 2 * ch)
    n = lax.axis_size(SP)
    halo = lax.ppermute(tokens[rows - HALO :], SP, [(i, i + 1) for i in range(n - 1)])
    v = jnp.concatenate([halo, tokens], 0).astype(f32)
    normed = (v * lax.rsqrt(jnp.mean(v * v, axis=1, keepdims=True) + EPS) * norm_gain).astype(bf16)
    step_all = jnp.dot(normed[HALO:], step_proj, preferred_element_type=f32)
    me = lax.axis_index("fs") * nt + lax.axis_index("tp")
    step = jax.nn.softplus(lax.dynamic_slice_in_dim(step_all, me * heads, heads, 1) + step_bias)
    log_step = (-jnp.exp(decay_log) * step + decay_extra.T).T
    cum_t = jnp.cumsum(log_step, axis=1)
    total = cum_t[:, -1]
    cum = jnp.repeat(cum_t.T, p, axis=1)
    step = jnp.repeat(step, p, axis=1)
    left = jnp.repeat(jnp.exp(total[:, None] - cum_t).T, p, axis=1)
    total = jnp.pad(total[None], ((0, 0), (0, STATE - heads)))
    gains = lax.all_gather(conv_gain, "tp")
    taps = jnp.concatenate([input_taps, write_taps], 1)
    send, xs, w16 = local_states(normed, first, taps, step, left, total, ny)
    got = lax.all_to_all(send, "sp_1", 0, 0, tiled=True)
    enter, before, send = line_states(got, iy, heads, p, lax.axis_size("sp_0"))
    got = lax.all_to_all(send, "sp_0", 0, 0, tiled=True)
    read16, zgate, mixed, inner, back = rows_local(normed, rest, fetch_taps, long_taps, xs, w16, cum, cum_t)
    back_other = lax.ppermute(back, "tp", [(i, nt - 1 - i) for i in range(nt)])
    sums, pre = rows_done(
        got, enter, before, initial_state, iz, read16, zgate, mixed, inner, cum, state_gain[None], nf * nt
    )
    sums = lax.all_to_all(sums, FT, 0, 0, tiled=True)
    both = lax.all_gather(pre, "tp", axis=0, tiled=True)
    out = output_rows(sums, both, gains, back, back_other, tp, nf, nt)
    pieces = lax.all_to_all(out, "fs", 0, 0, tiled=True)
    return jnp.sum(pieces.astype(f32), 0).astype(bf16)


def solution(mesh):
    torus = Mesh(
        mesh.devices.reshape(8, 8, mesh.shape["fs"], mesh.shape["tp"]), ("sp_0", "sp_1", "fs", "tp")
    )
    w = P(SP, FT)
    in_specs = (
        P(SP, None), P(), w, w, w, w, w, w, P(), P(FT), P(FT), P(FT, SP), P(None, FT), P(None, FT), P(None, FT),
        P(None, FT), P(FT), P(FT), w, w, P(FT, None, None),
    )

    return jax.shard_map(per_device, mesh=torus, in_specs=in_specs, out_specs=P((*SP, *FT), None), check_vma=False)
```

```python
import jax
import jax.numpy as jnp
from jax import lax
from jax.experimental import pallas as pl
from jax.experimental.pallas import tpu as pltpu
from jax.sharding import Mesh
from jax.sharding import PartitionSpec as P


C_CH = 1024
STATE = 128
D_INNER = 1024
WIDE = 31
SHORT = 4
HALO = 32
EPS = 1e-06
LOGS = 8
SP = ("sp_0", "sp_1")
FT = ("fs", "tp")
f32 = jnp.float32
bf16 = jnp.bfloat16
VMEM = pl.BlockSpec(memory_space=pltpu.VMEM)
SMEM = pl.BlockSpec(memory_space=pltpu.SMEM)
HIGHEST = lax.Precision.HIGHEST
SMALL = pltpu.CompilerParams(vmem_limit_bytes=12 * 2**20)


def dot(a, b, ca, cb, precision=None):
    return lax.dot_general(a, b, (((ca,), (cb,)), ((), ())), precision=precision, preferred_element_type=f32)


def sds(shape, dtype):
    return jax.ShapeDtypeStruct(shape, dtype)


def held(*arrays):
    return tuple(pltpu.with_memory_space_constraint(a, pltpu.VMEM) for a in arrays)


def fetched(*arrays):
    return tuple(pltpu.with_memory_space_constraint(a, pltpu.HBM) for a in arrays)


def lay_out(shards, copies):
    rows, ch = shards[0].shape
    n = len(shards)

    def body(*refs):
        for i in range(n):
            w = refs[i][...]
            for k in range(copies):
                refs[n][k, :, i * ch : (i + 1) * ch] = w

    return pl.pallas_call(
        body, out_shape=sds((copies, rows, n * ch), bf16), in_specs=[VMEM] * n, out_specs=VMEM, compiler_params=SMALL
    )(*fetched(*shards))


def log_rows(logs):
    hi = logs.astype(bf16).astype(f32)
    mid = (logs - hi).astype(bf16).astype(f32)
    lo = logs - hi - mid
    row = lax.broadcasted_iota(jnp.int32, (LOGS, STATE), 0)
    return jnp.where(row == 0, hi, jnp.where(row == 1, mid, jnp.where(row == 2, lo, 0.0))).astype(bf16)


def local_states(normed, first, taps, step, left, total, copies):
    ext, _ = normed.shape
    rows, ch = step.shape

    def body(nref, wref, tref, sref, lref, logs, send, xs, w16, buf):
        buf[...] = dot(nref[...], wref[...], 1, 0).astype(bf16).astype(f32)
        at = HALO - SHORT + 1
        mix = sum(buf[at + i : at + i + rows, :] * tref[i : i + 1, :] for i in range(SHORT))
        act = jax.nn.silu(mix)
        x = act[:, :ch] * sref[...]
        w = act[:, ch:].astype(bf16)
        xs[...] = x.astype(bf16)
        w16[...] = w
        ends = dot((x * lref[...]).astype(bf16), w, 0, 0).astype(bf16)
        tail = log_rows(logs[...])
        for k in range(copies):
            send[k, :ch, :] = ends
            send[k, ch:, :] = tail

    return pl.pallas_call(
        body,
        out_shape=(sds((copies, ch + LOGS, STATE), bf16), pltpu.VMEM((rows, ch), bf16), pltpu.VMEM((rows, STATE), bf16)),
        in_specs=[VMEM] * 6,
        out_specs=(VMEM,) * 3,
        scratch_shapes=[pltpu.VMEM((ext, 2 * ch), f32)],
        compiler_params=SMALL, name="local_states",
    )(*held(normed, first, taps, step, left, total))


def spread_heads(c, heads, p):
    return jnp.concatenate([jnp.broadcast_to(c[:, h : h + 1], (p, STATE)) for h in range(heads)], 0)


def line_states(got, index, heads, p, copies):
    n, size, _ = got.shape
    ch = heads * p

    def body(at, ref, enter, before, send):
        zero = jnp.zeros((1, STATE), f32)
        acc_in, acc_all = zero, zero
        ent = jnp.zeros((ch, STATE), f32)
        tot = jnp.zeros((ch, STATE), f32)
        for k in reversed(range(n)):
            logs = jnp.sum(ref[k, ch:, :].astype(f32), axis=0, keepdims=True)
            inside = (k < at[0]).astype(f32)
            piece = ref[k, :ch, :].astype(f32)
            ent = ent + piece * spread_heads(inside * jnp.exp(acc_in), heads, p)
            tot = tot + piece * spread_heads(jnp.exp(acc_all), heads, p)
            acc_in = acc_in + inside * logs
            acc_all = acc_all + logs
        enter[...] = ent
        before[...] = jnp.broadcast_to(acc_in, (8, STATE))
        line, tail = tot.astype(bf16), log_rows(acc_all)
        for k in range(copies):
            send[k, :ch, :] = line
            send[k, ch:, :] = tail

    return pl.pallas_call(
        body,
        out_shape=(pltpu.VMEM((ch, STATE), f32), pltpu.VMEM((8, STATE), f32), sds((copies, size, STATE), bf16)),
        in_specs=[SMEM, VMEM],
        out_specs=(VMEM,) * 3,
        compiler_params=SMALL, name="line_states",
    )(index, *held(got))


def rows_local(normed, rest, ftaps, ltaps, xs, w16, cum, cum_t):
    ext, d = normed.shape
    rows, ch = xs.shape
    heads = cum_t.shape[0]
    p = ch // heads
    ny, nz, piece, _ = rest.shape
    part = 64

    def body(nref, wref, ftaps, ltaps, xs, w16, cum, cum_t, read16, zgate, mixed, inner, back, acc, glu, wall, sems):
        def copies(z, y):
            at = (z * ny + y) * piece
            return (
                pltpu.make_async_copy(wref.at[y, z, :, : 4 * ch], wall.at[at : at + piece, :], sems.at[z, y, 0]),
                pltpu.make_async_copy(wref.at[y, z, :, 4 * ch :], back.at[at : at + piece, :], sems.at[z, y, 1]),
            )

        for z in range(nz):
            for y in range(ny):
                copies(z, y)[0].start()
        for z in range(nz):
            for y in range(ny):
                copies(z, y)[1].start()
        for z in range(0, nz, 2):
            for y in range(ny):
                copies(z, y)[0].wait()
                copies(z + 1, y)[0].wait()
            here = slice(z * ny * piece, (z + 2) * ny * piece)
            term = dot(nref[:, here], wall[here, :], 1, 0)
            acc[...] = term if z == 0 else acc[...] + term
        glu[...] = acc[:, 2 * ch : 3 * ch].astype(bf16).astype(f32) * jax.nn.sigmoid(
            acc[:, 3 * ch :].astype(bf16).astype(f32)
        )
        acc[:, : 2 * ch] = acc[:, : 2 * ch].astype(bf16).astype(f32)
        s_at, l_at = HALO - SHORT + 1, HALO - WIDE + 1
        read = sum(acc[s_at + i : s_at + i + rows, :ch] * ftaps[i : i + 1, :] for i in range(SHORT))
        read = jax.nn.silu(read).astype(bf16)
        read16[...] = read
        zgate[...] = jax.nn.silu(acc[HALO:, ch : 2 * ch])
        scores = dot(read, w16[...], 1, 1)
        lower = lax.broadcasted_iota(jnp.int32, (rows, rows), 0) >= lax.broadcasted_iota(jnp.int32, (rows, rows), 1)
        lane = lax.broadcasted_iota(jnp.int32, (rows, ch), 1)
        out = jnp.zeros((rows, ch), f32)
        for h in range(heads):
            gap = jnp.where(lower, cum[:, h * p : h * p + 1] - cum_t[h : h + 1, :], 0.0)
            m = jnp.where(lower, jnp.exp(gap) * scores, 0.0).astype(bf16)
            x = jnp.where(lane // p == h, xs[...].astype(f32), 0.0).astype(bf16)
            out = out + dot(m, x, 1, 0)
        inner[...] = out
        for r in range(0, rows, part):
            mixed[r : r + part, :] = sum(
                glu[l_at + r + i : l_at + r + i + part, :] * ltaps[i : i + 1, :] for i in range(WIDE)
            )
        for z in range(nz):
            for y in range(ny):
                copies(z, y)[1].wait()

    small = (ftaps, ltaps, xs, w16, cum, cum_t)
    return pl.pallas_call(
        body,
        out_shape=(
            pltpu.VMEM((rows, STATE), bf16), pltpu.VMEM((rows, ch), f32), pltpu.VMEM((rows, ch), f32),
            pltpu.VMEM((rows, ch), f32), pltpu.VMEM((d, 2 * ch), bf16),
        ),
        in_specs=[VMEM, pl.BlockSpec(memory_space=pltpu.HBM), *[VMEM] * len(small)],
        out_specs=(VMEM,) * 5,
        scratch_shapes=[
            pltpu.VMEM((ext, 4 * ch), f32), pltpu.VMEM((ext, ch), f32), pltpu.VMEM((d, 4 * ch), bf16),
            pltpu.SemaphoreType.DMA((nz, ny, 2)),
        ],
        compiler_params=SMALL, name="rows_local",
    )(*held(normed), *fetched(rest), *held(*small))


def rows_done(got, enter, before, init, index, read16, zgate, mixed, inner, cum, gain, copies):
    rows, ch = mixed.shape
    n, _, _ = got.shape
    heads = init.shape[0]
    p = ch // heads

    def body(at, got, enter, before, init, read16, zgate, mixed, inner, cum, gain, sums, pre):
        acc_in = jnp.zeros((1, STATE), f32)
        start = enter[...]
        b = before[0:1, :]
        for j in reversed(range(n)):
            logs = jnp.sum(got[j, ch:, :].astype(f32), axis=0, keepdims=True)
            inside = (j < at[0]).astype(f32)
            start = start + got[j, :ch, :].astype(f32) * spread_heads(inside * jnp.exp(acc_in + b), heads, p)
            acc_in = acc_in + inside * logs
        start = start + init[...].reshape(ch, STATE) * spread_heads(jnp.exp(acc_in + b), heads, p)
        y = inner[...] + dot(read16[...], start.astype(bf16), 1, 1) * jnp.exp(cum[...])
        gated = y * zgate[...]
        mix = mixed[...]
        squares = jnp.concatenate([mix, mix * mix, gated * gated], 1)
        pick = lax.broadcasted_iota(jnp.int32, (8, 3 * ch), 1) // ch == lax.broadcasted_iota(jnp.int32, (8, 3 * ch), 0)
        found = dot(jnp.where(pick, 1.0, 0.0), squares, 1, 1, HIGHEST)
        for j in range(copies):
            sums[j] = found[:3]
        pre[:, :ch] = mix.astype(bf16)
        pre[:, ch:] = (gated * gain[...]).astype(bf16)

    return pl.pallas_call(
        body,
        out_shape=(sds((copies, 3, rows), f32), pltpu.VMEM((rows, 2 * ch), bf16)),
        in_specs=[SMEM, *[VMEM] * 10],
        out_specs=(VMEM, VMEM),
        compiler_params=SMALL, name="rows_done",
    )(index, *held(got, enter, before, init, read16, zgate, mixed, inner, cum, gain))


def output_rows(sums, both, gains, own, other, index, nf, nt):
    copies, _, rows = sums.shape
    ch = gains.shape[1]
    d = own.shape[0]
    piece = rows // (nf * nt)

    def body(at, sref, bref, gref, wa, wb, out, cols, act):
        tp = at[0]
        s = sref[0]
        for j in range(1, copies):
            s = s + sref[j]
        cols[...] = jnp.transpose(jnp.concatenate([s, jnp.zeros((5, rows), f32)], 0))
        for i in range(nf):
            at_row = pl.multiple_of(i * (nt * piece) + tp * piece, piece)
            here = slice(i * piece, (i + 1) * piece)
            t = cols[pl.ds(at_row, piece), :]
            mean = t[:, 0:1] / C_CH
            rstd = lax.rsqrt(t[:, 1:2] / C_CH - mean * mean + EPS)
            scale = lax.rsqrt(t[:, 2:3] / D_INNER + EPS)
            for j in range(nt):
                src = tp if j == 0 else 1 - tp
                a = bref[pl.ds(pl.multiple_of(src * rows + at_row, piece), piece), :].astype(f32)
                conv = jax.nn.silu((a[:, :ch] - mean) * rstd * gref[pl.ds(src, 1), :])
                act[here, 2 * j * ch : (2 * j + 1) * ch] = conv.astype(bf16)
                act[here, (2 * j + 1) * ch : (2 * j + 2) * ch] = (a[:, ch:] * scale).astype(bf16)
        term = dot(act[:, : 2 * ch], wa[...], 1, 1) + dot(act[:, 2 * ch :], wb[...], 1, 1)
        out[...] = term.astype(bf16).reshape(nf, piece, d)

    return pl.pallas_call(
        body,
        out_shape=sds((nf, piece, d), bf16),
        in_specs=[SMEM, *[VMEM] * 5],
        out_specs=VMEM,
        scratch_shapes=[pltpu.VMEM((rows, 8), f32), pltpu.VMEM((nf * piece, 4 * ch), bf16)],
        compiler_params=SMALL, name="output_rows",
    )(index, *held(sums, both, gains, own, other))


def per_device(
    tokens, norm_gain, conv_value, conv_gate, mixer_gate, state_input, write_projection, state_read,
    step_proj, step_bias, decay_log, decay_extra, input_taps, write_taps, fetch_taps, long_taps,
    conv_gain, state_gain, conv_output, state_output, initial_state,
):
    rows = tokens.shape[0]
    ch = conv_value.shape[1]
    heads = step_bias.shape[0]
    p = ch // heads
    nf, nt = lax.axis_size("fs"), lax.axis_size("tp")
    iz, iy, tp = (lax.axis_index(a).astype(jnp.int32).reshape(1) for a in ("sp_0", "sp_1", "tp"))
    ny = lax.axis_size("sp_1")
    rest = lay_out((state_read, mixer_gate, conv_value, conv_gate, conv_output, state_output), lax.axis_size("sp_0"))
    rest = lax.all_to_all(rest, "sp_0", 0, 0, tiled=True)
    rest = lax.all_gather(rest, "sp_1", axis=0)
    first = lay_out((state_input, write_projection), lax.axis_size(SP))
    first = lax.all_to_all(first, SP, 0, 0, tiled=True).reshape(-1, 2 * ch)
    n = lax.axis_size(SP)
    halo = lax.ppermute(tokens[rows - HALO :], SP, [(i, i + 1) for i in range(n - 1)])
    v = jnp.concatenate([halo, tokens], 0).astype(f32)
    normed = (v * lax.rsqrt(jnp.mean(v * v, axis=1, keepdims=True) + EPS) * norm_gain).astype(bf16)
    step_all = jnp.dot(normed[HALO:], step_proj, preferred_element_type=f32)
    me = lax.axis_index("fs") * nt + lax.axis_index("tp")
    step = jax.nn.softplus(lax.dynamic_slice_in_dim(step_all, me * heads, heads, 1) + step_bias)
    log_step = (-jnp.exp(decay_log) * step + decay_extra.T).T
    cum_t = jnp.cumsum(log_step, axis=1)
    total = cum_t[:, -1]
    cum = jnp.repeat(cum_t.T, p, axis=1)
    step = jnp.repeat(step, p, axis=1)
    left = jnp.repeat(jnp.exp(total[:, None] - cum_t).T, p, axis=1)
    total = jnp.pad(total[None], ((0, 0), (0, STATE - heads)))
    gains = lax.all_gather(conv_gain, "tp")
    taps = jnp.concatenate([input_taps, write_taps], 1)
    send, xs, w16 = local_states(normed, first, taps, step, left, total, ny)
    got = lax.all_to_all(send, "sp_1", 0, 0, tiled=True)
    enter, before, send = line_states(got, iy, heads, p, lax.axis_size("sp_0"))
    got = lax.all_to_all(send, "sp_0", 0, 0, tiled=True)
    read16, zgate, mixed, inner, back = rows_local(normed, rest, fetch_taps, long_taps, xs, w16, cum, cum_t)
    back_other = lax.ppermute(back, "tp", [(i, nt - 1 - i) for i in range(nt)])
    sums, pre = rows_done(
        got, enter, before, initial_state, iz, read16, zgate, mixed, inner, cum, state_gain[None], nf * nt
    )
    sums = lax.all_to_all(sums, FT, 0, 0, tiled=True)
    both = lax.all_gather(pre, "tp", axis=0, tiled=True)
    out = output_rows(sums, both, gains, back, back_other, tp, nf, nt)
    pieces = lax.all_to_all(out, "fs", 0, 0, tiled=True)
    return jnp.sum(pieces.astype(f32), 0).astype(bf16)


def solution(mesh):
    torus = Mesh(
        mesh.devices.reshape(8, 8, mesh.shape["fs"], mesh.shape["tp"]), ("sp_0", "sp_1", "fs", "tp")
    )
    w = P(SP, FT)
    in_specs = (
        P(SP, None), P(), w, w, w, w, w, w, P(), P(FT), P(FT), P(FT, SP), P(None, FT), P(None, FT), P(None, FT),
        P(None, FT), P(FT), P(FT), w, w, P(FT, None, None),
    )

    return jax.shard_map(per_device, mesh=torus, in_specs=in_specs, out_specs=P((*SP, *FT), None), check_vma=False)
```

```python
import jax
import jax.numpy as jnp
from jax import lax
from jax.experimental import pallas as pl
from jax.experimental.pallas import tpu as pltpu
from jax.sharding import Mesh
from jax.sharding import PartitionSpec as P


C_CH = 1024
STATE = 128
D_INNER = 1024
WIDE = 31
SHORT = 4
HALO = 32
EPS = 1e-06
LOGS = 8
SP = ("sp_0", "sp_1")
FT = ("fs", "tp")
f32 = jnp.float32
bf16 = jnp.bfloat16
VMEM = pl.BlockSpec(memory_space=pltpu.VMEM)
SMEM = pl.BlockSpec(memory_space=pltpu.SMEM)
HIGHEST = lax.Precision.HIGHEST
SMALL = pltpu.CompilerParams(vmem_limit_bytes=12 * 2**20)


def dot(a, b, ca, cb, precision=None):
    return lax.dot_general(a, b, (((ca,), (cb,)), ((), ())), precision=precision, preferred_element_type=f32)


def sds(shape, dtype):
    return jax.ShapeDtypeStruct(shape, dtype)


def held(*arrays):
    return tuple(pltpu.with_memory_space_constraint(a, pltpu.VMEM) for a in arrays)


def fetched(*arrays):
    return tuple(pltpu.with_memory_space_constraint(a, pltpu.HBM) for a in arrays)


def lay_out(shards, copies):
    rows, ch = shards[0].shape
    n = len(shards)

    def body(*refs):
        for i in range(n):
            w = refs[i][...]
            for k in range(copies):
                refs[n][k, :, i * ch : (i + 1) * ch] = w

    return pl.pallas_call(
        body, out_shape=sds((copies, rows, n * ch), bf16), in_specs=[VMEM] * n, out_specs=VMEM, compiler_params=SMALL
    )(*fetched(*shards))


def log_rows(logs):
    hi = logs.astype(bf16).astype(f32)
    mid = (logs - hi).astype(bf16).astype(f32)
    lo = logs - hi - mid
    row = lax.broadcasted_iota(jnp.int32, (LOGS, STATE), 0)
    return jnp.where(row == 0, hi, jnp.where(row == 1, mid, jnp.where(row == 2, lo, 0.0))).astype(bf16)


def local_states(normed, first, taps, step, left, total, copies):
    ext, _ = normed.shape
    rows, ch = step.shape

    def body(nref, wref, tref, sref, lref, logs, send, xs, w16, buf):
        buf[...] = dot(nref[...], wref[...], 1, 0).astype(bf16).astype(f32)
        at = HALO - SHORT + 1
        mix = sum(buf[at + i : at + i + rows, :] * tref[i : i + 1, :] for i in range(SHORT))
        act = jax.nn.silu(mix)
        x = act[:, :ch] * sref[...]
        w = act[:, ch:].astype(bf16)
        xs[...] = x.astype(bf16)
        w16[...] = w
        ends = dot((x * lref[...]).astype(bf16), w, 0, 0).astype(bf16)
        tail = log_rows(logs[...])
        for k in range(copies):
            send[k, :ch, :] = ends
            send[k, ch:, :] = tail

    return pl.pallas_call(
        body,
        out_shape=(sds((copies, ch + LOGS, STATE), bf16), pltpu.VMEM((rows, ch), bf16), pltpu.VMEM((rows, STATE), bf16)),
        in_specs=[VMEM] * 6,
        out_specs=(VMEM,) * 3,
        scratch_shapes=[pltpu.VMEM((ext, 2 * ch), f32)],
        compiler_params=SMALL, name="local_states",
    )(*held(normed, first, taps, step, left, total))


def spread_heads(c, heads, p):
    return jnp.concatenate([jnp.broadcast_to(c[:, h : h + 1], (p, STATE)) for h in range(heads)], 0)


def line_states(got, index, heads, p, copies):
    n, size, _ = got.shape
    ch = heads * p

    def body(at, ref, enter, before, send):
        zero = jnp.zeros((1, STATE), f32)
        acc_in, acc_all = zero, zero
        ent = jnp.zeros((ch, STATE), f32)
        tot = jnp.zeros((ch, STATE), f32)
        for k in reversed(range(n)):
            logs = jnp.sum(ref[k, ch:, :].astype(f32), axis=0, keepdims=True)
            inside = (k < at[0]).astype(f32)
            piece = ref[k, :ch, :].astype(f32)
            ent = ent + piece * spread_heads(inside * jnp.exp(acc_in), heads, p)
            tot = tot + piece * spread_heads(jnp.exp(acc_all), heads, p)
            acc_in = acc_in + inside * logs
            acc_all = acc_all + logs
        enter[...] = ent
        before[...] = jnp.broadcast_to(acc_in, (8, STATE))
        line, tail = tot.astype(bf16), log_rows(acc_all)
        for k in range(copies):
            send[k, :ch, :] = line
            send[k, ch:, :] = tail

    return pl.pallas_call(
        body,
        out_shape=(pltpu.VMEM((ch, STATE), f32), pltpu.VMEM((8, STATE), f32), sds((copies, size, STATE), bf16)),
        in_specs=[SMEM, VMEM],
        out_specs=(VMEM,) * 3,
        compiler_params=SMALL, name="line_states",
    )(index, *held(got))


def rows_local(normed, rest, ftaps, ltaps, xs, w16, cum, cum_t):
    ext, d = normed.shape
    rows, ch = xs.shape
    heads = cum_t.shape[0]
    p = ch // heads
    part, n = 64, 8
    kc = d // n

    def body(nref, wref, ftaps, ltaps, xs, w16, cum, cum_t, read16, zgate, mixed, inner, back, acc, glu, wall, sems):
        def fetch(i):
            at = slice(i * kc, (i + 1) * kc)
            return pltpu.make_async_copy(wref.at[at, : 4 * ch], wall.at[at, :], sems.at[0, i])

        def fetch_back(i):
            at = slice(i * kc, (i + 1) * kc)
            return pltpu.make_async_copy(wref.at[at, 4 * ch :], back.at[at, :], sems.at[1, i])

        for i in range(n):
            fetch(i).start()
        for i in range(n):
            fetch_back(i).start()
        for i in range(n):
            fetch(i).wait()
            at = slice(i * kc, (i + 1) * kc)
            term = dot(nref[:, at], wall[at, :], 1, 0)
            acc[...] = term if i == 0 else acc[...] + term
        glu[...] = acc[:, 2 * ch : 3 * ch].astype(bf16).astype(f32) * jax.nn.sigmoid(
            acc[:, 3 * ch :].astype(bf16).astype(f32)
        )
        acc[:, : 2 * ch] = acc[:, : 2 * ch].astype(bf16).astype(f32)
        s_at, l_at = HALO - SHORT + 1, HALO - WIDE + 1
        read = sum(acc[s_at + i : s_at + i + rows, :ch] * ftaps[i : i + 1, :] for i in range(SHORT))
        read = jax.nn.silu(read).astype(bf16)
        read16[...] = read
        zgate[...] = jax.nn.silu(acc[HALO:, ch : 2 * ch])
        scores = dot(read, w16[...], 1, 1)
        lower = lax.broadcasted_iota(jnp.int32, (rows, rows), 0) >= lax.broadcasted_iota(jnp.int32, (rows, rows), 1)
        lane = lax.broadcasted_iota(jnp.int32, (rows, ch), 1)
        y = jnp.zeros((rows, ch), f32)
        for h in range(heads):
            gap = jnp.where(lower, cum[:, h * p : h * p + 1] - cum_t[h : h + 1, :], 0.0)
            m = jnp.where(lower, jnp.exp(gap) * scores, 0.0).astype(bf16)
            x = jnp.where(lane // p == h, xs[...].astype(f32), 0.0).astype(bf16)
            y = y + dot(m, x, 1, 0)
        inner[...] = y
        for r in range(0, rows, part):
            mixed[r : r + part, :] = sum(
                glu[l_at + r + i : l_at + r + i + part, :] * ltaps[i : i + 1, :] for i in range(WIDE)
            )
        for i in range(n):
            fetch_back(i).wait()

    small = (ftaps, ltaps, xs, w16, cum, cum_t)
    return pl.pallas_call(
        body,
        out_shape=(
            pltpu.VMEM((rows, STATE), bf16), pltpu.VMEM((rows, ch), f32), pltpu.VMEM((rows, ch), f32),
            pltpu.VMEM((rows, ch), f32), pltpu.VMEM((d, 2 * ch), bf16),
        ),
        in_specs=[VMEM, pl.BlockSpec(memory_space=pltpu.HBM), *[VMEM] * len(small)],
        out_specs=(VMEM,) * 5,
        scratch_shapes=[
            pltpu.VMEM((ext, 4 * ch), f32), pltpu.VMEM((ext, ch), f32), pltpu.VMEM((d, 4 * ch), bf16),
            pltpu.SemaphoreType.DMA((2, n)),
        ],
        compiler_params=SMALL, name="rows_local",
    )(*held(normed), *fetched(rest), *held(*small))


def rows_done(got, enter, before, init, index, read16, zgate, mixed, inner, cum, gain, copies):
    rows, ch = mixed.shape
    n, _, _ = got.shape
    heads = init.shape[0]
    p = ch // heads

    def body(at, got, enter, before, init, read16, zgate, mixed, inner, cum, gain, sums, pre):
        acc_in = jnp.zeros((1, STATE), f32)
        start = enter[...]
        b = before[0:1, :]
        for j in reversed(range(n)):
            logs = jnp.sum(got[j, ch:, :].astype(f32), axis=0, keepdims=True)
            inside = (j < at[0]).astype(f32)
            start = start + got[j, :ch, :].astype(f32) * spread_heads(inside * jnp.exp(acc_in + b), heads, p)
            acc_in = acc_in + inside * logs
        start = start + init[...].reshape(ch, STATE) * spread_heads(jnp.exp(acc_in + b), heads, p)
        y = inner[...] + dot(read16[...], start.astype(bf16), 1, 1) * jnp.exp(cum[...])
        gated = y * zgate[...]
        mix = mixed[...]
        squares = jnp.concatenate([mix, mix * mix, gated * gated], 1)
        pick = lax.broadcasted_iota(jnp.int32, (8, 3 * ch), 1) // ch == lax.broadcasted_iota(jnp.int32, (8, 3 * ch), 0)
        found = dot(jnp.where(pick, 1.0, 0.0), squares, 1, 1, HIGHEST)
        for j in range(copies):
            sums[j] = found[:3]
        pre[:, :ch] = mix.astype(bf16)
        pre[:, ch:] = (gated * gain[...]).astype(bf16)

    return pl.pallas_call(
        body,
        out_shape=(sds((copies, 3, rows), f32), pltpu.VMEM((rows, 2 * ch), bf16)),
        in_specs=[SMEM, *[VMEM] * 10],
        out_specs=(VMEM, VMEM),
        compiler_params=SMALL, name="rows_done",
    )(index, *held(got, enter, before, init, read16, zgate, mixed, inner, cum, gain))


def output_rows(sums, both, gains, own, other, index, nf, nt):
    copies, _, rows = sums.shape
    ch = gains.shape[1]
    d = own.shape[0]
    piece = rows // (nf * nt)

    def body(at, sref, bref, gref, wa, wb, out, cols, act):
        tp = at[0]
        s = sref[0]
        for j in range(1, copies):
            s = s + sref[j]
        cols[...] = jnp.transpose(jnp.concatenate([s, jnp.zeros((5, rows), f32)], 0))
        for i in range(nf):
            at_row = pl.multiple_of(i * (nt * piece) + tp * piece, piece)
            here = slice(i * piece, (i + 1) * piece)
            t = cols[pl.ds(at_row, piece), :]
            mean = t[:, 0:1] / C_CH
            rstd = lax.rsqrt(t[:, 1:2] / C_CH - mean * mean + EPS)
            scale = lax.rsqrt(t[:, 2:3] / D_INNER + EPS)
            for j in range(nt):
                src = tp if j == 0 else 1 - tp
                a = bref[pl.ds(pl.multiple_of(src * rows + at_row, piece), piece), :].astype(f32)
                conv = jax.nn.silu((a[:, :ch] - mean) * rstd * gref[pl.ds(src, 1), :])
                act[here, 2 * j * ch : (2 * j + 1) * ch] = conv.astype(bf16)
                act[here, (2 * j + 1) * ch : (2 * j + 2) * ch] = (a[:, ch:] * scale).astype(bf16)
        term = dot(act[:, : 2 * ch], wa[...], 1, 1) + dot(act[:, 2 * ch :], wb[...], 1, 1)
        out[...] = term.astype(bf16).reshape(nf, piece, d)

    return pl.pallas_call(
        body,
        out_shape=sds((nf, piece, d), bf16),
        in_specs=[SMEM, *[VMEM] * 5],
        out_specs=VMEM,
        scratch_shapes=[pltpu.VMEM((rows, 8), f32), pltpu.VMEM((nf * piece, 4 * ch), bf16)],
        compiler_params=SMALL, name="output_rows",
    )(index, *held(sums, both, gains, own, other))


def per_device(
    tokens, norm_gain, conv_value, conv_gate, mixer_gate, state_input, write_projection, state_read,
    step_proj, step_bias, decay_log, decay_extra, input_taps, write_taps, fetch_taps, long_taps,
    conv_gain, state_gain, conv_output, state_output, initial_state,
):
    rows = tokens.shape[0]
    ch = conv_value.shape[1]
    heads = step_bias.shape[0]
    p = ch // heads
    nf, nt = lax.axis_size("fs"), lax.axis_size("tp")
    iz, iy, tp = (lax.axis_index(a).astype(jnp.int32).reshape(1) for a in ("sp_0", "sp_1", "tp"))
    ny = lax.axis_size("sp_1")
    rest = lay_out((state_read, mixer_gate, conv_value, conv_gate, conv_output, state_output), ny)
    rest = lax.all_to_all(rest, "sp_1", 0, 0, tiled=True).reshape(-1, 6 * ch)
    rest = lax.all_gather(rest, "sp_0", axis=0, tiled=True)
    first = lay_out((state_input, write_projection), lax.axis_size(SP))
    first = lax.all_to_all(first, SP, 0, 0, tiled=True).reshape(-1, 2 * ch)
    n = lax.axis_size(SP)
    halo = lax.ppermute(tokens[rows - HALO :], SP, [(i, i + 1) for i in range(n - 1)])
    v = jnp.concatenate([halo, tokens], 0).astype(f32)
    normed = (v * lax.rsqrt(jnp.mean(v * v, axis=1, keepdims=True) + EPS) * norm_gain).astype(bf16)
    step_all = jnp.dot(normed[HALO:], step_proj, preferred_element_type=f32)
    me = lax.axis_index("fs") * nt + lax.axis_index("tp")
    step = jax.nn.softplus(lax.dynamic_slice_in_dim(step_all, me * heads, heads, 1) + step_bias)
    log_step = (-jnp.exp(decay_log) * step + decay_extra.T).T
    cum_t = jnp.cumsum(log_step, axis=1)
    total = cum_t[:, -1]
    cum = jnp.repeat(cum_t.T, p, axis=1)
    step = jnp.repeat(step, p, axis=1)
    left = jnp.repeat(jnp.exp(total[:, None] - cum_t).T, p, axis=1)
    total = jnp.pad(total[None], ((0, 0), (0, STATE - heads)))
    gains = lax.all_gather(conv_gain, "tp")
    taps = jnp.concatenate([input_taps, write_taps], 1)
    send, xs, w16 = local_states(normed, first, taps, step, left, total, ny)
    got = lax.all_to_all(send, "sp_1", 0, 0, tiled=True)
    enter, before, send = line_states(got, iy, heads, p, lax.axis_size("sp_0"))
    got = lax.all_to_all(send, "sp_0", 0, 0, tiled=True)
    read16, zgate, mixed, inner, back = rows_local(normed, rest, fetch_taps, long_taps, xs, w16, cum, cum_t)
    back_other = lax.ppermute(back, "tp", [(i, nt - 1 - i) for i in range(nt)])
    sums, pre = rows_done(
        got, enter, before, initial_state, iz, read16, zgate, mixed, inner, cum, state_gain[None], nf * nt
    )
    sums = lax.all_to_all(sums, FT, 0, 0, tiled=True)
    both = lax.all_gather(pre, "tp", axis=0, tiled=True)
    out = output_rows(sums, both, gains, back, back_other, tp, nf, nt)
    pieces = lax.all_to_all(out, "fs", 0, 0, tiled=True)
    return jnp.sum(pieces.astype(f32), 0).astype(bf16)


def solution(mesh):
    torus = Mesh(
        mesh.devices.reshape(8, 8, mesh.shape["fs"], mesh.shape["tp"]), ("sp_0", "sp_1", "fs", "tp")
    )
    w = P(SP, FT)
    in_specs = (
        P(SP, None), P(), w, w, w, w, w, w, P(), P(FT), P(FT), P(FT, SP), P(None, FT), P(None, FT), P(None, FT),
        P(None, FT), P(FT), P(FT), w, w, P(FT, None, None),
    )

    return jax.shard_map(per_device, mesh=torus, in_specs=in_specs, out_specs=P((*SP, *FT), None), check_vma=False)
```

```python
import jax
import jax.numpy as jnp
from jax import lax
from jax.experimental import pallas as pl
from jax.experimental.pallas import tpu as pltpu
from jax.sharding import Mesh
from jax.sharding import PartitionSpec as P


C_CH = 1024
STATE = 128
D_INNER = 1024
WIDE = 31
SHORT = 4
HALO = 32
EPS = 1e-06
LOGS = 8
SP = ("sp_0", "sp_1")
FT = ("fs", "tp")
f32 = jnp.float32
bf16 = jnp.bfloat16
VMEM = pl.BlockSpec(memory_space=pltpu.VMEM)
SMEM = pl.BlockSpec(memory_space=pltpu.SMEM)
HIGHEST = lax.Precision.HIGHEST
SMALL = pltpu.CompilerParams(vmem_limit_bytes=12 * 2**20)


def dot(a, b, ca, cb, precision=None):
    return lax.dot_general(a, b, (((ca,), (cb,)), ((), ())), precision=precision, preferred_element_type=f32)


def sds(shape, dtype):
    return jax.ShapeDtypeStruct(shape, dtype)


def held(*arrays):
    return tuple(pltpu.with_memory_space_constraint(a, pltpu.VMEM) for a in arrays)


def fetched(*arrays):
    return tuple(pltpu.with_memory_space_constraint(a, pltpu.HBM) for a in arrays)


def lay_out(shards, copies):
    rows, ch = shards[0].shape
    n = len(shards)

    def body(*refs):
        for i in range(n):
            w = refs[i][...]
            for k in range(copies):
                refs[n][k, :, i * ch : (i + 1) * ch] = w

    return pl.pallas_call(
        body, out_shape=sds((copies, rows, n * ch), bf16), in_specs=[VMEM] * n, out_specs=VMEM, compiler_params=SMALL
    )(*fetched(*shards))


def copies_of(block, copies):
    def body(ref, out):
        for k in range(copies):
            out[k] = ref[...]

    return pl.pallas_call(
        body, out_shape=sds((copies, *block.shape), bf16), in_specs=[VMEM], out_specs=VMEM, compiler_params=SMALL
    )(*held(block))


def log_rows(logs):
    hi = logs.astype(bf16).astype(f32)
    mid = (logs - hi).astype(bf16).astype(f32)
    lo = logs - hi - mid
    row = lax.broadcasted_iota(jnp.int32, (LOGS, STATE), 0)
    return jnp.where(row == 0, hi, jnp.where(row == 1, mid, jnp.where(row == 2, lo, 0.0))).astype(bf16)


def local_states(normed, first, taps, step, left, total, copies):
    ext, _ = normed.shape
    rows, ch = step.shape

    def body(nref, wref, tref, sref, lref, logs, send, xs, w16, buf):
        buf[...] = dot(nref[...], wref[...], 1, 0).astype(bf16).astype(f32)
        at = HALO - SHORT + 1
        mix = sum(buf[at + i : at + i + rows, :] * tref[i : i + 1, :] for i in range(SHORT))
        act = jax.nn.silu(mix)
        x = act[:, :ch] * sref[...]
        w = act[:, ch:].astype(bf16)
        xs[...] = x.astype(bf16)
        w16[...] = w
        ends = dot((x * lref[...]).astype(bf16), w, 0, 0).astype(bf16)
        tail = log_rows(logs[...])
        for k in range(copies):
            send[k, :ch, :] = ends
            send[k, ch:, :] = tail

    return pl.pallas_call(
        body,
        out_shape=(sds((copies, ch + LOGS, STATE), bf16), pltpu.VMEM((rows, ch), bf16), pltpu.VMEM((rows, STATE), bf16)),
        in_specs=[VMEM] * 6,
        out_specs=(VMEM,) * 3,
        scratch_shapes=[pltpu.VMEM((ext, 2 * ch), f32)],
        compiler_params=SMALL, name="local_states",
    )(*held(normed, first, taps, step, left, total))


def spread_heads(c, heads, p):
    return jnp.concatenate([jnp.broadcast_to(c[:, h : h + 1], (p, STATE)) for h in range(heads)], 0)


def line_states(got, index, heads, p, copies):
    n, size, _ = got.shape
    ch = heads * p

    def body(at, ref, enter, before, send):
        zero = jnp.zeros((1, STATE), f32)
        acc_in, acc_all = zero, zero
        ent = jnp.zeros((ch, STATE), f32)
        tot = jnp.zeros((ch, STATE), f32)
        for k in reversed(range(n)):
            logs = jnp.sum(ref[k, ch:, :].astype(f32), axis=0, keepdims=True)
            inside = (k < at[0]).astype(f32)
            piece = ref[k, :ch, :].astype(f32)
            ent = ent + piece * spread_heads(inside * jnp.exp(acc_in), heads, p)
            tot = tot + piece * spread_heads(jnp.exp(acc_all), heads, p)
            acc_in = acc_in + inside * logs
            acc_all = acc_all + logs
        enter[...] = ent
        before[...] = jnp.broadcast_to(acc_in, (8, STATE))
        line, tail = tot.astype(bf16), log_rows(acc_all)
        for k in range(copies):
            send[k, :ch, :] = line
            send[k, ch:, :] = tail

    return pl.pallas_call(
        body,
        out_shape=(pltpu.VMEM((ch, STATE), f32), pltpu.VMEM((8, STATE), f32), sds((copies, size, STATE), bf16)),
        in_specs=[SMEM, VMEM],
        out_specs=(VMEM,) * 3,
        compiler_params=SMALL, name="line_states",
    )(index, *held(got))


def rows_local(normed, rest, ftaps, ltaps, xs, w16, cum, cum_t):
    ext, d = normed.shape
    rows, ch = xs.shape
    heads = cum_t.shape[0]
    p = ch // heads
    part, n = 64, 8
    kc = d // n

    def body(nref, wref, ftaps, ltaps, xs, w16, cum, cum_t, read16, zgate, mixed, inner, back, acc, glu, wall, sems):
        def fetch(i):
            at = slice(i * kc, (i + 1) * kc)
            return pltpu.make_async_copy(wref.at[at, : 4 * ch], wall.at[at, :], sems.at[0, i])

        def fetch_back(i):
            at = slice(i * kc, (i + 1) * kc)
            return pltpu.make_async_copy(wref.at[at, 4 * ch :], back.at[at, :], sems.at[1, i])

        for i in range(n):
            fetch(i).start()
        for i in range(n):
            fetch_back(i).start()
        for i in range(n):
            fetch(i).wait()
            at = slice(i * kc, (i + 1) * kc)
            term = dot(nref[:, at], wall[at, :], 1, 0)
            acc[...] = term if i == 0 else acc[...] + term
        glu[...] = acc[:, 2 * ch : 3 * ch].astype(bf16).astype(f32) * jax.nn.sigmoid(
            acc[:, 3 * ch :].astype(bf16).astype(f32)
        )
        acc[:, : 2 * ch] = acc[:, : 2 * ch].astype(bf16).astype(f32)
        s_at, l_at = HALO - SHORT + 1, HALO - WIDE + 1
        read = sum(acc[s_at + i : s_at + i + rows, :ch] * ftaps[i : i + 1, :] for i in range(SHORT))
        read = jax.nn.silu(read).astype(bf16)
        read16[...] = read
        zgate[...] = jax.nn.silu(acc[HALO:, ch : 2 * ch])
        scores = dot(read, w16[...], 1, 1)
        lower = lax.broadcasted_iota(jnp.int32, (rows, rows), 0) >= lax.broadcasted_iota(jnp.int32, (rows, rows), 1)
        lane = lax.broadcasted_iota(jnp.int32, (rows, ch), 1)
        y = jnp.zeros((rows, ch), f32)
        for h in range(heads):
            gap = jnp.where(lower, cum[:, h * p : h * p + 1] - cum_t[h : h + 1, :], 0.0)
            m = jnp.where(lower, jnp.exp(gap) * scores, 0.0).astype(bf16)
            x = jnp.where(lane // p == h, xs[...].astype(f32), 0.0).astype(bf16)
            y = y + dot(m, x, 1, 0)
        inner[...] = y
        for r in range(0, rows, part):
            mixed[r : r + part, :] = sum(
                glu[l_at + r + i : l_at + r + i + part, :] * ltaps[i : i + 1, :] for i in range(WIDE)
            )
        for i in range(n):
            fetch_back(i).wait()

    small = (ftaps, ltaps, xs, w16, cum, cum_t)
    return pl.pallas_call(
        body,
        out_shape=(
            pltpu.VMEM((rows, STATE), bf16), pltpu.VMEM((rows, ch), f32), pltpu.VMEM((rows, ch), f32),
            pltpu.VMEM((rows, ch), f32), pltpu.VMEM((d, 2 * ch), bf16),
        ),
        in_specs=[VMEM, pl.BlockSpec(memory_space=pltpu.HBM), *[VMEM] * len(small)],
        out_specs=(VMEM,) * 5,
        scratch_shapes=[
            pltpu.VMEM((ext, 4 * ch), f32), pltpu.VMEM((ext, ch), f32), pltpu.VMEM((d, 4 * ch), bf16),
            pltpu.SemaphoreType.DMA((2, n)),
        ],
        compiler_params=SMALL, name="rows_local",
    )(*held(normed), *fetched(rest), *held(*small))


def rows_done(got, enter, before, init, index, read16, zgate, mixed, inner, cum, gain, copies):
    rows, ch = mixed.shape
    n, _, _ = got.shape
    heads = init.shape[0]
    p = ch // heads

    def body(at, got, enter, before, init, read16, zgate, mixed, inner, cum, gain, sums, pre):
        acc_in = jnp.zeros((1, STATE), f32)
        start = enter[...]
        b = before[0:1, :]
        for j in reversed(range(n)):
            logs = jnp.sum(got[j, ch:, :].astype(f32), axis=0, keepdims=True)
            inside = (j < at[0]).astype(f32)
            start = start + got[j, :ch, :].astype(f32) * spread_heads(inside * jnp.exp(acc_in + b), heads, p)
            acc_in = acc_in + inside * logs
        start = start + init[...].reshape(ch, STATE) * spread_heads(jnp.exp(acc_in + b), heads, p)
        y = inner[...] + dot(read16[...], start.astype(bf16), 1, 1) * jnp.exp(cum[...])
        gated = y * zgate[...]
        mix = mixed[...]
        squares = jnp.concatenate([mix, mix * mix, gated * gated], 1)
        pick = lax.broadcasted_iota(jnp.int32, (8, 3 * ch), 1) // ch == lax.broadcasted_iota(jnp.int32, (8, 3 * ch), 0)
        found = dot(jnp.where(pick, 1.0, 0.0), squares, 1, 1, HIGHEST)
        for j in range(copies):
            sums[j] = found[:3]
        pre[:, :ch] = mix.astype(bf16)
        pre[:, ch:] = (gated * gain[...]).astype(bf16)

    return pl.pallas_call(
        body,
        out_shape=(sds((copies, 3, rows), f32), pltpu.VMEM((rows, 2 * ch), bf16)),
        in_specs=[SMEM, *[VMEM] * 10],
        out_specs=(VMEM, VMEM),
        compiler_params=SMALL, name="rows_done",
    )(index, *held(got, enter, before, init, read16, zgate, mixed, inner, cum, gain))


def output_rows(sums, both, gains, own, other, index, nf, nt):
    copies, _, rows = sums.shape
    ch = gains.shape[1]
    d = own.shape[0]
    piece = rows // (nf * nt)

    def body(at, sref, bref, gref, wa, wb, out, cols, act):
        tp = at[0]
        s = sref[0]
        for j in range(1, copies):
            s = s + sref[j]
        cols[...] = jnp.transpose(jnp.concatenate([s, jnp.zeros((5, rows), f32)], 0))
        for i in range(nf):
            at_row = pl.multiple_of(i * (nt * piece) + tp * piece, piece)
            here = slice(i * piece, (i + 1) * piece)
            t = cols[pl.ds(at_row, piece), :]
            mean = t[:, 0:1] / C_CH
            rstd = lax.rsqrt(t[:, 1:2] / C_CH - mean * mean + EPS)
            scale = lax.rsqrt(t[:, 2:3] / D_INNER + EPS)
            for j in range(nt):
                src = tp if j == 0 else 1 - tp
                a = bref[pl.ds(pl.multiple_of(src * rows + at_row, piece), piece), :].astype(f32)
                conv = jax.nn.silu((a[:, :ch] - mean) * rstd * gref[pl.ds(src, 1), :])
                act[here, 2 * j * ch : (2 * j + 1) * ch] = conv.astype(bf16)
                act[here, (2 * j + 1) * ch : (2 * j + 2) * ch] = (a[:, ch:] * scale).astype(bf16)
        term = dot(act[:, : 2 * ch], wa[...], 1, 1) + dot(act[:, 2 * ch :], wb[...], 1, 1)
        out[...] = term.astype(bf16).reshape(nf, piece, d)

    return pl.pallas_call(
        body,
        out_shape=sds((nf, piece, d), bf16),
        in_specs=[SMEM, *[VMEM] * 5],
        out_specs=VMEM,
        scratch_shapes=[pltpu.VMEM((rows, 8), f32), pltpu.VMEM((nf * piece, 4 * ch), bf16)],
        compiler_params=SMALL, name="output_rows",
    )(index, *held(sums, both, gains, own, other))


def per_device(
    tokens, norm_gain, conv_value, conv_gate, mixer_gate, state_input, write_projection, state_read,
    step_proj, step_bias, decay_log, decay_extra, input_taps, write_taps, fetch_taps, long_taps,
    conv_gain, state_gain, conv_output, state_output, initial_state,
):
    rows = tokens.shape[0]
    ch = conv_value.shape[1]
    heads = step_bias.shape[0]
    p = ch // heads
    nf, nt = lax.axis_size("fs"), lax.axis_size("tp")
    iz, iy, tp = (lax.axis_index(a).astype(jnp.int32).reshape(1) for a in ("sp_0", "sp_1", "tp"))
    ny = lax.axis_size("sp_1")
    rest = lay_out((state_read, mixer_gate, conv_value, conv_gate, conv_output, state_output), 1)
    rest = lax.all_gather(rest[0], SP, axis=0, tiled=True)
    first = lay_out((state_input, write_projection), ny)
    first = lax.all_to_all(first, "sp_1", 0, 0, tiled=True)
    first = copies_of(first, lax.axis_size("sp_0"))
    first = lax.all_to_all(first, "sp_0", 0, 0, tiled=True).reshape(-1, 2 * ch)
    n = lax.axis_size(SP)
    halo = lax.ppermute(tokens[rows - HALO :], SP, [(i, i + 1) for i in range(n - 1)])
    v = jnp.concatenate([halo, tokens], 0).astype(f32)
    normed = (v * lax.rsqrt(jnp.mean(v * v, axis=1, keepdims=True) + EPS) * norm_gain).astype(bf16)
    step_all = jnp.dot(normed[HALO:], step_proj, preferred_element_type=f32)
    me = lax.axis_index("fs") * nt + lax.axis_index("tp")
    step = jax.nn.softplus(lax.dynamic_slice_in_dim(step_all, me * heads, heads, 1) + step_bias)
    log_step = (-jnp.exp(decay_log) * step + decay_extra.T).T
    cum_t = jnp.cumsum(log_step, axis=1)
    total = cum_t[:, -1]
    cum = jnp.repeat(cum_t.T, p, axis=1)
    step = jnp.repeat(step, p, axis=1)
    left = jnp.repeat(jnp.exp(total[:, None] - cum_t).T, p, axis=1)
    total = jnp.pad(total[None], ((0, 0), (0, STATE - heads)))
    gains = lax.all_gather(conv_gain, "tp")
    taps = jnp.concatenate([input_taps, write_taps], 1)
    send, xs, w16 = local_states(normed, first, taps, step, left, total, ny)
    got = lax.all_to_all(send, "sp_1", 0, 0, tiled=True)
    enter, before, send = line_states(got, iy, heads, p, lax.axis_size("sp_0"))
    got = lax.all_to_all(send, "sp_0", 0, 0, tiled=True)
    read16, zgate, mixed, inner, back = rows_local(normed, rest, fetch_taps, long_taps, xs, w16, cum, cum_t)
    back_other = lax.ppermute(back, "tp", [(i, nt - 1 - i) for i in range(nt)])
    sums, pre = rows_done(
        got, enter, before, initial_state, iz, read16, zgate, mixed, inner, cum, state_gain[None], nf * nt
    )
    sums = lax.all_to_all(sums, FT, 0, 0, tiled=True)
    both = lax.all_gather(pre, "tp", axis=0, tiled=True)
    out = output_rows(sums, both, gains, back, back_other, tp, nf, nt)
    pieces = lax.all_to_all(out, "fs", 0, 0, tiled=True)
    return jnp.sum(pieces.astype(f32), 0).astype(bf16)


def solution(mesh):
    torus = Mesh(
        mesh.devices.reshape(8, 8, mesh.shape["fs"], mesh.shape["tp"]), ("sp_0", "sp_1", "fs", "tp")
    )
    w = P(SP, FT)
    in_specs = (
        P(SP, None), P(), w, w, w, w, w, w, P(), P(FT), P(FT), P(FT, SP), P(None, FT), P(None, FT), P(None, FT),
        P(None, FT), P(FT), P(FT), w, w, P(FT, None, None),
    )

    return jax.shard_map(per_device, mesh=torus, in_specs=in_specs, out_specs=P((*SP, *FT), None), check_vma=False)
```

```python
import jax
import jax.numpy as jnp
from jax import lax
from jax.experimental import pallas as pl
from jax.experimental.pallas import tpu as pltpu
from jax.sharding import Mesh
from jax.sharding import PartitionSpec as P


C_CH = 1024
STATE = 128
D_INNER = 1024
WIDE = 31
SHORT = 4
HALO = 32
EPS = 1e-06
LOGS = 8
SP = ("sp_0", "sp_1")
FT = ("fs", "tp")
f32 = jnp.float32
bf16 = jnp.bfloat16
VMEM = pl.BlockSpec(memory_space=pltpu.VMEM)
SMEM = pl.BlockSpec(memory_space=pltpu.SMEM)
HIGHEST = lax.Precision.HIGHEST
SMALL = pltpu.CompilerParams(vmem_limit_bytes=12 * 2**20)


def dot(a, b, ca, cb, precision=None):
    return lax.dot_general(a, b, (((ca,), (cb,)), ((), ())), precision=precision, preferred_element_type=f32)


def sds(shape, dtype):
    return jax.ShapeDtypeStruct(shape, dtype)


def held(*arrays):
    return tuple(pltpu.with_memory_space_constraint(a, pltpu.VMEM) for a in arrays)


def fetched(*arrays):
    return tuple(pltpu.with_memory_space_constraint(a, pltpu.HBM) for a in arrays)


def lay_out(shards, copies):
    rows, ch = shards[0].shape
    n = len(shards)

    def body(*refs):
        for i in range(n):
            w = refs[i][...]
            for k in range(copies):
                refs[n][k, :, i * ch : (i + 1) * ch] = w

    return pl.pallas_call(
        body, out_shape=sds((copies, rows, n * ch), bf16), in_specs=[VMEM] * n, out_specs=VMEM, compiler_params=SMALL
    )(*fetched(*shards))


def copies_of(block, copies):
    def body(ref, out):
        for k in range(copies):
            out[k] = ref[...]

    return pl.pallas_call(
        body, out_shape=sds((copies, *block.shape), bf16), in_specs=[VMEM], out_specs=VMEM, compiler_params=SMALL
    )(*held(block))


def log_rows(logs):
    hi = logs.astype(bf16).astype(f32)
    mid = (logs - hi).astype(bf16).astype(f32)
    lo = logs - hi - mid
    row = lax.broadcasted_iota(jnp.int32, (LOGS, STATE), 0)
    return jnp.where(row == 0, hi, jnp.where(row == 1, mid, jnp.where(row == 2, lo, 0.0))).astype(bf16)


def local_states(halo, own, most, last, taps, step, left, total, copies):
    rows, d = own.shape
    ch = step.shape[1]
    nz, main, _ = most.shape
    size = main + last.shape[1]

    def body(href, nref, mref, rref, tref, sref, lref, logs, send, xs, w16, buf, wall):
        for z in range(nz):
            wall[z * size : z * size + main, :] = mref[z]
            wall[z * size + main : (z + 1) * size, :] = rref[z]
        buf[:HALO, :] = dot(href[...], wall[...], 1, 0).astype(bf16).astype(f32)
        buf[HALO:, :] = dot(nref[...], wall[...], 1, 0).astype(bf16).astype(f32)
        at = HALO - SHORT + 1
        mix = sum(buf[at + i : at + i + rows, :] * tref[i : i + 1, :] for i in range(SHORT))
        act = jax.nn.silu(mix)
        x = act[:, :ch] * sref[...]
        w = act[:, ch:].astype(bf16)
        xs[...] = x.astype(bf16)
        w16[...] = w
        ends = dot((x * lref[...]).astype(bf16), w, 0, 0).astype(bf16)
        tail = log_rows(logs[...])
        for k in range(copies):
            send[k, :ch, :] = ends
            send[k, ch:, :] = tail

    return pl.pallas_call(
        body,
        out_shape=(sds((copies, ch + LOGS, STATE), bf16), pltpu.VMEM((rows, ch), bf16), pltpu.VMEM((rows, STATE), bf16)),
        in_specs=[VMEM] * 8,
        out_specs=(VMEM,) * 3,
        scratch_shapes=[pltpu.VMEM((HALO + rows, 2 * ch), f32), pltpu.VMEM((d, 2 * ch), bf16)],
        compiler_params=SMALL, name="local_states",
    )(*held(halo, own, most, last, taps, step, left, total))


def spread_heads(c, heads, p):
    return jnp.concatenate([jnp.broadcast_to(c[:, h : h + 1], (p, STATE)) for h in range(heads)], 0)


def line_states(got, index, heads, p, copies):
    n, size, _ = got.shape
    ch = heads * p

    def body(at, ref, enter, before, send):
        zero = jnp.zeros((1, STATE), f32)
        acc_in, acc_all = zero, zero
        ent = jnp.zeros((ch, STATE), f32)
        tot = jnp.zeros((ch, STATE), f32)
        for k in reversed(range(n)):
            logs = jnp.sum(ref[k, ch:, :].astype(f32), axis=0, keepdims=True)
            inside = (k < at[0]).astype(f32)
            piece = ref[k, :ch, :].astype(f32)
            ent = ent + piece * spread_heads(inside * jnp.exp(acc_in), heads, p)
            tot = tot + piece * spread_heads(jnp.exp(acc_all), heads, p)
            acc_in = acc_in + inside * logs
            acc_all = acc_all + logs
        enter[...] = ent
        before[...] = jnp.broadcast_to(acc_in, (8, STATE))
        line, tail = tot.astype(bf16), log_rows(acc_all)
        for k in range(copies):
            send[k, :ch, :] = line
            send[k, ch:, :] = tail

    return pl.pallas_call(
        body,
        out_shape=(pltpu.VMEM((ch, STATE), f32), pltpu.VMEM((8, STATE), f32), sds((copies, size, STATE), bf16)),
        in_specs=[SMEM, VMEM],
        out_specs=(VMEM,) * 3,
        compiler_params=SMALL, name="line_states",
    )(index, *held(got))


def rows_done(halo, own, rest, ltaps, got, enter, before, init, index, ftaps, xs, w16, cum, cum_t, gain, copies):
    rows, d = own.shape
    ch = xs.shape[1]
    ext = HALO + rows
    n, _, _ = got.shape
    heads = cum_t.shape[0]
    p = ch // heads
    part, parts = 64, 8
    kc = d // parts

    def body(
        at, href, nref, wref, lref, got, enter, before, init, ftaps, xs, w16, cum, cum_t, gain,
        sums, pre, back, acc, glu, wall, ltaps, sems,
    ):
        def fetch(i):
            here = slice(i * kc, (i + 1) * kc)
            return pltpu.make_async_copy(wref.at[here, : 4 * ch], wall.at[here, :], sems.at[0, i])

        def fetch_back(i):
            here = slice(i * kc, (i + 1) * kc)
            return pltpu.make_async_copy(wref.at[here, 4 * ch :], back.at[here, :], sems.at[1, i])

        fetch_taps = pltpu.make_async_copy(lref, ltaps, sems.at[2, 0])
        for i in range(parts):
            fetch(i).start()
        fetch_taps.start()
        for i in range(parts):
            fetch_back(i).start()
        acc_in = jnp.zeros((1, STATE), f32)
        start = enter[...]
        b = before[0:1, :]
        for j in reversed(range(n)):
            logs = jnp.sum(got[j, ch:, :].astype(f32), axis=0, keepdims=True)
            inside = (j < at[0]).astype(f32)
            start = start + got[j, :ch, :].astype(f32) * spread_heads(inside * jnp.exp(acc_in + b), heads, p)
            acc_in = acc_in + inside * logs
        start = start + init[...].reshape(ch, STATE) * spread_heads(jnp.exp(acc_in + b), heads, p)
        start = start.astype(bf16)
        for i in range(parts):
            fetch(i).wait()
            here = slice(i * kc, (i + 1) * kc)
            first = dot(href[:, here], wall[here, :], 1, 0)
            term = dot(nref[:, here], wall[here, :], 1, 0)
            acc[:HALO, :] = first if i == 0 else acc[:HALO, :] + first
            acc[HALO:, :] = term if i == 0 else acc[HALO:, :] + term
        glu[...] = acc[:, 2 * ch : 3 * ch].astype(bf16).astype(f32) * jax.nn.sigmoid(
            acc[:, 3 * ch :].astype(bf16).astype(f32)
        )
        acc[:, : 2 * ch] = acc[:, : 2 * ch].astype(bf16).astype(f32)
        s_at, l_at = HALO - SHORT + 1, HALO - WIDE + 1
        read = sum(acc[s_at + i : s_at + i + rows, :ch] * ftaps[i : i + 1, :] for i in range(SHORT))
        read = jax.nn.silu(read).astype(bf16)
        y = dot(read, start, 1, 1) * jnp.exp(cum[...])
        scores = dot(read, w16[...], 1, 1)
        lower = lax.broadcasted_iota(jnp.int32, (rows, rows), 0) >= lax.broadcasted_iota(jnp.int32, (rows, rows), 1)
        lane = lax.broadcasted_iota(jnp.int32, (rows, ch), 1)
        for h in range(heads):
            gap = jnp.where(lower, cum[:, h * p : h * p + 1] - cum_t[h : h + 1, :], 0.0)
            m = jnp.where(lower, jnp.exp(gap) * scores, 0.0).astype(bf16)
            x = jnp.where(lane // p == h, xs[...].astype(f32), 0.0).astype(bf16)
            y = y + dot(m, x, 1, 0)
        gated = y * jax.nn.silu(acc[HALO:, ch : 2 * ch])
        fetch_taps.wait()
        mix = jnp.concatenate(
            [
                sum(glu[l_at + r + i : l_at + r + i + part, :] * ltaps[i : i + 1, :] for i in range(WIDE))
                for r in range(0, rows, part)
            ],
            0,
        )
        squares = jnp.concatenate([mix, mix * mix, gated * gated], 1)
        pick = lax.broadcasted_iota(jnp.int32, (8, 3 * ch), 1) // ch == lax.broadcasted_iota(jnp.int32, (8, 3 * ch), 0)
        found = dot(jnp.where(pick, 1.0, 0.0), squares, 1, 1, HIGHEST)
        for j in range(copies):
            sums[j] = found[:3]
        pre[:, :ch] = mix.astype(bf16)
        pre[:, ch:] = (gated * gain[...]).astype(bf16)
        for i in range(parts):
            fetch_back(i).wait()

    hbm = pl.BlockSpec(memory_space=pltpu.HBM)
    return pl.pallas_call(
        body,
        out_shape=(sds((copies, 3, rows), f32), pltpu.VMEM((rows, 2 * ch), bf16), pltpu.VMEM((d, 2 * ch), bf16)),
        in_specs=[SMEM, VMEM, VMEM, hbm, hbm, *[VMEM] * 10],
        out_specs=(VMEM,) * 3,
        scratch_shapes=[
            pltpu.VMEM((ext, 4 * ch), f32), pltpu.VMEM((ext, ch), f32), pltpu.VMEM((d, 4 * ch), bf16),
            pltpu.VMEM(ltaps.shape, f32), pltpu.SemaphoreType.DMA((3, parts)),
        ],
        compiler_params=SMALL, name="rows_done",
    )(index, *held(halo, own), *fetched(rest, ltaps), *held(got, enter, before, init, ftaps, xs, w16, cum, cum_t, gain))


def output_rows(sums, both, gains, own, other, index, nf, nt):
    copies, _, rows = sums.shape
    ch = gains.shape[1]
    d = own.shape[0]
    piece = rows // (nf * nt)

    def body(at, sref, bref, gref, wa, wb, out, cols, act):
        tp = at[0]
        s = sref[0]
        for j in range(1, copies):
            s = s + sref[j]
        cols[...] = jnp.transpose(jnp.concatenate([s, jnp.zeros((5, rows), f32)], 0))
        for i in range(nf):
            at_row = pl.multiple_of(i * (nt * piece) + tp * piece, piece)
            here = slice(i * piece, (i + 1) * piece)
            t = cols[pl.ds(at_row, piece), :]
            mean = t[:, 0:1] / C_CH
            rstd = lax.rsqrt(t[:, 1:2] / C_CH - mean * mean + EPS)
            scale = lax.rsqrt(t[:, 2:3] / D_INNER + EPS)
            for j in range(nt):
                src = tp if j == 0 else 1 - tp
                a = bref[pl.ds(pl.multiple_of(src * rows + at_row, piece), piece), :].astype(f32)
                conv = jax.nn.silu((a[:, :ch] - mean) * rstd * gref[pl.ds(src, 1), :])
                act[here, 2 * j * ch : (2 * j + 1) * ch] = conv.astype(bf16)
                act[here, (2 * j + 1) * ch : (2 * j + 2) * ch] = (a[:, ch:] * scale).astype(bf16)
        term = dot(act[:, : 2 * ch], wa[...], 1, 1) + dot(act[:, 2 * ch :], wb[...], 1, 1)
        out[...] = term.astype(bf16).reshape(nf, piece, d)

    return pl.pallas_call(
        body,
        out_shape=sds((nf, piece, d), bf16),
        in_specs=[SMEM, *[VMEM] * 5],
        out_specs=VMEM,
        scratch_shapes=[pltpu.VMEM((rows, 8), f32), pltpu.VMEM((nf * piece, 4 * ch), bf16)],
        compiler_params=SMALL, name="output_rows",
    )(index, *held(sums, both, gains, own, other))


def per_device(
    tokens, norm_gain, conv_value, conv_gate, mixer_gate, state_input, write_projection, state_read,
    step_proj, step_bias, decay_log, decay_extra, input_taps, write_taps, fetch_taps, long_taps,
    conv_gain, state_gain, conv_output, state_output, initial_state,
):
    rows = tokens.shape[0]
    ch = conv_value.shape[1]
    heads = step_bias.shape[0]
    p = ch // heads
    nf, nt = lax.axis_size("fs"), lax.axis_size("tp")
    iz, iy, tp = (lax.axis_index(a).astype(jnp.int32).reshape(1) for a in ("sp_0", "sp_1", "tp"))
    ny = lax.axis_size("sp_1")
    rest = lay_out((state_read, mixer_gate, conv_value, conv_gate, conv_output, state_output), 1)
    rest = lax.all_gather(rest[0], SP, axis=0, tiled=True)
    first = lay_out((state_input, write_projection), ny)
    first = lax.all_to_all(first, "sp_1", 0, 0, tiled=True)
    first = first.reshape(-1, 2 * ch)
    main = first.shape[0] - first.shape[0] // 16
    last = copies_of(first[main:], lax.axis_size("sp_0"))
    last = lax.all_to_all(last, "sp_0", 0, 0, tiled=True)
    most = lax.all_gather(first[:main], "sp_0", axis=0)
    n = lax.axis_size(SP)
    halo = lax.ppermute(tokens[rows - HALO :], SP, [(i, i + 1) for i in range(n - 1)])

    def unit(x):
        v = x.astype(f32)
        return (v * lax.rsqrt(jnp.mean(v * v, axis=1, keepdims=True) + EPS) * norm_gain).astype(bf16)

    own = unit(tokens)
    halo = unit(halo)
    step_all = jnp.dot(own, step_proj, preferred_element_type=f32)
    me = lax.axis_index("fs") * nt + lax.axis_index("tp")
    step = jax.nn.softplus(lax.dynamic_slice_in_dim(step_all, me * heads, heads, 1) + step_bias)
    log_step = (-jnp.exp(decay_log) * step + decay_extra.T).T
    cum_t = jnp.cumsum(log_step, axis=1)
    total = cum_t[:, -1]
    cum = jnp.repeat(cum_t.T, p, axis=1)
    step = jnp.repeat(step, p, axis=1)
    left = jnp.repeat(jnp.exp(total[:, None] - cum_t).T, p, axis=1)
    total = jnp.pad(total[None], ((0, 0), (0, STATE - heads)))
    gains = lax.all_gather(conv_gain, "tp")
    taps = jnp.concatenate([input_taps, write_taps], 1)
    send, xs, w16 = local_states(halo, own, most, last, taps, step, left, total, ny)
    got = lax.all_to_all(send, "sp_1", 0, 0, tiled=True)
    enter, before, send = line_states(got, iy, heads, p, lax.axis_size("sp_0"))
    got = lax.all_to_all(send, "sp_0", 0, 0, tiled=True)
    sums, pre, back = rows_done(
        halo, own, rest, long_taps, got, enter, before, initial_state, iz, fetch_taps, xs, w16, cum, cum_t,
        state_gain[None], nf * nt,
    )
    back_other = lax.ppermute(back, "tp", [(i, nt - 1 - i) for i in range(nt)])
    sums = lax.all_to_all(sums, FT, 0, 0, tiled=True)
    both = lax.all_gather(pre, "tp", axis=0, tiled=True)
    out = output_rows(sums, both, gains, back, back_other, tp, nf, nt)
    pieces = lax.all_to_all(out, "fs", 0, 0, tiled=True)
    return jnp.sum(pieces.astype(f32), 0).astype(bf16)


def solution(mesh):
    torus = Mesh(
        mesh.devices.reshape(8, 8, mesh.shape["fs"], mesh.shape["tp"]), ("sp_0", "sp_1", "fs", "tp")
    )
    w = P(SP, FT)
    in_specs = (
        P(SP, None), P(), w, w, w, w, w, w, P(), P(FT), P(FT), P(FT, SP), P(None, FT), P(None, FT), P(None, FT),
        P(None, FT), P(FT), P(FT), w, w, P(FT, None, None),
    )

    return jax.shard_map(per_device, mesh=torus, in_specs=in_specs, out_specs=P((*SP, *FT), None), check_vma=False)
```

```python
import jax
import jax.numpy as jnp
from jax import lax
from jax.experimental import pallas as pl
from jax.experimental.pallas import tpu as pltpu
from jax.sharding import Mesh
from jax.sharding import PartitionSpec as P


C_CH = 1024
STATE = 128
D_INNER = 1024
WIDE = 31
SHORT = 4
HALO = 32
EPS = 1e-06
LOGS = 8
SP = ("sp_0", "sp_1")
FT = ("fs", "tp")
f32 = jnp.float32
bf16 = jnp.bfloat16
VMEM = pl.BlockSpec(memory_space=pltpu.VMEM)
SMEM = pl.BlockSpec(memory_space=pltpu.SMEM)
HIGHEST = lax.Precision.HIGHEST
SMALL = pltpu.CompilerParams(vmem_limit_bytes=12 * 2**20)


def dot(a, b, ca, cb, precision=None):
    return lax.dot_general(a, b, (((ca,), (cb,)), ((), ())), precision=precision, preferred_element_type=f32)


def sds(shape, dtype):
    return jax.ShapeDtypeStruct(shape, dtype)


def held(*arrays):
    return tuple(pltpu.with_memory_space_constraint(a, pltpu.VMEM) for a in arrays)


def fetched(*arrays):
    return tuple(pltpu.with_memory_space_constraint(a, pltpu.HBM) for a in arrays)


def lay_out(shards, copies):
    rows, ch = shards[0].shape
    n = len(shards)

    def body(*refs):
        for i in range(n):
            w = refs[i][...]
            for k in range(copies):
                refs[n][k, :, i * ch : (i + 1) * ch] = w

    return pl.pallas_call(
        body, out_shape=sds((copies, rows, n * ch), bf16), in_specs=[VMEM] * n, out_specs=VMEM, compiler_params=SMALL
    )(*fetched(*shards))


def parted(near, first, copies):
    ny, piece, width = near.shape
    size = ny * piece
    main = size - size // 16

    def body(ref, rest, most, last):
        for y in range(ny):
            rest[y * piece : (y + 1) * piece, :] = ref[y, :, first:]
            if (y + 1) * piece <= main:
                most[y * piece : (y + 1) * piece, :] = ref[y, :, :first]
        inside = main % piece
        if inside:
            most[main - inside :, :] = ref[main // piece, :inside, :first]
        for k in range(copies):
            last[k] = ref[ny - 1, piece - (size - main) :, :first]

    return pl.pallas_call(
        body,
        out_shape=(sds((size, width - first), bf16), pltpu.VMEM((main, first), bf16), sds((copies, size - main, first), bf16)),
        in_specs=[VMEM], out_specs=(VMEM,) * 3, compiler_params=SMALL, name="parted",
    )(*held(near))


def log_rows(logs):
    hi = logs.astype(bf16).astype(f32)
    mid = (logs - hi).astype(bf16).astype(f32)
    lo = logs - hi - mid
    row = lax.broadcasted_iota(jnp.int32, (LOGS, STATE), 0)
    return jnp.where(row == 0, hi, jnp.where(row == 1, mid, jnp.where(row == 2, lo, 0.0))).astype(bf16)


def steps_of(own, step_proj, extra, bias, rate_log, index, p):
    rows, _ = own.shape
    heads = extra.shape[0]
    ch = heads * p
    every = step_proj.shape[1]

    def body(at, bref, rref, nref, wref, eref, step, left, cum, cum_t, total):
        raw = dot(wref[...], nref[...], 0, 1)
        which = lax.broadcasted_iota(jnp.int32, (every, rows), 0)
        size, logs = [], []
        for h in range(heads):
            x = jnp.sum(jnp.where(which == at[0] * heads + h, raw, 0.0), axis=0, keepdims=True) + bref[h]
            size.append(jnp.maximum(x, 0.0) + jnp.log1p(jnp.exp(-jnp.abs(x))))
            logs.append(-jnp.exp(jnp.full((1, rows), rref[h], f32)) * size[h] + eref[h : h + 1, :])
        none = [jnp.zeros((8 - heads, rows), f32)]
        upto = lax.broadcasted_iota(jnp.int32, (rows, rows), 0) <= lax.broadcasted_iota(jnp.int32, (rows, rows), 1)
        run = dot(jnp.concatenate(logs + none, 0), jnp.where(upto, 1.0, 0.0), 1, 0, HIGHEST)
        lane = lax.broadcasted_iota(jnp.int32, (rows, ch), 1) // p

        def wide(cols):
            out = jnp.broadcast_to(cols[:, 0:1], (rows, ch))
            for h in range(1, heads):
                out = jnp.where(lane == h, cols[:, h : h + 1], out)
            return out

        cum_t[...] = run[:heads]
        cum[...] = wide(jnp.transpose(run))
        left[...] = wide(jnp.transpose(jnp.exp(run[:, rows - 1 :] - run)))
        step[...] = wide(jnp.transpose(jnp.concatenate(size + none, 0)))
        place = lax.broadcasted_iota(jnp.int32, (1, STATE), 1)
        ends = jnp.zeros((1, STATE), f32)
        for h in range(heads):
            ends = jnp.where(place == h, run[h : h + 1, rows - 1 :], ends)
        total[...] = ends

    wide = pltpu.VMEM((rows, ch), f32)
    return pl.pallas_call(
        body,
        out_shape=(wide, wide, wide, pltpu.VMEM((heads, rows), f32), pltpu.VMEM((1, STATE), f32)),
        in_specs=[SMEM, SMEM, SMEM, VMEM, VMEM, VMEM],
        out_specs=(VMEM,) * 5,
        compiler_params=SMALL, name="steps_of",
    )(index, bias, rate_log, *held(own, step_proj, extra))


def local_states(halo, own, most, last, taps, step, left, total, copies):
    rows, d = own.shape
    ch = step.shape[1]
    nz, main, _ = most.shape
    size = main + last.shape[1]

    def body(href, nref, mref, rref, tref, sref, lref, logs, send, xs, w16, buf, wall):
        for z in range(nz):
            wall[z * size : z * size + main, :] = mref[z]
            wall[z * size + main : (z + 1) * size, :] = rref[z]
        buf[:HALO, :] = dot(href[...], wall[...], 1, 0).astype(bf16).astype(f32)
        buf[HALO:, :] = dot(nref[...], wall[...], 1, 0).astype(bf16).astype(f32)
        at = HALO - SHORT + 1
        mix = sum(buf[at + i : at + i + rows, :] * tref[i : i + 1, :] for i in range(SHORT))
        act = jax.nn.silu(mix)
        x = act[:, :ch] * sref[...]
        w = act[:, ch:].astype(bf16)
        xs[...] = x.astype(bf16)
        w16[...] = w
        ends = dot((x * lref[...]).astype(bf16), w, 0, 0).astype(bf16)
        tail = log_rows(logs[...])
        for k in range(copies):
            send[k, :ch, :] = ends
            send[k, ch:, :] = tail

    return pl.pallas_call(
        body,
        out_shape=(sds((copies, ch + LOGS, STATE), bf16), pltpu.VMEM((rows, ch), bf16), pltpu.VMEM((rows, STATE), bf16)),
        in_specs=[VMEM] * 8,
        out_specs=(VMEM,) * 3,
        scratch_shapes=[pltpu.VMEM((HALO + rows, 2 * ch), f32), pltpu.VMEM((d, 2 * ch), bf16)],
        compiler_params=SMALL, name="local_states",
    )(*held(halo, own, most, last, taps, step, left, total))


def spread_heads(c, heads, p):
    return jnp.concatenate([jnp.broadcast_to(c[:, h : h + 1], (p, STATE)) for h in range(heads)], 0)


def line_states(got, index, heads, p, copies):
    n, size, _ = got.shape
    ch = heads * p

    def body(at, ref, enter, before, send):
        zero = jnp.zeros((1, STATE), f32)
        acc_in, acc_all = zero, zero
        ent = jnp.zeros((ch, STATE), f32)
        tot = jnp.zeros((ch, STATE), f32)
        for k in reversed(range(n)):
            logs = jnp.sum(ref[k, ch:, :].astype(f32), axis=0, keepdims=True)
            inside = (k < at[0]).astype(f32)
            piece = ref[k, :ch, :].astype(f32)
            ent = ent + piece * spread_heads(inside * jnp.exp(acc_in), heads, p)
            tot = tot + piece * spread_heads(jnp.exp(acc_all), heads, p)
            acc_in = acc_in + inside * logs
            acc_all = acc_all + logs
        enter[...] = ent
        before[...] = jnp.broadcast_to(acc_in, (8, STATE))
        line, tail = tot.astype(bf16), log_rows(acc_all)
        for k in range(copies):
            send[k, :ch, :] = line
            send[k, ch:, :] = tail

    return pl.pallas_call(
        body,
        out_shape=(pltpu.VMEM((ch, STATE), f32), pltpu.VMEM((8, STATE), f32), sds((copies, size, STATE), bf16)),
        in_specs=[SMEM, VMEM],
        out_specs=(VMEM,) * 3,
        compiler_params=SMALL, name="line_states",
    )(index, *held(got))


def rows_local(halo, own, rest, ftaps, ltaps, xs, w16, cum, cum_t):
    rows, d = own.shape
    ch = xs.shape[1]
    ext = HALO + rows
    heads = cum_t.shape[0]
    p = ch // heads
    part, n = 64, 8
    kc = d // n

    def body(
        hall, nall, wref, ftaps, ltaps, xs, w16, cum, cum_t, read16, zgate, mixed, inner, back, acc, glu, wall, href, nref, sems
    ):
        def fetch(i):
            at = slice(i * kc, (i + 1) * kc)
            return pltpu.make_async_copy(wref.at[at, : 4 * ch], wall.at[at, :], sems.at[0, i])

        def fetch_back(i):
            at = slice(i * kc, (i + 1) * kc)
            return pltpu.make_async_copy(wref.at[at, 4 * ch :], back.at[at, :], sems.at[1, i])

        near = (
            pltpu.make_async_copy(hall, href, sems.at[2, 0]),
            pltpu.make_async_copy(nall, nref, sems.at[2, 1]),
        )
        for copy in near:
            copy.start()
        for i in range(n):
            fetch(i).start()
        for i in range(n):
            fetch_back(i).start()
        for copy in near:
            copy.wait()
        for i in range(n):
            fetch(i).wait()
            at = slice(i * kc, (i + 1) * kc)
            before = dot(href[:, at], wall[at, :], 1, 0)
            term = dot(nref[:, at], wall[at, :], 1, 0)
            acc[:HALO, :] = before if i == 0 else acc[:HALO, :] + before
            acc[HALO:, :] = term if i == 0 else acc[HALO:, :] + term
        glu[...] = acc[:, 2 * ch : 3 * ch].astype(bf16).astype(f32) * jax.nn.sigmoid(
            acc[:, 3 * ch :].astype(bf16).astype(f32)
        )
        acc[:, : 2 * ch] = acc[:, : 2 * ch].astype(bf16).astype(f32)
        s_at, l_at = HALO - SHORT + 1, HALO - WIDE + 1
        read = sum(acc[s_at + i : s_at + i + rows, :ch] * ftaps[i : i + 1, :] for i in range(SHORT))
        read = jax.nn.silu(read).astype(bf16)
        read16[...] = read
        zgate[...] = jax.nn.silu(acc[HALO:, ch : 2 * ch])
        scores = dot(read, w16[...], 1, 1)
        lower = lax.broadcasted_iota(jnp.int32, (rows, rows), 0) >= lax.broadcasted_iota(jnp.int32, (rows, rows), 1)
        lane = lax.broadcasted_iota(jnp.int32, (rows, ch), 1)
        y = jnp.zeros((rows, ch), f32)
        for h in range(heads):
            gap = jnp.where(lower, cum[:, h * p : h * p + 1] - cum_t[h : h + 1, :], 0.0)
            m = jnp.where(lower, jnp.exp(gap) * scores, 0.0).astype(bf16)
            x = jnp.where(lane // p == h, xs[...].astype(f32), 0.0).astype(bf16)
            y = y + dot(m, x, 1, 0)
        inner[...] = y
        for r in range(0, rows, part):
            mixed[r : r + part, :] = sum(
                glu[l_at + r + i : l_at + r + i + part, :] * ltaps[i : i + 1, :] for i in range(WIDE)
            )
        for i in range(n):
            fetch_back(i).wait()

    small = (ftaps, ltaps, xs, w16, cum, cum_t)
    return pl.pallas_call(
        body,
        out_shape=(
            pltpu.VMEM((rows, STATE), bf16), pltpu.VMEM((rows, ch), f32), pltpu.VMEM((rows, ch), f32),
            pltpu.VMEM((rows, ch), f32), pltpu.VMEM((d, 2 * ch), bf16),
        ),
        in_specs=[*[pl.BlockSpec(memory_space=pltpu.HBM)] * 3, *[VMEM] * len(small)],
        out_specs=(VMEM,) * 5,
        scratch_shapes=[
            pltpu.VMEM((ext, 4 * ch), f32), pltpu.VMEM((ext, ch), f32), pltpu.VMEM((d, 4 * ch), bf16),
            pltpu.VMEM(halo.shape, bf16), pltpu.VMEM(own.shape, bf16), pltpu.SemaphoreType.DMA((3, n)),
        ],
        compiler_params=SMALL, name="rows_local",
    )(*fetched(halo, own, rest), *held(*small))


def rows_done(got, enter, before, init, index, read16, zgate, mixed, inner, cum, gain, copies):
    rows, ch = mixed.shape
    n, _, _ = got.shape
    heads = init.shape[0]
    p = ch // heads

    def body(at, got, enter, before, init, read16, zgate, mixed, inner, cum, gain, sums, pre):
        acc_in = jnp.zeros((1, STATE), f32)
        start = enter[...]
        b = before[0:1, :]
        for j in reversed(range(n)):
            logs = jnp.sum(got[j, ch:, :].astype(f32), axis=0, keepdims=True)
            inside = (j < at[0]).astype(f32)
            start = start + got[j, :ch, :].astype(f32) * spread_heads(inside * jnp.exp(acc_in + b), heads, p)
            acc_in = acc_in + inside * logs
        start = start + init[...].reshape(ch, STATE) * spread_heads(jnp.exp(acc_in + b), heads, p)
        y = inner[...] + dot(read16[...], start.astype(bf16), 1, 1) * jnp.exp(cum[...])
        gated = y * zgate[...]
        mix = mixed[...]
        squares = jnp.concatenate([mix, mix * mix, gated * gated], 1)
        pick = lax.broadcasted_iota(jnp.int32, (8, 3 * ch), 1) // ch == lax.broadcasted_iota(jnp.int32, (8, 3 * ch), 0)
        found = dot(jnp.where(pick, 1.0, 0.0), squares, 1, 1, HIGHEST)
        for j in range(copies):
            sums[j] = found[:3]
        high = mix.astype(bf16)
        pre[:, :ch] = high
        pre[:, ch : 2 * ch] = (mix - high.astype(f32)).astype(bf16)
        pre[:, 2 * ch :] = (gated * gain[...]).astype(bf16)

    return pl.pallas_call(
        body,
        out_shape=(sds((copies, 3, rows), f32), pltpu.VMEM((rows, 3 * ch), bf16)),
        in_specs=[SMEM, *[VMEM] * 10],
        out_specs=(VMEM, VMEM),
        compiler_params=SMALL, name="rows_done",
    )(index, *held(got, enter, before, init, read16, zgate, mixed, inner, cum, gain))


def output_rows(sums, both, gains, own, other, index, nf, nt):
    copies, _, rows = sums.shape
    ch = gains.shape[1]
    d = own.shape[0]
    piece = rows // (nf * nt)

    def body(at, sref, bref, gref, wa, wb, out, cols, act):
        tp = at[0]
        s = sref[0]
        for j in range(1, copies):
            s = s + sref[j]
        cols[...] = jnp.transpose(jnp.concatenate([s, jnp.zeros((5, rows), f32)], 0))
        for i in range(nf):
            at_row = pl.multiple_of(i * (nt * piece) + tp * piece, piece)
            here = slice(i * piece, (i + 1) * piece)
            t = cols[pl.ds(at_row, piece), :]
            mean = t[:, 0:1] / C_CH
            rstd = lax.rsqrt(t[:, 1:2] / C_CH - mean * mean + EPS)
            scale = lax.rsqrt(t[:, 2:3] / D_INNER + EPS)
            for j in range(nt):
                src = tp if j == 0 else 1 - tp
                a = bref[pl.ds(pl.multiple_of(src * rows + at_row, piece), piece), :].astype(f32)
                mix = a[:, :ch] + a[:, ch : 2 * ch]
                conv = jax.nn.silu((mix - mean) * rstd * gref[pl.ds(src, 1), :])
                act[here, 2 * j * ch : (2 * j + 1) * ch] = conv.astype(bf16)
                act[here, (2 * j + 1) * ch : (2 * j + 2) * ch] = (a[:, 2 * ch :] * scale).astype(bf16)
        term = dot(act[:, : 2 * ch], wa[...], 1, 1) + dot(act[:, 2 * ch :], wb[...], 1, 1)
        out[...] = term.astype(bf16).reshape(nf, piece, d)

    return pl.pallas_call(
        body,
        out_shape=sds((nf, piece, d), bf16),
        in_specs=[SMEM, *[VMEM] * 5],
        out_specs=VMEM,
        scratch_shapes=[pltpu.VMEM((rows, 8), f32), pltpu.VMEM((nf * piece, 4 * ch), bf16)],
        compiler_params=SMALL, name="output_rows",
    )(index, *held(sums, both, gains, own, other))


def per_device(
    tokens, norm_gain, conv_value, conv_gate, mixer_gate, state_input, write_projection, state_read,
    step_proj, step_bias, decay_log, decay_extra, input_taps, write_taps, fetch_taps, long_taps,
    conv_gain, state_gain, conv_output, state_output, initial_state,
):
    rows = tokens.shape[0]
    ch = conv_value.shape[1]
    heads = step_bias.shape[0]
    p = ch // heads
    nf, nt = lax.axis_size("fs"), lax.axis_size("tp")
    iz, iy, tp = (lax.axis_index(a).astype(jnp.int32).reshape(1) for a in ("sp_0", "sp_1", "tp"))
    ny = lax.axis_size("sp_1")
    near = lay_out(
        (state_input, write_projection, state_read, mixer_gate, conv_value, conv_gate, conv_output, state_output), ny
    )
    near = lax.all_to_all(near, "sp_1", 0, 0, tiled=True)
    rest, most, last = parted(near, 2 * ch, lax.axis_size("sp_0"))
    rest = lax.all_gather(rest, "sp_0", axis=0, tiled=True)
    last = lax.all_to_all(last, "sp_0", 0, 0, tiled=True)
    most = lax.all_gather(most, "sp_0", axis=0)
    n = lax.axis_size(SP)
    halo = lax.ppermute(tokens[rows - HALO :], SP, [(i, i + 1) for i in range(n - 1)])

    def unit(x):
        v = x.astype(f32)
        return (v * lax.rsqrt(jnp.mean(v * v, axis=1, keepdims=True) + EPS) * norm_gain).astype(bf16)

    own = unit(tokens)
    halo = unit(halo)
    me = lax.axis_index("fs").astype(jnp.int32).reshape(1) * nt + tp
    step, left, cum, cum_t, total = steps_of(own, step_proj, decay_extra, step_bias, decay_log, me, p)
    gains = lax.all_gather(conv_gain, "tp")
    taps = jnp.concatenate([input_taps, write_taps], 1)
    send, xs, w16 = local_states(halo, own, most, last, taps, step, left, total, ny)
    got = lax.all_to_all(send, "sp_1", 0, 0, tiled=True)
    enter, before, send = line_states(got, iy, heads, p, lax.axis_size("sp_0"))
    got = lax.all_to_all(send, "sp_0", 0, 0, tiled=True)
    read16, zgate, mixed, inner, back = rows_local(halo, own, rest, fetch_taps, long_taps, xs, w16, cum, cum_t)
    back_other = lax.ppermute(back, "tp", [(i, nt - 1 - i) for i in range(nt)])
    sums, pre = rows_done(
        got, enter, before, initial_state, iz, read16, zgate, mixed, inner, cum, state_gain[None], nf * nt
    )
    sums = lax.all_to_all(sums, FT, 0, 0, tiled=True)
    both = lax.all_gather(pre, "tp", axis=0, tiled=True)
    out = output_rows(sums, both, gains, back, back_other, tp, nf, nt)
    pieces = lax.all_to_all(out, "fs", 0, 0, tiled=True)
    return jnp.sum(pieces.astype(f32), 0).astype(bf16)


def solution(mesh):
    torus = Mesh(
        mesh.devices.reshape(8, 8, mesh.shape["fs"], mesh.shape["tp"]), ("sp_0", "sp_1", "fs", "tp")
    )
    w = P(SP, FT)
    in_specs = (
        P(SP, None), P(), w, w, w, w, w, w, P(), P(FT), P(FT), P(FT, SP), P(None, FT), P(None, FT), P(None, FT),
        P(None, FT), P(FT), P(FT), w, w, P(FT, None, None),
    )

    return jax.shard_map(per_device, mesh=torus, in_specs=in_specs, out_specs=P((*SP, *FT), None), check_vma=False)
```

```python
import jax
import jax.numpy as jnp
from jax import lax
from jax.experimental import pallas as pl
from jax.experimental.pallas import tpu as pltpu
from jax.sharding import Mesh
from jax.sharding import PartitionSpec as P


C_CH = 1024
STATE = 128
D_INNER = 1024
WIDE = 31
SHORT = 4
HALO = 32
EPS = 1e-06
LOGS = 8
SP = ("sp_0", "sp_1")
FT = ("fs", "tp")
f32 = jnp.float32
bf16 = jnp.bfloat16
VMEM = pl.BlockSpec(memory_space=pltpu.VMEM)
SMEM = pl.BlockSpec(memory_space=pltpu.SMEM)
HIGHEST = lax.Precision.HIGHEST
SMALL = pltpu.CompilerParams(vmem_limit_bytes=12 * 2**20)


def dot(a, b, ca, cb, precision=None):
    return lax.dot_general(a, b, (((ca,), (cb,)), ((), ())), precision=precision, preferred_element_type=f32)


def sds(shape, dtype):
    return jax.ShapeDtypeStruct(shape, dtype)


def held(*arrays):
    return tuple(pltpu.with_memory_space_constraint(a, pltpu.VMEM) for a in arrays)


def fetched(*arrays):
    return tuple(pltpu.with_memory_space_constraint(a, pltpu.HBM) for a in arrays)


def lay_out(shards, copies):
    rows, ch = shards[0].shape
    n = len(shards)

    def body(*refs):
        for i in range(n):
            w = refs[i][...]
            for k in range(copies):
                refs[n][k, :, i * ch : (i + 1) * ch] = w

    return pl.pallas_call(
        body, out_shape=sds((copies, rows, n * ch), bf16), in_specs=[VMEM] * n, out_specs=VMEM, compiler_params=SMALL
    )(*fetched(*shards))


def log_rows(logs):
    hi = logs.astype(bf16).astype(f32)
    mid = (logs - hi).astype(bf16).astype(f32)
    lo = logs - hi - mid
    row = lax.broadcasted_iota(jnp.int32, (LOGS, STATE), 0)
    return jnp.where(row == 0, hi, jnp.where(row == 1, mid, jnp.where(row == 2, lo, 0.0))).astype(bf16)


def local_states(normed, first, taps, step, left, total, copies):
    ext, _ = normed.shape
    rows, ch = step.shape

    def body(nref, wref, tref, sref, lref, logs, send, xs, w16, buf):
        buf[...] = dot(nref[...], wref[...], 1, 0).astype(bf16).astype(f32)
        at = HALO - SHORT + 1
        mix = sum(buf[at + i : at + i + rows, :] * tref[i : i + 1, :] for i in range(SHORT))
        act = jax.nn.silu(mix)
        x = act[:, :ch] * sref[...]
        w = act[:, ch:].astype(bf16)
        xs[...] = x.astype(bf16)
        w16[...] = w
        ends = dot((x * lref[...]).astype(bf16), w, 0, 0).astype(bf16)
        tail = log_rows(logs[...])
        for k in range(copies):
            send[k, :ch, :] = ends
            send[k, ch:, :] = tail

    return pl.pallas_call(
        body,
        out_shape=(sds((copies, ch + LOGS, STATE), bf16), pltpu.VMEM((rows, ch), bf16), pltpu.VMEM((rows, STATE), bf16)),
        in_specs=[VMEM] * 6,
        out_specs=(VMEM,) * 3,
        scratch_shapes=[pltpu.VMEM((ext, 2 * ch), f32)],
        compiler_params=SMALL, name="local_states",
    )(*held(normed, first, taps, step, left, total))


def spread_heads(c, heads, p):
    return jnp.concatenate([jnp.broadcast_to(c[:, h : h + 1], (p, STATE)) for h in range(heads)], 0)


def line_states(got, index, heads, p, copies):
    n, size, _ = got.shape
    ch = heads * p

    def body(at, ref, enter, before, send):
        zero = jnp.zeros((1, STATE), f32)
        acc_in, acc_all = zero, zero
        ent = jnp.zeros((ch, STATE), f32)
        tot = jnp.zeros((ch, STATE), f32)
        for k in reversed(range(n)):
            logs = jnp.sum(ref[k, ch:, :].astype(f32), axis=0, keepdims=True)
            inside = (k < at[0]).astype(f32)
            piece = ref[k, :ch, :].astype(f32)
            ent = ent + piece * spread_heads(inside * jnp.exp(acc_in), heads, p)
            tot = tot + piece * spread_heads(jnp.exp(acc_all), heads, p)
            acc_in = acc_in + inside * logs
            acc_all = acc_all + logs
        enter[...] = ent
        before[...] = jnp.broadcast_to(acc_in, (8, STATE))
        line, tail = tot.astype(bf16), log_rows(acc_all)
        for k in range(copies):
            send[k, :ch, :] = line
            send[k, ch:, :] = tail

    return pl.pallas_call(
        body,
        out_shape=(pltpu.VMEM((ch, STATE), f32), pltpu.VMEM((8, STATE), f32), sds((copies, size, STATE), bf16)),
        in_specs=[SMEM, VMEM],
        out_specs=(VMEM,) * 3,
        compiler_params=SMALL, name="line_states",
    )(index, *held(got))


def rows_local(normed, rest, ftaps, ltaps, xs, w16, cum, cum_t):
    ext, d = normed.shape
    rows, ch = xs.shape
    heads = cum_t.shape[0]
    p = ch // heads
    part, n = 64, 8
    kc = d // n

    def body(nref, wref, ftaps, ltaps, xs, w16, cum, cum_t, read16, zgate, mixed, inner, back, acc, glu, wall, sems):
        def fetch(i):
            at = slice(i * kc, (i + 1) * kc)
            return pltpu.make_async_copy(wref.at[at, : 4 * ch], wall.at[at, :], sems.at[0, i])

        def fetch_back(i):
            at = slice(i * kc, (i + 1) * kc)
            return pltpu.make_async_copy(wref.at[at, 4 * ch :], back.at[at, :], sems.at[1, i])

        for i in range(n):
            fetch(i).start()
        for i in range(n):
            fetch_back(i).start()
        for i in range(n):
            fetch(i).wait()
            at = slice(i * kc, (i + 1) * kc)
            term = dot(nref[:, at], wall[at, :], 1, 0)
            acc[...] = term if i == 0 else acc[...] + term
        glu[...] = acc[:, 2 * ch : 3 * ch].astype(bf16).astype(f32) * jax.nn.sigmoid(
            acc[:, 3 * ch :].astype(bf16).astype(f32)
        )
        acc[:, : 2 * ch] = acc[:, : 2 * ch].astype(bf16).astype(f32)
        s_at, l_at = HALO - SHORT + 1, HALO - WIDE + 1
        read = sum(acc[s_at + i : s_at + i + rows, :ch] * ftaps[i : i + 1, :] for i in range(SHORT))
        read = jax.nn.silu(read).astype(bf16)
        read16[...] = read
        zgate[...] = jax.nn.silu(acc[HALO:, ch : 2 * ch])
        scores = dot(read, w16[...], 1, 1)
        lower = lax.broadcasted_iota(jnp.int32, (rows, rows), 0) >= lax.broadcasted_iota(jnp.int32, (rows, rows), 1)
        lane = lax.broadcasted_iota(jnp.int32, (rows, ch), 1)
        y = jnp.zeros((rows, ch), f32)
        for h in range(heads):
            gap = jnp.where(lower, cum[:, h * p : h * p + 1] - cum_t[h : h + 1, :], 0.0)
            m = jnp.where(lower, jnp.exp(gap) * scores, 0.0).astype(bf16)
            x = jnp.where(lane // p == h, xs[...].astype(f32), 0.0).astype(bf16)
            y = y + dot(m, x, 1, 0)
        inner[...] = y
        for r in range(0, rows, part):
            mixed[r : r + part, :] = sum(
                glu[l_at + r + i : l_at + r + i + part, :] * ltaps[i : i + 1, :] for i in range(WIDE)
            )
        for i in range(n):
            fetch_back(i).wait()

    small = (ftaps, ltaps, xs, w16, cum, cum_t)
    return pl.pallas_call(
        body,
        out_shape=(
            pltpu.VMEM((rows, STATE), bf16), pltpu.VMEM((rows, ch), f32), pltpu.VMEM((rows, ch), f32),
            pltpu.VMEM((rows, ch), f32), pltpu.VMEM((d, 2 * ch), bf16),
        ),
        in_specs=[VMEM, pl.BlockSpec(memory_space=pltpu.HBM), *[VMEM] * len(small)],
        out_specs=(VMEM,) * 5,
        scratch_shapes=[
            pltpu.VMEM((ext, 4 * ch), f32), pltpu.VMEM((ext, ch), f32), pltpu.VMEM((d, 4 * ch), bf16),
            pltpu.SemaphoreType.DMA((2, n)),
        ],
        compiler_params=SMALL, name="rows_local",
    )(*held(normed), *fetched(rest), *held(*small))


def rows_done(got, enter, before, init, index, read16, zgate, mixed, inner, cum, gain, copies):
    rows, ch = mixed.shape
    n, _, _ = got.shape
    heads = init.shape[0]
    p = ch // heads

    def body(at, got, enter, before, init, read16, zgate, mixed, inner, cum, gain, sums, pre):
        acc_in = jnp.zeros((1, STATE), f32)
        start = enter[...]
        b = before[0:1, :]
        for j in reversed(range(n)):
            logs = jnp.sum(got[j, ch:, :].astype(f32), axis=0, keepdims=True)
            inside = (j < at[0]).astype(f32)
            start = start + got[j, :ch, :].astype(f32) * spread_heads(inside * jnp.exp(acc_in + b), heads, p)
            acc_in = acc_in + inside * logs
        start = start + init[...].reshape(ch, STATE) * spread_heads(jnp.exp(acc_in + b), heads, p)
        y = inner[...] + dot(read16[...], start.astype(bf16), 1, 1) * jnp.exp(cum[...])
        gated = y * zgate[...]
        mix = mixed[...]
        squares = jnp.concatenate([mix, mix * mix, gated * gated], 1)
        pick = lax.broadcasted_iota(jnp.int32, (8, 3 * ch), 1) // ch == lax.broadcasted_iota(jnp.int32, (8, 3 * ch), 0)
        found = dot(jnp.where(pick, 1.0, 0.0), squares, 1, 1, HIGHEST)
        for j in range(copies):
            sums[j] = found[:3]
        high = mix.astype(bf16)
        pre[:, :ch] = high
        pre[:, ch : 2 * ch] = (mix - high.astype(f32)).astype(bf16)
        pre[:, 2 * ch :] = (gated * gain[...]).astype(bf16)

    return pl.pallas_call(
        body,
        out_shape=(sds((copies, 3, rows), f32), pltpu.VMEM((rows, 3 * ch), bf16)),
        in_specs=[SMEM, *[VMEM] * 10],
        out_specs=(VMEM, VMEM),
        compiler_params=SMALL, name="rows_done",
    )(index, *held(got, enter, before, init, read16, zgate, mixed, inner, cum, gain))


def output_rows(sums, both, gains, own, other, index, nf, nt):
    copies, _, rows = sums.shape
    ch = gains.shape[1]
    d = own.shape[0]
    piece = rows // (nf * nt)

    def body(at, sref, bref, gref, wa, wb, out, cols, act):
        tp = at[0]
        s = sref[0]
        for j in range(1, copies):
            s = s + sref[j]
        cols[...] = jnp.transpose(jnp.concatenate([s, jnp.zeros((5, rows), f32)], 0))
        for i in range(nf):
            at_row = pl.multiple_of(i * (nt * piece) + tp * piece, piece)
            here = slice(i * piece, (i + 1) * piece)
            t = cols[pl.ds(at_row, piece), :]
            mean = t[:, 0:1] / C_CH
            rstd = lax.rsqrt(t[:, 1:2] / C_CH - mean * mean + EPS)
            scale = lax.rsqrt(t[:, 2:3] / D_INNER + EPS)
            for j in range(nt):
                src = tp if j == 0 else 1 - tp
                a = bref[pl.ds(pl.multiple_of(src * rows + at_row, piece), piece), :].astype(f32)
                mix = a[:, :ch] + a[:, ch : 2 * ch]
                conv = jax.nn.silu((mix - mean) * rstd * gref[pl.ds(src, 1), :])
                act[here, 2 * j * ch : (2 * j + 1) * ch] = conv.astype(bf16)
                act[here, (2 * j + 1) * ch : (2 * j + 2) * ch] = (a[:, 2 * ch :] * scale).astype(bf16)
        term = dot(act[:, : 2 * ch], wa[...], 1, 1) + dot(act[:, 2 * ch :], wb[...], 1, 1)
        out[...] = term.astype(bf16).reshape(nf, piece, d)

    return pl.pallas_call(
        body,
        out_shape=sds((nf, piece, d), bf16),
        in_specs=[SMEM, *[VMEM] * 5],
        out_specs=VMEM,
        scratch_shapes=[pltpu.VMEM((rows, 8), f32), pltpu.VMEM((nf * piece, 4 * ch), bf16)],
        compiler_params=SMALL, name="output_rows",
    )(index, *held(sums, both, gains, own, other))


def per_device(
    tokens, norm_gain, conv_value, conv_gate, mixer_gate, state_input, write_projection, state_read,
    step_proj, step_bias, decay_log, decay_extra, input_taps, write_taps, fetch_taps, long_taps,
    conv_gain, state_gain, conv_output, state_output, initial_state,
):
    rows = tokens.shape[0]
    ch = conv_value.shape[1]
    heads = step_bias.shape[0]
    p = ch // heads
    nf, nt = lax.axis_size("fs"), lax.axis_size("tp")
    iz, iy, tp = (lax.axis_index(a).astype(jnp.int32).reshape(1) for a in ("sp_0", "sp_1", "tp"))
    ny = lax.axis_size("sp_1")
    rest = lay_out((state_read, mixer_gate, conv_value, conv_gate, conv_output, state_output), ny)
    rest = lax.all_to_all(rest, "sp_1", 0, 0, tiled=True).reshape(-1, 6 * ch)
    rest = lax.all_gather(rest, "sp_0", axis=0, tiled=True)
    first = lay_out((state_input, write_projection), lax.axis_size(SP))
    first = lax.all_to_all(first, SP, 0, 0, tiled=True).reshape(-1, 2 * ch)
    n = lax.axis_size(SP)
    halo = lax.ppermute(tokens[rows - HALO :], SP, [(i, i + 1) for i in range(n - 1)])
    v = jnp.concatenate([halo, tokens], 0).astype(f32)
    normed = (v * lax.rsqrt(jnp.mean(v * v, axis=1, keepdims=True) + EPS) * norm_gain).astype(bf16)
    step_all = jnp.dot(normed[HALO:], step_proj, preferred_element_type=f32)
    me = lax.axis_index("fs") * nt + lax.axis_index("tp")
    step = jax.nn.softplus(lax.dynamic_slice_in_dim(step_all, me * heads, heads, 1) + step_bias)
    log_step = (-jnp.exp(decay_log) * step + decay_extra.T).T
    cum_t = jnp.cumsum(log_step, axis=1)
    total = cum_t[:, -1]
    cum = jnp.repeat(cum_t.T, p, axis=1)
    step = jnp.repeat(step, p, axis=1)
    left = jnp.repeat(jnp.exp(total[:, None] - cum_t).T, p, axis=1)
    total = jnp.pad(total[None], ((0, 0), (0, STATE - heads)))
    gains = lax.all_gather(conv_gain, "tp")
    taps = jnp.concatenate([input_taps, write_taps], 1)
    send, xs, w16 = local_states(normed, first, taps, step, left, total, ny)
    got = lax.all_to_all(send, "sp_1", 0, 0, tiled=True)
    enter, before, send = line_states(got, iy, heads, p, lax.axis_size("sp_0"))
    got = lax.all_to_all(send, "sp_0", 0, 0, tiled=True)
    read16, zgate, mixed, inner, back = rows_local(normed, rest, fetch_taps, long_taps, xs, w16, cum, cum_t)
    back_other = lax.ppermute(back, "tp", [(i, nt - 1 - i) for i in range(nt)])
    sums, pre = rows_done(
        got, enter, before, initial_state, iz, read16, zgate, mixed, inner, cum, state_gain[None], nf * nt
    )
    sums = lax.all_to_all(sums, FT, 0, 0, tiled=True)
    both = lax.all_gather(pre, "tp", axis=0, tiled=True)
    out = output_rows(sums, both, gains, back, back_other, tp, nf, nt)
    pieces = lax.all_to_all(out, "fs", 0, 0, tiled=True)
    return jnp.sum(pieces.astype(f32), 0).astype(bf16)


def solution(mesh):
    torus = Mesh(
        mesh.devices.reshape(8, 8, mesh.shape["fs"], mesh.shape["tp"]), ("sp_0", "sp_1", "fs", "tp")
    )
    w = P(SP, FT)
    in_specs = (
        P(SP, None), P(), w, w, w, w, w, w, P(), P(FT), P(FT), P(FT, SP), P(None, FT), P(None, FT), P(None, FT),
        P(None, FT), P(FT), P(FT), w, w, P(FT, None, None),
    )

    return jax.shard_map(per_device, mesh=torus, in_specs=in_specs, out_specs=P((*SP, *FT), None), check_vma=False)
```

```python
import jax
import jax.numpy as jnp
from jax import lax
from jax.experimental import pallas as pl
from jax.experimental.pallas import tpu as pltpu
from jax.sharding import Mesh
from jax.sharding import PartitionSpec as P


C_CH = 1024
STATE = 128
D_INNER = 1024
WIDE = 31
SHORT = 4
HALO = 32
EPS = 1e-06
LOGS = 8
SP = ("sp_0", "sp_1")
FT = ("fs", "tp")
f32 = jnp.float32
bf16 = jnp.bfloat16
VMEM = pl.BlockSpec(memory_space=pltpu.VMEM)
SMEM = pl.BlockSpec(memory_space=pltpu.SMEM)
HIGHEST = lax.Precision.HIGHEST
SMALL = pltpu.CompilerParams(vmem_limit_bytes=12 * 2**20)


def dot(a, b, ca, cb, precision=None):
    return lax.dot_general(a, b, (((ca,), (cb,)), ((), ())), precision=precision, preferred_element_type=f32)


def sds(shape, dtype):
    return jax.ShapeDtypeStruct(shape, dtype)


def held(*arrays):
    return tuple(pltpu.with_memory_space_constraint(a, pltpu.VMEM) for a in arrays)


def fetched(*arrays):
    return tuple(pltpu.with_memory_space_constraint(a, pltpu.HBM) for a in arrays)


def lay_out(shards, copies):
    rows, ch = shards[0].shape
    n = len(shards)

    def body(*refs):
        for i in range(n):
            w = refs[i][...]
            for k in range(copies):
                refs[n][k, :, i * ch : (i + 1) * ch] = w

    return pl.pallas_call(
        body, out_shape=sds((copies, rows, n * ch), bf16), in_specs=[VMEM] * n, out_specs=VMEM, compiler_params=SMALL
    )(*fetched(*shards))


def first_columns(near, first, copies):
    ny, piece, _ = near.shape

    def body(ref, out):
        for y in range(ny):
            w = ref[y, :, :first]
            for k in range(copies):
                out[k, y * piece : (y + 1) * piece, :] = w

    return pl.pallas_call(
        body, out_shape=pltpu.HBM((copies, ny * piece, first), bf16), in_specs=[VMEM], out_specs=VMEM,
        compiler_params=SMALL, name="first_columns",
    )(*held(near))


def other_columns(near, first, after):
    ny, piece, width = near.shape

    def body(ref, late, out):
        for y in range(ny):
            out[y * piece : (y + 1) * piece, :] = ref[y, :, first:]

    return pl.pallas_call(
        body, out_shape=sds((ny * piece, width - first), bf16), in_specs=[VMEM, VMEM], out_specs=VMEM,
        compiler_params=SMALL, name="other_columns",
    )(*held(near, after))


def log_rows(logs):
    hi = logs.astype(bf16).astype(f32)
    mid = (logs - hi).astype(bf16).astype(f32)
    lo = logs - hi - mid
    row = lax.broadcasted_iota(jnp.int32, (LOGS, STATE), 0)
    return jnp.where(row == 0, hi, jnp.where(row == 1, mid, jnp.where(row == 2, lo, 0.0))).astype(bf16)


def steps_of(own, step_proj, extra, bias, rate_log, index, p):
    rows, _ = own.shape
    heads = extra.shape[0]
    ch = heads * p
    every = step_proj.shape[1]

    def body(at, bref, rref, nref, wref, eref, step, left, cum, cum_t, total):
        raw = dot(wref[...], nref[...], 0, 1)
        which = lax.broadcasted_iota(jnp.int32, (every, rows), 0)
        size, logs = [], []
        for h in range(heads):
            x = jnp.sum(jnp.where(which == at[0] * heads + h, raw, 0.0), axis=0, keepdims=True) + bref[h]
            size.append(jnp.maximum(x, 0.0) + jnp.log1p(jnp.exp(-jnp.abs(x))))
            logs.append(-jnp.exp(jnp.full((1, rows), rref[h], f32)) * size[h] + eref[h : h + 1, :])
        none = [jnp.zeros((8 - heads, rows), f32)]
        upto = lax.broadcasted_iota(jnp.int32, (rows, rows), 0) <= lax.broadcasted_iota(jnp.int32, (rows, rows), 1)
        run = dot(jnp.concatenate(logs + none, 0), jnp.where(upto, 1.0, 0.0), 1, 0, HIGHEST)
        lane = lax.broadcasted_iota(jnp.int32, (rows, ch), 1) // p

        def wide(cols):
            out = jnp.broadcast_to(cols[:, 0:1], (rows, ch))
            for h in range(1, heads):
                out = jnp.where(lane == h, cols[:, h : h + 1], out)
            return out

        cum_t[...] = run[:heads]
        cum[...] = wide(jnp.transpose(run))
        left[...] = wide(jnp.transpose(jnp.exp(run[:, rows - 1 :] - run)))
        step[...] = wide(jnp.transpose(jnp.concatenate(size + none, 0)))
        place = lax.broadcasted_iota(jnp.int32, (1, STATE), 1)
        ends = jnp.zeros((1, STATE), f32)
        for h in range(heads):
            ends = jnp.where(place == h, run[h : h + 1, rows - 1 :], ends)
        total[...] = ends

    wide = pltpu.VMEM((rows, ch), f32)
    return pl.pallas_call(
        body,
        out_shape=(wide, wide, wide, pltpu.VMEM((heads, rows), f32), pltpu.VMEM((1, STATE), f32)),
        in_specs=[SMEM, SMEM, SMEM, VMEM, VMEM, VMEM],
        out_specs=(VMEM,) * 5,
        compiler_params=SMALL, name="steps_of",
    )(index, bias, rate_log, *held(own, step_proj, extra))


def local_states(halo, own, first, taps, step, left, total, copies):
    rows, _ = own.shape
    ch = step.shape[1]

    def body(href, nref, wref, tref, sref, lref, logs, send, xs, w16, buf):
        buf[:HALO, :] = dot(href[...], wref[...], 1, 0).astype(bf16).astype(f32)
        buf[HALO:, :] = dot(nref[...], wref[...], 1, 0).astype(bf16).astype(f32)
        at = HALO - SHORT + 1
        mix = sum(buf[at + i : at + i + rows, :] * tref[i : i + 1, :] for i in range(SHORT))
        act = jax.nn.silu(mix)
        x = act[:, :ch] * sref[...]
        w = act[:, ch:].astype(bf16)
        xs[...] = x.astype(bf16)
        w16[...] = w
        ends = dot((x * lref[...]).astype(bf16), w, 0, 0).astype(bf16)
        tail = log_rows(logs[...])
        for k in range(copies):
            send[k, :ch, :] = ends
            send[k, ch:, :] = tail

    return pl.pallas_call(
        body,
        out_shape=(sds((copies, ch + LOGS, STATE), bf16), pltpu.VMEM((rows, ch), bf16), pltpu.VMEM((rows, STATE), bf16)),
        in_specs=[VMEM] * 7,
        out_specs=(VMEM,) * 3,
        scratch_shapes=[pltpu.VMEM((HALO + rows, 2 * ch), f32)],
        compiler_params=SMALL, name="local_states",
    )(*held(halo, own, first, taps, step, left, total))


def spread_heads(c, heads, p):
    return jnp.concatenate([jnp.broadcast_to(c[:, h : h + 1], (p, STATE)) for h in range(heads)], 0)


def line_states(got, index, heads, p, copies):
    n, size, _ = got.shape
    ch = heads * p

    def body(at, ref, enter, before, send):
        zero = jnp.zeros((1, STATE), f32)
        acc_in, acc_all = zero, zero
        ent = jnp.zeros((ch, STATE), f32)
        tot = jnp.zeros((ch, STATE), f32)
        for k in reversed(range(n)):
            logs = jnp.sum(ref[k, ch:, :].astype(f32), axis=0, keepdims=True)
            inside = (k < at[0]).astype(f32)
            piece = ref[k, :ch, :].astype(f32)
            ent = ent + piece * spread_heads(inside * jnp.exp(acc_in), heads, p)
            tot = tot + piece * spread_heads(jnp.exp(acc_all), heads, p)
            acc_in = acc_in + inside * logs
            acc_all = acc_all + logs
        enter[...] = ent
        before[...] = jnp.broadcast_to(acc_in, (8, STATE))
        line, tail = tot.astype(bf16), log_rows(acc_all)
        for k in range(copies):
            send[k, :ch, :] = line
            send[k, ch:, :] = tail

    return pl.pallas_call(
        body,
        out_shape=(pltpu.VMEM((ch, STATE), f32), pltpu.VMEM((8, STATE), f32), sds((copies, size, STATE), bf16)),
        in_specs=[SMEM, VMEM],
        out_specs=(VMEM,) * 3,
        compiler_params=SMALL, name="line_states",
    )(index, *held(got))


def rows_local(halo, own, rest, ftaps, ltaps, xs, w16, cum, cum_t):
    rows, d = own.shape
    ch = xs.shape[1]
    ext = HALO + rows
    heads = cum_t.shape[0]
    p = ch // heads
    part, n = 64, 8
    kc = d // n

    def body(
        hall, nall, wref, ftaps, ltaps, xs, w16, cum, cum_t, read16, zgate, mixed, inner, back, acc, glu, wall, href, nref, sems
    ):
        def fetch(i):
            at = slice(i * kc, (i + 1) * kc)
            return pltpu.make_async_copy(wref.at[at, : 4 * ch], wall.at[at, :], sems.at[0, i])

        def fetch_back(i):
            at = slice(i * kc, (i + 1) * kc)
            return pltpu.make_async_copy(wref.at[at, 4 * ch :], back.at[at, :], sems.at[1, i])

        near = (
            pltpu.make_async_copy(hall, href, sems.at[2, 0]),
            pltpu.make_async_copy(nall, nref, sems.at[2, 1]),
        )
        for copy in near:
            copy.start()
        for i in range(n):
            fetch(i).start()
        for i in range(n):
            fetch_back(i).start()
        for copy in near:
            copy.wait()
        for i in range(n):
            fetch(i).wait()
            at = slice(i * kc, (i + 1) * kc)
            before = dot(href[:, at], wall[at, :], 1, 0)
            term = dot(nref[:, at], wall[at, :], 1, 0)
            acc[:HALO, :] = before if i == 0 else acc[:HALO, :] + before
            acc[HALO:, :] = term if i == 0 else acc[HALO:, :] + term
        glu[...] = acc[:, 2 * ch : 3 * ch].astype(bf16).astype(f32) * jax.nn.sigmoid(
            acc[:, 3 * ch :].astype(bf16).astype(f32)
        )
        acc[:, : 2 * ch] = acc[:, : 2 * ch].astype(bf16).astype(f32)
        s_at, l_at = HALO - SHORT + 1, HALO - WIDE + 1
        read = sum(acc[s_at + i : s_at + i + rows, :ch] * ftaps[i : i + 1, :] for i in range(SHORT))
        read = jax.nn.silu(read).astype(bf16)
        read16[...] = read
        zgate[...] = jax.nn.silu(acc[HALO:, ch : 2 * ch])
        scores = dot(read, w16[...], 1, 1)
        lower = lax.broadcasted_iota(jnp.int32, (rows, rows), 0) >= lax.broadcasted_iota(jnp.int32, (rows, rows), 1)
        lane = lax.broadcasted_iota(jnp.int32, (rows, ch), 1)
        y = jnp.zeros((rows, ch), f32)
        for h in range(heads):
            gap = jnp.where(lower, cum[:, h * p : h * p + 1] - cum_t[h : h + 1, :], 0.0)
            m = jnp.where(lower, jnp.exp(gap) * scores, 0.0).astype(bf16)
            x = jnp.where(lane // p == h, xs[...].astype(f32), 0.0).astype(bf16)
            y = y + dot(m, x, 1, 0)
        inner[...] = y
        for r in range(0, rows, part):
            mixed[r : r + part, :] = sum(
                glu[l_at + r + i : l_at + r + i + part, :] * ltaps[i : i + 1, :] for i in range(WIDE)
            )
        for i in range(n):
            fetch_back(i).wait()

    small = (ftaps, ltaps, xs, w16, cum, cum_t)
    return pl.pallas_call(
        body,
        out_shape=(
            pltpu.VMEM((rows, STATE), bf16), pltpu.VMEM((rows, ch), f32), pltpu.VMEM((rows, ch), f32),
            pltpu.VMEM((rows, ch), f32), pltpu.VMEM((d, 2 * ch), bf16),
        ),
        in_specs=[*[pl.BlockSpec(memory_space=pltpu.HBM)] * 3, *[VMEM] * len(small)],
        out_specs=(VMEM,) * 5,
        scratch_shapes=[
            pltpu.VMEM((ext, 4 * ch), f32), pltpu.VMEM((ext, ch), f32), pltpu.VMEM((d, 4 * ch), bf16),
            pltpu.VMEM(halo.shape, bf16), pltpu.VMEM(own.shape, bf16), pltpu.SemaphoreType.DMA((3, n)),
        ],
        compiler_params=SMALL, name="rows_local",
    )(*fetched(halo, own, rest), *held(*small))


def rows_done(got, enter, before, init, index, read16, zgate, mixed, inner, cum, gain, copies):
    rows, ch = mixed.shape
    n, _, _ = got.shape
    heads = init.shape[0]
    p = ch // heads

    def body(at, got, enter, before, init, read16, zgate, mixed, inner, cum, gain, sums, pre):
        acc_in = jnp.zeros((1, STATE), f32)
        start = enter[...]
        b = before[0:1, :]
        for j in reversed(range(n)):
            logs = jnp.sum(got[j, ch:, :].astype(f32), axis=0, keepdims=True)
            inside = (j < at[0]).astype(f32)
            start = start + got[j, :ch, :].astype(f32) * spread_heads(inside * jnp.exp(acc_in + b), heads, p)
            acc_in = acc_in + inside * logs
        start = start + init[...].reshape(ch, STATE) * spread_heads(jnp.exp(acc_in + b), heads, p)
        y = inner[...] + dot(read16[...], start.astype(bf16), 1, 1) * jnp.exp(cum[...])
        gated = y * zgate[...]
        mix = mixed[...]
        squares = jnp.concatenate([mix, mix * mix, gated * gated], 1)
        pick = lax.broadcasted_iota(jnp.int32, (8, 3 * ch), 1) // ch == lax.broadcasted_iota(jnp.int32, (8, 3 * ch), 0)
        found = dot(jnp.where(pick, 1.0, 0.0), squares, 1, 1, HIGHEST)
        for j in range(copies):
            sums[j] = found[:3]
        high = mix.astype(bf16)
        pre[:, :ch] = high
        pre[:, ch : 2 * ch] = (mix - high.astype(f32)).astype(bf16)
        pre[:, 2 * ch :] = (gated * gain[...]).astype(bf16)

    return pl.pallas_call(
        body,
        out_shape=(sds((copies, 3, rows), f32), pltpu.VMEM((rows, 3 * ch), bf16)),
        in_specs=[SMEM, *[VMEM] * 10],
        out_specs=(VMEM, VMEM),
        compiler_params=SMALL, name="rows_done",
    )(index, *held(got, enter, before, init, read16, zgate, mixed, inner, cum, gain))


def output_rows(sums, both, gains, own, other, index, nf, nt):
    copies, _, rows = sums.shape
    ch = gains.shape[1]
    d = own.shape[0]
    piece = rows // (nf * nt)

    def body(at, sref, bref, gref, wa, wb, out, cols, act):
        tp = at[0]
        s = sref[0]
        for j in range(1, copies):
            s = s + sref[j]
        cols[...] = jnp.transpose(jnp.concatenate([s, jnp.zeros((5, rows), f32)], 0))
        for i in range(nf):
            at_row = pl.multiple_of(i * (nt * piece) + tp * piece, piece)
            here = slice(i * piece, (i + 1) * piece)
            t = cols[pl.ds(at_row, piece), :]
            mean = t[:, 0:1] / C_CH
            rstd = lax.rsqrt(t[:, 1:2] / C_CH - mean * mean + EPS)
            scale = lax.rsqrt(t[:, 2:3] / D_INNER + EPS)
            for j in range(nt):
                src = tp if j == 0 else 1 - tp
                a = bref[pl.ds(pl.multiple_of(src * rows + at_row, piece), piece), :].astype(f32)
                mix = a[:, :ch] + a[:, ch : 2 * ch]
                conv = jax.nn.silu((mix - mean) * rstd * gref[pl.ds(src, 1), :])
                act[here, 2 * j * ch : (2 * j + 1) * ch] = conv.astype(bf16)
                act[here, (2 * j + 1) * ch : (2 * j + 2) * ch] = (a[:, 2 * ch :] * scale).astype(bf16)
        term = dot(act[:, : 2 * ch], wa[...], 1, 1) + dot(act[:, 2 * ch :], wb[...], 1, 1)
        out[...] = term.astype(bf16).reshape(nf, piece, d)

    return pl.pallas_call(
        body,
        out_shape=sds((nf, piece, d), bf16),
        in_specs=[SMEM, *[VMEM] * 5],
        out_specs=VMEM,
        scratch_shapes=[pltpu.VMEM((rows, 8), f32), pltpu.VMEM((nf * piece, 4 * ch), bf16)],
        compiler_params=SMALL, name="output_rows",
    )(index, *held(sums, both, gains, own, other))


def per_device(
    tokens, norm_gain, conv_value, conv_gate, mixer_gate, state_input, write_projection, state_read,
    step_proj, step_bias, decay_log, decay_extra, input_taps, write_taps, fetch_taps, long_taps,
    conv_gain, state_gain, conv_output, state_output, initial_state,
):
    rows = tokens.shape[0]
    ch = conv_value.shape[1]
    heads = step_bias.shape[0]
    p = ch // heads
    nf, nt = lax.axis_size("fs"), lax.axis_size("tp")
    iz, iy, tp = (lax.axis_index(a).astype(jnp.int32).reshape(1) for a in ("sp_0", "sp_1", "tp"))
    ny = lax.axis_size("sp_1")
    near = lay_out(
        (state_input, write_projection, state_read, mixer_gate, conv_value, conv_gate, conv_output, state_output), ny
    )
    near = lax.all_to_all(near, "sp_1", 0, 0, tiled=True)
    first = first_columns(near, 2 * ch, lax.axis_size("sp_0"))
    first = lax.all_to_all(first, "sp_0", 0, 0, tiled=True).reshape(-1, 2 * ch)
    n = lax.axis_size(SP)
    halo = lax.ppermute(tokens[rows - HALO :], SP, [(i, i + 1) for i in range(n - 1)])

    def unit(x):
        v = x.astype(f32)
        return (v * lax.rsqrt(jnp.mean(v * v, axis=1, keepdims=True) + EPS) * norm_gain).astype(bf16)

    own = unit(tokens)
    halo = unit(halo)
    me = lax.axis_index("fs").astype(jnp.int32).reshape(1) * nt + tp
    step, left, cum, cum_t, total = steps_of(own, step_proj, decay_extra, step_bias, decay_log, me, p)
    rest = other_columns(near, 2 * ch, total)
    rest = lax.all_gather(rest, "sp_0", axis=0, tiled=True)
    gains = lax.all_gather(conv_gain, "tp")
    taps = jnp.concatenate([input_taps, write_taps], 1)
    send, xs, w16 = local_states(halo, own, first, taps, step, left, total, ny)
    got = lax.all_to_all(send, "sp_1", 0, 0, tiled=True)
    enter, before, send = line_states(got, iy, heads, p, lax.axis_size("sp_0"))
    got = lax.all_to_all(send, "sp_0", 0, 0, tiled=True)
    read16, zgate, mixed, inner, back = rows_local(halo, own, rest, fetch_taps, long_taps, xs, w16, cum, cum_t)
    back_other = lax.ppermute(back, "tp", [(i, nt - 1 - i) for i in range(nt)])
    sums, pre = rows_done(
        got, enter, before, initial_state, iz, read16, zgate, mixed, inner, cum, state_gain[None], nf * nt
    )
    sums = lax.all_to_all(sums, FT, 0, 0, tiled=True)
    both = lax.all_gather(pre, "tp", axis=0, tiled=True)
    out = output_rows(sums, both, gains, back, back_other, tp, nf, nt)
    pieces = lax.all_to_all(out, "fs", 0, 0, tiled=True)
    return jnp.sum(pieces.astype(f32), 0).astype(bf16)


def solution(mesh):
    torus = Mesh(
        mesh.devices.reshape(8, 8, mesh.shape["fs"], mesh.shape["tp"]), ("sp_0", "sp_1", "fs", "tp")
    )
    w = P(SP, FT)
    in_specs = (
        P(SP, None), P(), w, w, w, w, w, w, P(), P(FT), P(FT), P(FT, SP), P(None, FT), P(None, FT), P(None, FT),
        P(None, FT), P(FT), P(FT), w, w, P(FT, None, None),
    )

    return jax.shard_map(per_device, mesh=torus, in_specs=in_specs, out_specs=P((*SP, *FT), None), check_vma=False)
```

```python
import jax
import jax.numpy as jnp
from jax import lax
from jax.experimental import pallas as pl
from jax.experimental.pallas import tpu as pltpu
from jax.sharding import Mesh
from jax.sharding import PartitionSpec as P


C_CH = 1024
STATE = 128
D_INNER = 1024
WIDE = 31
SHORT = 4
HALO = 32
EPS = 1e-06
LOGS = 8
SP = ("sp_0", "sp_1")
FT = ("fs", "tp")
f32 = jnp.float32
bf16 = jnp.bfloat16
VMEM = pl.BlockSpec(memory_space=pltpu.VMEM)
SMEM = pl.BlockSpec(memory_space=pltpu.SMEM)
HIGHEST = lax.Precision.HIGHEST
SMALL = pltpu.CompilerParams(vmem_limit_bytes=12 * 2**20)


def dot(a, b, ca, cb, precision=None):
    return lax.dot_general(a, b, (((ca,), (cb,)), ((), ())), precision=precision, preferred_element_type=f32)


def sds(shape, dtype):
    return jax.ShapeDtypeStruct(shape, dtype)


def held(*arrays):
    return tuple(pltpu.with_memory_space_constraint(a, pltpu.VMEM) for a in arrays)


def fetched(*arrays):
    return tuple(pltpu.with_memory_space_constraint(a, pltpu.HBM) for a in arrays)


def lay_out(shards, copies):
    rows, ch = shards[0].shape
    n = len(shards)

    def body(*refs):
        for i in range(n):
            w = refs[i][...]
            for k in range(copies):
                refs[n][k, :, i * ch : (i + 1) * ch] = w

    return pl.pallas_call(
        body, out_shape=sds((copies, rows, n * ch), bf16), in_specs=[VMEM] * n, out_specs=VMEM, compiler_params=SMALL
    )(*fetched(*shards))


def log_rows(logs):
    hi = logs.astype(bf16).astype(f32)
    mid = (logs - hi).astype(bf16).astype(f32)
    lo = logs - hi - mid
    row = lax.broadcasted_iota(jnp.int32, (LOGS, STATE), 0)
    return jnp.where(row == 0, hi, jnp.where(row == 1, mid, jnp.where(row == 2, lo, 0.0))).astype(bf16)


def local_states(normed, first, taps, step, left, total, copies):
    ext, _ = normed.shape
    rows, ch = step.shape

    def body(nref, wref, tref, sref, lref, logs, send, xs, w16, buf):
        buf[...] = dot(nref[...], wref[...], 1, 0).astype(bf16).astype(f32)
        at = HALO - SHORT + 1
        mix = sum(buf[at + i : at + i + rows, :] * tref[i : i + 1, :] for i in range(SHORT))
        act = jax.nn.silu(mix)
        x = act[:, :ch] * sref[...]
        w = act[:, ch:].astype(bf16)
        xs[...] = x.astype(bf16)
        w16[...] = w
        ends = dot((x * lref[...]).astype(bf16), w, 0, 0).astype(bf16)
        tail = log_rows(logs[...])
        for k in range(copies):
            send[k, :ch, :] = ends
            send[k, ch:, :] = tail

    return pl.pallas_call(
        body,
        out_shape=(sds((copies, ch + LOGS, STATE), bf16), pltpu.VMEM((rows, ch), bf16), pltpu.VMEM((rows, STATE), bf16)),
        in_specs=[VMEM] * 6,
        out_specs=(VMEM,) * 3,
        scratch_shapes=[pltpu.VMEM((ext, 2 * ch), f32)],
        compiler_params=SMALL, name="local_states",
    )(*held(normed, first, taps, step, left, total))


def spread_heads(c, heads, p):
    return jnp.concatenate([jnp.broadcast_to(c[:, h : h + 1], (p, STATE)) for h in range(heads)], 0)


def line_states(got, index, heads, p, copies):
    n, size, _ = got.shape
    ch = heads * p

    def body(at, ref, enter, before, send):
        zero = jnp.zeros((1, STATE), f32)
        acc_in, acc_all = zero, zero
        ent = jnp.zeros((ch, STATE), f32)
        tot = jnp.zeros((ch, STATE), f32)
        for k in reversed(range(n)):
            logs = jnp.sum(ref[k, ch:, :].astype(f32), axis=0, keepdims=True)
            inside = (k < at[0]).astype(f32)
            piece = ref[k, :ch, :].astype(f32)
            ent = ent + piece * spread_heads(inside * jnp.exp(acc_in), heads, p)
            tot = tot + piece * spread_heads(jnp.exp(acc_all), heads, p)
            acc_in = acc_in + inside * logs
            acc_all = acc_all + logs
        enter[...] = ent
        before[...] = jnp.broadcast_to(acc_in, (8, STATE))
        line, tail = tot.astype(bf16), log_rows(acc_all)
        for k in range(copies):
            send[k, :ch, :] = line
            send[k, ch:, :] = tail

    return pl.pallas_call(
        body,
        out_shape=(pltpu.VMEM((ch, STATE), f32), pltpu.VMEM((8, STATE), f32), sds((copies, size, STATE), bf16)),
        in_specs=[SMEM, VMEM],
        out_specs=(VMEM,) * 3,
        compiler_params=SMALL, name="line_states",
    )(index, *held(got))


def row_sums(arrays, at):
    _, ch = arrays[0].shape
    wide = (8, len(arrays) * ch)
    pick = lax.broadcasted_iota(jnp.int32, wide, 1) // ch + at == lax.broadcasted_iota(jnp.int32, wide, 0)
    return dot(jnp.where(pick, 1.0, 0.0), jnp.concatenate(arrays, 1), 1, 1, HIGHEST)


def rows_local(normed, rest, ftaps, ltaps, xs, w16, cum, cum_t):
    ext, d = normed.shape
    rows, ch = xs.shape
    heads = cum_t.shape[0]
    p = ch // heads
    part, n = 64, 8
    kc = d // n

    def body(nref, wref, ftaps, ltaps, xs, w16, cum, cum_t, read16, zgate, mixed, inner, moments, acc, glu, wall, sems):
        def fetch(i):
            at = slice(i * kc, (i + 1) * kc)
            return pltpu.make_async_copy(wref.at[at, : 4 * ch], wall.at[at, :], sems.at[i])

        for i in range(n):
            fetch(i).start()
        for i in range(n):
            fetch(i).wait()
            at = slice(i * kc, (i + 1) * kc)
            term = dot(nref[:, at], wall[at, :], 1, 0)
            acc[...] = term if i == 0 else acc[...] + term
        glu[...] = acc[:, 2 * ch : 3 * ch].astype(bf16).astype(f32) * jax.nn.sigmoid(
            acc[:, 3 * ch :].astype(bf16).astype(f32)
        )
        acc[:, : 2 * ch] = acc[:, : 2 * ch].astype(bf16).astype(f32)
        s_at, l_at = HALO - SHORT + 1, HALO - WIDE + 1
        read = sum(acc[s_at + i : s_at + i + rows, :ch] * ftaps[i : i + 1, :] for i in range(SHORT))
        read = jax.nn.silu(read).astype(bf16)
        read16[...] = read
        zgate[...] = jax.nn.silu(acc[HALO:, ch : 2 * ch])
        scores = dot(read, w16[...], 1, 1)
        lower = lax.broadcasted_iota(jnp.int32, (rows, rows), 0) >= lax.broadcasted_iota(jnp.int32, (rows, rows), 1)
        lane = lax.broadcasted_iota(jnp.int32, (rows, ch), 1)
        y = jnp.zeros((rows, ch), f32)
        for h in range(heads):
            gap = jnp.where(lower, cum[:, h * p : h * p + 1] - cum_t[h : h + 1, :], 0.0)
            m = jnp.where(lower, jnp.exp(gap) * scores, 0.0).astype(bf16)
            x = jnp.where(lane // p == h, xs[...].astype(f32), 0.0).astype(bf16)
            y = y + dot(m, x, 1, 0)
        inner[...] = y
        mix = jnp.concatenate(
            [
                sum(glu[l_at + r + i : l_at + r + i + part, :] * ltaps[i : i + 1, :] for i in range(WIDE))
                for r in range(0, rows, part)
            ],
            0,
        )
        high = mix.astype(bf16)
        mixed[:, :ch] = high
        mixed[:, ch:] = (mix - high.astype(f32)).astype(bf16)
        moments[...] = row_sums([mix, mix * mix], 0)

    small = (ftaps, ltaps, xs, w16, cum, cum_t)
    return pl.pallas_call(
        body,
        out_shape=(
            pltpu.VMEM((rows, STATE), bf16), pltpu.VMEM((rows, ch), f32), pltpu.VMEM((rows, 2 * ch), bf16),
            pltpu.VMEM((rows, ch), f32), pltpu.VMEM((8, rows), f32),
        ),
        in_specs=[VMEM, pl.BlockSpec(memory_space=pltpu.HBM), *[VMEM] * len(small)],
        out_specs=(VMEM,) * 5,
        scratch_shapes=[
            pltpu.VMEM((ext, 4 * ch), f32), pltpu.VMEM((ext, ch), f32), pltpu.VMEM((d, 4 * ch), bf16),
            pltpu.SemaphoreType.DMA((n,)),
        ],
        compiler_params=SMALL, name="rows_local",
    )(*held(normed), *fetched(rest), *held(*small))


def rows_done(rest, got, enter, before, init, index, read16, zgate, mixed, inner, moments, cum, gain, copies):
    rows, ch = inner.shape
    d = rest.shape[0]
    parts = 4
    kc = d // parts
    n, _, _ = got.shape
    heads = init.shape[0]
    p = ch // heads

    def body(at, wref, got, enter, before, init, read16, zgate, mixed, inner, moments, cum, gain, sums, pre, back, sems):
        def fetch(i):
            here = slice(i * kc, (i + 1) * kc)
            return pltpu.make_async_copy(wref.at[here, 4 * ch :], back.at[here, :], sems.at[i])

        for i in range(parts):
            fetch(i).start()
        acc_in = jnp.zeros((1, STATE), f32)
        start = enter[...]
        b = before[0:1, :]
        for j in reversed(range(n)):
            logs = jnp.sum(got[j, ch:, :].astype(f32), axis=0, keepdims=True)
            inside = (j < at[0]).astype(f32)
            start = start + got[j, :ch, :].astype(f32) * spread_heads(inside * jnp.exp(acc_in + b), heads, p)
            acc_in = acc_in + inside * logs
        start = start + init[...].reshape(ch, STATE) * spread_heads(jnp.exp(acc_in + b), heads, p)
        y = inner[...] + dot(read16[...], start.astype(bf16), 1, 1) * jnp.exp(cum[...])
        gated = y * zgate[...]
        found = moments[...] + row_sums([gated * gated], 2)
        for j in range(copies):
            sums[j] = found[:3]
        pre[:, : 2 * ch] = mixed[...]
        pre[:, 2 * ch :] = (gated * gain[...]).astype(bf16)
        for i in range(parts):
            fetch(i).wait()

    return pl.pallas_call(
        body,
        out_shape=(sds((copies, 3, rows), f32), pltpu.VMEM((rows, 3 * ch), bf16), pltpu.VMEM((d, 2 * ch), bf16)),
        in_specs=[SMEM, pl.BlockSpec(memory_space=pltpu.HBM), *[VMEM] * 11],
        out_specs=(VMEM,) * 3,
        scratch_shapes=[pltpu.SemaphoreType.DMA((parts,))],
        compiler_params=SMALL, name="rows_done",
    )(index, *fetched(rest), *held(got, enter, before, init, read16, zgate, mixed, inner, moments, cum, gain))


def output_rows(sums, both, gains, own, other, index, nf, nt):
    copies, _, rows = sums.shape
    ch = gains.shape[1]
    d = own.shape[0]
    piece = rows // (nf * nt)

    def body(at, sref, bref, gref, wa, wb, out, cols, act):
        tp = at[0]
        s = sref[0]
        for j in range(1, copies):
            s = s + sref[j]
        cols[...] = jnp.transpose(jnp.concatenate([s, jnp.zeros((5, rows), f32)], 0))
        for i in range(nf):
            at_row = pl.multiple_of(i * (nt * piece) + tp * piece, piece)
            here = slice(i * piece, (i + 1) * piece)
            t = cols[pl.ds(at_row, piece), :]
            mean = t[:, 0:1] / C_CH
            rstd = lax.rsqrt(t[:, 1:2] / C_CH - mean * mean + EPS)
            scale = lax.rsqrt(t[:, 2:3] / D_INNER + EPS)
            for j in range(nt):
                src = tp if j == 0 else 1 - tp
                a = bref[pl.ds(pl.multiple_of(src * rows + at_row, piece), piece), :].astype(f32)
                mix = a[:, :ch] + a[:, ch : 2 * ch]
                conv = jax.nn.silu((mix - mean) * rstd * gref[pl.ds(src, 1), :])
                act[here, 2 * j * ch : (2 * j + 1) * ch] = conv.astype(bf16)
                act[here, (2 * j + 1) * ch : (2 * j + 2) * ch] = (a[:, 2 * ch :] * scale).astype(bf16)
        term = dot(act[:, : 2 * ch], wa[...], 1, 1) + dot(act[:, 2 * ch :], wb[...], 1, 1)
        out[...] = term.astype(bf16).reshape(nf, piece, d)

    return pl.pallas_call(
        body,
        out_shape=sds((nf, piece, d), bf16),
        in_specs=[SMEM, *[VMEM] * 5],
        out_specs=VMEM,
        scratch_shapes=[pltpu.VMEM((rows, 8), f32), pltpu.VMEM((nf * piece, 4 * ch), bf16)],
        compiler_params=SMALL, name="output_rows",
    )(index, *held(sums, both, gains, own, other))


def per_device(
    tokens, norm_gain, conv_value, conv_gate, mixer_gate, state_input, write_projection, state_read,
    step_proj, step_bias, decay_log, decay_extra, input_taps, write_taps, fetch_taps, long_taps,
    conv_gain, state_gain, conv_output, state_output, initial_state,
):
    rows = tokens.shape[0]
    ch = conv_value.shape[1]
    heads = step_bias.shape[0]
    p = ch // heads
    nf, nt = lax.axis_size("fs"), lax.axis_size("tp")
    iz, iy, tp = (lax.axis_index(a).astype(jnp.int32).reshape(1) for a in ("sp_0", "sp_1", "tp"))
    ny = lax.axis_size("sp_1")
    rest = lay_out((state_read, mixer_gate, conv_value, conv_gate, conv_output, state_output), ny)
    rest = lax.all_to_all(rest, "sp_1", 0, 0, tiled=True).reshape(-1, 6 * ch)
    rest = lax.all_gather(rest, "sp_0", axis=0, tiled=True)
    first = lay_out((state_input, write_projection), lax.axis_size(SP))
    first = lax.all_to_all(first, SP, 0, 0, tiled=True).reshape(-1, 2 * ch)
    n = lax.axis_size(SP)
    halo = lax.ppermute(tokens[rows - HALO :], SP, [(i, i + 1) for i in range(n - 1)])
    v = jnp.concatenate([halo, tokens], 0).astype(f32)
    normed = (v * lax.rsqrt(jnp.mean(v * v, axis=1, keepdims=True) + EPS) * norm_gain).astype(bf16)
    step_all = jnp.dot(normed[HALO:], step_proj, preferred_element_type=f32)
    me = lax.axis_index("fs") * nt + lax.axis_index("tp")
    step = jax.nn.softplus(lax.dynamic_slice_in_dim(step_all, me * heads, heads, 1) + step_bias)
    log_step = (-jnp.exp(decay_log) * step + decay_extra.T).T
    cum_t = jnp.cumsum(log_step, axis=1)
    total = cum_t[:, -1]
    cum = jnp.repeat(cum_t.T, p, axis=1)
    step = jnp.repeat(step, p, axis=1)
    left = jnp.repeat(jnp.exp(total[:, None] - cum_t).T, p, axis=1)
    total = jnp.pad(total[None], ((0, 0), (0, STATE - heads)))
    gains = lax.all_gather(conv_gain, "tp")
    taps = jnp.concatenate([input_taps, write_taps], 1)
    send, xs, w16 = local_states(normed, first, taps, step, left, total, ny)
    got = lax.all_to_all(send, "sp_1", 0, 0, tiled=True)
    enter, before, send = line_states(got, iy, heads, p, lax.axis_size("sp_0"))
    got = lax.all_to_all(send, "sp_0", 0, 0, tiled=True)
    read16, zgate, mixed, inner, moments = rows_local(normed, rest, fetch_taps, long_taps, xs, w16, cum, cum_t)
    sums, pre, back = rows_done(
        rest, got, enter, before, initial_state, iz, read16, zgate, mixed, inner, moments, cum, state_gain[None],
        nf * nt,
    )
    back_other = lax.ppermute(back, "tp", [(i, nt - 1 - i) for i in range(nt)])
    sums = lax.all_to_all(sums, FT, 0, 0, tiled=True)
    both = lax.all_gather(pre, "tp", axis=0, tiled=True)
    out = output_rows(sums, both, gains, back, back_other, tp, nf, nt)
    pieces = lax.all_to_all(out, "fs", 0, 0, tiled=True)
    return jnp.sum(pieces.astype(f32), 0).astype(bf16)


def solution(mesh):
    torus = Mesh(
        mesh.devices.reshape(8, 8, mesh.shape["fs"], mesh.shape["tp"]), ("sp_0", "sp_1", "fs", "tp")
    )
    w = P(SP, FT)
    in_specs = (
        P(SP, None), P(), w, w, w, w, w, w, P(), P(FT), P(FT), P(FT, SP), P(None, FT), P(None, FT), P(None, FT),
        P(None, FT), P(FT), P(FT), w, w, P(FT, None, None),
    )

    return jax.shard_map(per_device, mesh=torus, in_specs=in_specs, out_specs=P((*SP, *FT), None), check_vma=False)
```

```python
import jax
import jax.numpy as jnp
from jax import lax
from jax.experimental import pallas as pl
from jax.experimental.pallas import tpu as pltpu
from jax.sharding import Mesh
from jax.sharding import PartitionSpec as P


C_CH = 1024
STATE = 128
D_INNER = 1024
WIDE = 31
SHORT = 4
HALO = 32
EPS = 1e-06
LOGS = 8
SP = ("sp_0", "sp_1")
FT = ("fs", "tp")
f32 = jnp.float32
bf16 = jnp.bfloat16
VMEM = pl.BlockSpec(memory_space=pltpu.VMEM)
SMEM = pl.BlockSpec(memory_space=pltpu.SMEM)
HIGHEST = lax.Precision.HIGHEST
SMALL = pltpu.CompilerParams(vmem_limit_bytes=12 * 2**20)


def dot(a, b, ca, cb, precision=None):
    return lax.dot_general(a, b, (((ca,), (cb,)), ((), ())), precision=precision, preferred_element_type=f32)


def sds(shape, dtype):
    return jax.ShapeDtypeStruct(shape, dtype)


def held(*arrays):
    return tuple(pltpu.with_memory_space_constraint(a, pltpu.VMEM) for a in arrays)


def fetched(*arrays):
    return tuple(pltpu.with_memory_space_constraint(a, pltpu.HBM) for a in arrays)


def lay_out(shards, copies):
    rows, ch = shards[0].shape
    n = len(shards)

    def body(*refs):
        for i in range(n):
            w = refs[i][...]
            for k in range(copies):
                refs[n][k, :, i * ch : (i + 1) * ch] = w

    return pl.pallas_call(
        body, out_shape=sds((copies, rows, n * ch), bf16), in_specs=[VMEM] * n, out_specs=VMEM, compiler_params=SMALL
    )(*fetched(*shards))


def log_rows(logs):
    hi = logs.astype(bf16).astype(f32)
    mid = (logs - hi).astype(bf16).astype(f32)
    lo = logs - hi - mid
    row = lax.broadcasted_iota(jnp.int32, (LOGS, STATE), 0)
    return jnp.where(row == 0, hi, jnp.where(row == 1, mid, jnp.where(row == 2, lo, 0.0))).astype(bf16)


def steps_of(own, step_proj, extra, bias, rate_log, index, p):
    rows = own.shape[0] - HALO
    heads = extra.shape[0]
    ch = heads * p
    every = step_proj.shape[1]

    def body(at, bref, rref, nref, wref, eref, step, left, cum, cum_t, total):
        raw = dot(wref[...], nref[HALO:, :], 0, 1)
        which = lax.broadcasted_iota(jnp.int32, (every, rows), 0)
        size, logs = [], []
        for h in range(heads):
            x = jnp.sum(jnp.where(which == at[3] * heads + h, raw, 0.0), axis=0, keepdims=True) + bref[h]
            size.append(jnp.maximum(x, 0.0) + jnp.log1p(jnp.exp(-jnp.abs(x))))
            logs.append(-jnp.exp(jnp.full((1, rows), rref[h], f32)) * size[h] + eref[h : h + 1, :])
        none = [jnp.zeros((8 - heads, rows), f32)]
        upto = lax.broadcasted_iota(jnp.int32, (rows, rows), 0) <= lax.broadcasted_iota(jnp.int32, (rows, rows), 1)
        run = dot(jnp.concatenate(logs + none, 0), jnp.where(upto, 1.0, 0.0), 1, 0, HIGHEST)
        lane = lax.broadcasted_iota(jnp.int32, (rows, ch), 1) // p

        def wide(cols):
            out = jnp.broadcast_to(cols[:, 0:1], (rows, ch))
            for h in range(1, heads):
                out = jnp.where(lane == h, cols[:, h : h + 1], out)
            return out

        cum_t[...] = run[:heads]
        cum[...] = wide(jnp.transpose(run))
        left[...] = wide(jnp.transpose(jnp.exp(run[:, rows - 1 :] - run)))
        step[...] = wide(jnp.transpose(jnp.concatenate(size + none, 0)))
        place = lax.broadcasted_iota(jnp.int32, (1, STATE), 1)
        ends = jnp.zeros((1, STATE), f32)
        for h in range(heads):
            ends = jnp.where(place == h, run[h : h + 1, rows - 1 :], ends)
        total[...] = ends

    wide = pltpu.VMEM((rows, ch), f32)
    return pl.pallas_call(
        body,
        out_shape=(wide, wide, wide, pltpu.VMEM((heads, rows), f32), pltpu.VMEM((1, STATE), f32)),
        in_specs=[SMEM, SMEM, SMEM, VMEM, VMEM, VMEM],
        out_specs=(VMEM,) * 5,
        compiler_params=SMALL, name="steps_of",
    )(index, bias, rate_log, *held(own, step_proj, extra))


def local_states(normed, first, taps, step, left, total, index, copies):
    ext, _ = normed.shape
    rows, ch = step.shape

    def body(at, nref, wref, tref, sref, lref, logs, send, xs, w16, buf):
        buf[...] = dot(nref[...], wref[...], 1, 0).astype(bf16).astype(f32)
        at = HALO - SHORT + 1
        mix = sum(buf[at + i : at + i + rows, :] * tref[i : i + 1, :] for i in range(SHORT))
        act = jax.nn.silu(mix)
        x = act[:, :ch] * sref[...]
        w = act[:, ch:].astype(bf16)
        xs[...] = x.astype(bf16)
        w16[...] = w
        ends = dot((x * lref[...]).astype(bf16), w, 0, 0).astype(bf16)
        tail = log_rows(logs[...])
        for k in range(copies):
            send[k, :ch, :] = ends
            send[k, ch:, :] = tail

    return pl.pallas_call(
        body,
        out_shape=(sds((copies, ch + LOGS, STATE), bf16), pltpu.VMEM((rows, ch), bf16), pltpu.VMEM((rows, STATE), bf16)),
        in_specs=[SMEM, *[VMEM] * 6],
        out_specs=(VMEM,) * 3,
        scratch_shapes=[pltpu.VMEM((ext, 2 * ch), f32)],
        compiler_params=SMALL, name="local_states",
    )(index, *held(normed, first, taps, step, left, total))


def spread_heads(c, heads, p):
    return jnp.concatenate([jnp.broadcast_to(c[:, h : h + 1], (p, STATE)) for h in range(heads)], 0)


def line_states(got, index, heads, p, copies):
    n, size, _ = got.shape
    ch = heads * p

    def body(at, ref, enter, before, send):
        zero = jnp.zeros((1, STATE), f32)
        acc_in, acc_all = zero, zero
        ent = jnp.zeros((ch, STATE), f32)
        tot = jnp.zeros((ch, STATE), f32)
        for k in reversed(range(n)):
            logs = jnp.sum(ref[k, ch:, :].astype(f32), axis=0, keepdims=True)
            inside = (k < at[1]).astype(f32)
            piece = ref[k, :ch, :].astype(f32)
            ent = ent + piece * spread_heads(inside * jnp.exp(acc_in), heads, p)
            tot = tot + piece * spread_heads(jnp.exp(acc_all), heads, p)
            acc_in = acc_in + inside * logs
            acc_all = acc_all + logs
        enter[...] = ent
        before[...] = jnp.broadcast_to(acc_in, (8, STATE))
        line, tail = tot.astype(bf16), log_rows(acc_all)
        for k in range(copies):
            send[k, :ch, :] = line
            send[k, ch:, :] = tail

    return pl.pallas_call(
        body,
        out_shape=(pltpu.VMEM((ch, STATE), f32), pltpu.VMEM((8, STATE), f32), sds((copies, size, STATE), bf16)),
        in_specs=[SMEM, VMEM],
        out_specs=(VMEM,) * 3,
        compiler_params=SMALL, name="line_states",
    )(index, *held(got))


def rows_local(normed, rest, ftaps, ltaps, xs, w16, cum, cum_t):
    ext, d = normed.shape
    rows, ch = xs.shape
    heads = cum_t.shape[0]
    p = ch // heads
    part, n = 64, 8
    kc = d // n

    def body(nref, wref, ftaps, ltaps, xs, w16, cum, cum_t, read16, zgate, mixed, inner, back, acc, glu, wall, sems):
        def fetch(i):
            at = slice(i * kc, (i + 1) * kc)
            return pltpu.make_async_copy(wref.at[at, : 4 * ch], wall.at[at, :], sems.at[0, i])

        def fetch_back(i):
            at = slice(i * kc, (i + 1) * kc)
            return pltpu.make_async_copy(wref.at[at, 4 * ch :], back.at[at, :], sems.at[1, i])

        for i in range(n):
            fetch(i).start()
        for i in range(n):
            fetch_back(i).start()
        for i in range(n):
            fetch(i).wait()
            at = slice(i * kc, (i + 1) * kc)
            term = dot(nref[:, at], wall[at, :], 1, 0)
            acc[...] = term if i == 0 else acc[...] + term
        glu[...] = acc[:, 2 * ch : 3 * ch].astype(bf16).astype(f32) * jax.nn.sigmoid(
            acc[:, 3 * ch :].astype(bf16).astype(f32)
        )
        acc[:, : 2 * ch] = acc[:, : 2 * ch].astype(bf16).astype(f32)
        s_at, l_at = HALO - SHORT + 1, HALO - WIDE + 1
        read = sum(acc[s_at + i : s_at + i + rows, :ch] * ftaps[i : i + 1, :] for i in range(SHORT))
        read = jax.nn.silu(read).astype(bf16)
        read16[...] = read
        zgate[...] = jax.nn.silu(acc[HALO:, ch : 2 * ch])
        scores = dot(read, w16[...], 1, 1)
        lower = lax.broadcasted_iota(jnp.int32, (rows, rows), 0) >= lax.broadcasted_iota(jnp.int32, (rows, rows), 1)
        lane = lax.broadcasted_iota(jnp.int32, (rows, ch), 1)
        y = jnp.zeros((rows, ch), f32)
        for h in range(heads):
            gap = jnp.where(lower, cum[:, h * p : h * p + 1] - cum_t[h : h + 1, :], 0.0)
            m = jnp.where(lower, jnp.exp(gap) * scores, 0.0).astype(bf16)
            x = jnp.where(lane // p == h, xs[...].astype(f32), 0.0).astype(bf16)
            y = y + dot(m, x, 1, 0)
        inner[...] = y
        for r in range(0, rows, part):
            mixed[r : r + part, :] = sum(
                glu[l_at + r + i : l_at + r + i + part, :] * ltaps[i : i + 1, :] for i in range(WIDE)
            )
        for i in range(n):
            fetch_back(i).wait()

    small = (ftaps, ltaps, xs, w16, cum, cum_t)
    return pl.pallas_call(
        body,
        out_shape=(
            pltpu.VMEM((rows, STATE), bf16), pltpu.VMEM((rows, ch), f32), pltpu.VMEM((rows, ch), f32),
            pltpu.VMEM((rows, ch), f32), pltpu.VMEM((d, 2 * ch), bf16),
        ),
        in_specs=[VMEM, pl.BlockSpec(memory_space=pltpu.HBM), *[VMEM] * len(small)],
        out_specs=(VMEM,) * 5,
        scratch_shapes=[
            pltpu.VMEM((ext, 4 * ch), f32), pltpu.VMEM((ext, ch), f32), pltpu.VMEM((d, 4 * ch), bf16),
            pltpu.SemaphoreType.DMA((2, n)),
        ],
        compiler_params=SMALL, name="rows_local",
    )(*held(normed), *fetched(rest), *held(*small))


def rows_done(got, enter, before, init, index, read16, zgate, mixed, inner, cum, gain, copies):
    rows, ch = mixed.shape
    n, _, _ = got.shape
    heads = init.shape[0]
    p = ch // heads

    def body(at, got, enter, before, init, read16, zgate, mixed, inner, cum, gain, sums, pre):
        acc_in = jnp.zeros((1, STATE), f32)
        start = enter[...]
        b = before[0:1, :]
        for j in reversed(range(n)):
            logs = jnp.sum(got[j, ch:, :].astype(f32), axis=0, keepdims=True)
            inside = (j < at[0]).astype(f32)
            start = start + got[j, :ch, :].astype(f32) * spread_heads(inside * jnp.exp(acc_in + b), heads, p)
            acc_in = acc_in + inside * logs
        start = start + init[...].reshape(ch, STATE) * spread_heads(jnp.exp(acc_in + b), heads, p)
        y = inner[...] + dot(read16[...], start.astype(bf16), 1, 1) * jnp.exp(cum[...])
        gated = y * zgate[...]
        mix = mixed[...]
        squares = jnp.concatenate([mix, mix * mix, gated * gated], 1)
        pick = lax.broadcasted_iota(jnp.int32, (8, 3 * ch), 1) // ch == lax.broadcasted_iota(jnp.int32, (8, 3 * ch), 0)
        found = dot(jnp.where(pick, 1.0, 0.0), squares, 1, 1, HIGHEST)
        for j in range(copies):
            sums[j] = found[:3]
        high = mix.astype(bf16)
        pre[:, :ch] = high
        pre[:, ch : 2 * ch] = (mix - high.astype(f32)).astype(bf16)
        pre[:, 2 * ch :] = (gated * gain[...]).astype(bf16)

    return pl.pallas_call(
        body,
        out_shape=(sds((copies, 3, rows), f32), pltpu.VMEM((rows, 3 * ch), bf16)),
        in_specs=[SMEM, *[VMEM] * 10],
        out_specs=(VMEM, VMEM),
        compiler_params=SMALL, name="rows_done",
    )(index, *held(got, enter, before, init, read16, zgate, mixed, inner, cum, gain))


def output_rows(sums, both, gains, own, other, index, nf, nt):
    copies, _, rows = sums.shape
    ch = gains.shape[1]
    d = own.shape[0]
    piece = rows // (nf * nt)

    def body(at, sref, bref, gref, wa, wb, out, cols, act):
        tp = at[2]
        s = sref[0]
        for j in range(1, copies):
            s = s + sref[j]
        cols[...] = jnp.transpose(jnp.concatenate([s, jnp.zeros((5, rows), f32)], 0))
        for i in range(nf):
            at_row = pl.multiple_of(i * (nt * piece) + tp * piece, piece)
            here = slice(i * piece, (i + 1) * piece)
            t = cols[pl.ds(at_row, piece), :]
            mean = t[:, 0:1] / C_CH
            rstd = lax.rsqrt(t[:, 1:2] / C_CH - mean * mean + EPS)
            scale = lax.rsqrt(t[:, 2:3] / D_INNER + EPS)
            for j in range(nt):
                src = tp if j == 0 else 1 - tp
                a = bref[pl.ds(pl.multiple_of(src * rows + at_row, piece), piece), :].astype(f32)
                mix = a[:, :ch] + a[:, ch : 2 * ch]
                conv = jax.nn.silu((mix - mean) * rstd * gref[pl.ds(src, 1), :])
                act[here, 2 * j * ch : (2 * j + 1) * ch] = conv.astype(bf16)
                act[here, (2 * j + 1) * ch : (2 * j + 2) * ch] = (a[:, 2 * ch :] * scale).astype(bf16)
        term = dot(act[:, : 2 * ch], wa[...], 1, 1) + dot(act[:, 2 * ch :], wb[...], 1, 1)
        out[...] = term.astype(bf16).reshape(nf, piece, d)

    return pl.pallas_call(
        body,
        out_shape=sds((nf, piece, d), bf16),
        in_specs=[SMEM, *[VMEM] * 5],
        out_specs=VMEM,
        scratch_shapes=[pltpu.VMEM((rows, 8), f32), pltpu.VMEM((nf * piece, 4 * ch), bf16)],
        compiler_params=SMALL, name="output_rows",
    )(index, *held(sums, both, gains, own, other))


def per_device(
    tokens, norm_gain, conv_value, conv_gate, mixer_gate, state_input, write_projection, state_read,
    step_proj, step_bias, decay_log, decay_extra, input_taps, write_taps, fetch_taps, long_taps,
    conv_gain, state_gain, conv_output, state_output, initial_state,
):
    rows = tokens.shape[0]
    ch = conv_value.shape[1]
    heads = step_bias.shape[0]
    p = ch // heads
    nf, nt = lax.axis_size("fs"), lax.axis_size("tp")
    iz, iy, tp = (lax.axis_index(a).astype(jnp.int32) for a in ("sp_0", "sp_1", "tp"))
    at = jnp.stack([iz, iy, tp, lax.axis_index("fs").astype(jnp.int32) * nt + tp])
    ny = lax.axis_size("sp_1")
    rest = lay_out((state_read, mixer_gate, conv_value, conv_gate, conv_output, state_output), ny)
    rest = lax.all_to_all(rest, "sp_1", 0, 0, tiled=True).reshape(-1, 6 * ch)
    rest = lax.all_gather(rest, "sp_0", axis=0, tiled=True)
    first = lay_out((state_input, write_projection), lax.axis_size(SP))
    first = lax.all_to_all(first, SP, 0, 0, tiled=True).reshape(-1, 2 * ch)
    n = lax.axis_size(SP)
    halo = lax.ppermute(tokens[rows - HALO :], SP, [(i, i + 1) for i in range(n - 1)])
    v = jnp.concatenate([halo, tokens], 0).astype(f32)
    normed = (v * lax.rsqrt(jnp.mean(v * v, axis=1, keepdims=True) + EPS) * norm_gain).astype(bf16)
    step, left, cum, cum_t, total = steps_of(normed, step_proj, decay_extra, step_bias, decay_log, at, p)
    gains = lax.all_gather(conv_gain, "tp")
    taps = jnp.concatenate([input_taps, write_taps], 1)
    send, xs, w16 = local_states(normed, first, taps, step, left, total, at, ny)
    got = lax.all_to_all(send, "sp_1", 0, 0, tiled=True)
    enter, before, send = line_states(got, at, heads, p, lax.axis_size("sp_0"))
    got = lax.all_to_all(send, "sp_0", 0, 0, tiled=True)
    read16, zgate, mixed, inner, back = rows_local(normed, rest, fetch_taps, long_taps, xs, w16, cum, cum_t)
    back_other = lax.ppermute(back, "tp", [(i, nt - 1 - i) for i in range(nt)])
    sums, pre = rows_done(
        got, enter, before, initial_state, at, read16, zgate, mixed, inner, cum, state_gain[None], nf * nt
    )
    sums = lax.all_to_all(sums, FT, 0, 0, tiled=True)
    both = lax.all_gather(pre, "tp", axis=0, tiled=True)
    out = output_rows(sums, both, gains, back, back_other, at, nf, nt)
    pieces = lax.all_to_all(out, "fs", 0, 0, tiled=True)
    return jnp.sum(pieces.astype(f32), 0).astype(bf16)


def solution(mesh):
    torus = Mesh(
        mesh.devices.reshape(8, 8, mesh.shape["fs"], mesh.shape["tp"]), ("sp_0", "sp_1", "fs", "tp")
    )
    w = P(SP, FT)
    in_specs = (
        P(SP, None), P(), w, w, w, w, w, w, P(), P(FT), P(FT), P(FT, SP), P(None, FT), P(None, FT), P(None, FT),
        P(None, FT), P(FT), P(FT), w, w, P(FT, None, None),
    )

    return jax.shard_map(per_device, mesh=torus, in_specs=in_specs, out_specs=P((*SP, *FT), None), check_vma=False)
```

```python
import jax
import jax.numpy as jnp
from jax import lax
from jax.experimental import pallas as pl
from jax.experimental.pallas import tpu as pltpu
from jax.sharding import Mesh
from jax.sharding import PartitionSpec as P


C_CH = 1024
STATE = 128
D_INNER = 1024
WIDE = 31
SHORT = 4
HALO = 32
EPS = 1e-06
LOGS = 8
SP = ("sp_0", "sp_1")
FT = ("fs", "tp")
f32 = jnp.float32
bf16 = jnp.bfloat16
VMEM = pl.BlockSpec(memory_space=pltpu.VMEM)
SMEM = pl.BlockSpec(memory_space=pltpu.SMEM)
HIGHEST = lax.Precision.HIGHEST
SMALL = pltpu.CompilerParams(vmem_limit_bytes=12 * 2**20)


def dot(a, b, ca, cb, precision=None):
    return lax.dot_general(a, b, (((ca,), (cb,)), ((), ())), precision=precision, preferred_element_type=f32)


def sds(shape, dtype):
    return jax.ShapeDtypeStruct(shape, dtype)


def held(*arrays):
    return tuple(pltpu.with_memory_space_constraint(a, pltpu.VMEM) for a in arrays)


def fetched(*arrays):
    return tuple(pltpu.with_memory_space_constraint(a, pltpu.HBM) for a in arrays)


def lay_out(shards, copies):
    rows, ch = shards[0].shape
    n = len(shards)

    def body(*refs):
        for i in range(n):
            w = refs[i][...]
            for k in range(copies):
                refs[n][k, :, i * ch : (i + 1) * ch] = w

    return pl.pallas_call(
        body, out_shape=sds((copies, rows, n * ch), bf16), in_specs=[VMEM] * n, out_specs=VMEM, compiler_params=SMALL
    )(*fetched(*shards))


def log_rows(logs):
    hi = logs.astype(bf16).astype(f32)
    mid = (logs - hi).astype(bf16).astype(f32)
    lo = logs - hi - mid
    row = lax.broadcasted_iota(jnp.int32, (LOGS, STATE), 0)
    return jnp.where(row == 0, hi, jnp.where(row == 1, mid, jnp.where(row == 2, lo, 0.0))).astype(bf16)


def steps_of(own, step_proj, extra, bias, rate_log, index, p):
    rows = own.shape[0] - HALO
    heads = extra.shape[0]
    ch = heads * p
    every = step_proj.shape[1]

    def body(iz, iy, shard, tp, bref, rref, nref, wref, eref, step, left, cum, cum_t, total, at):
        raw = dot(wref[...], nref[HALO:, :], 0, 1)
        which = lax.broadcasted_iota(jnp.int32, (every, rows), 0)
        size, logs = [], []
        for h in range(heads):
            x = jnp.sum(jnp.where(which == shard[0] * heads + h, raw, 0.0), axis=0, keepdims=True) + bref[h]
            size.append(jnp.maximum(x, 0.0) + jnp.log1p(jnp.exp(-jnp.abs(x))))
            logs.append(-jnp.exp(jnp.full((1, rows), rref[h], f32)) * size[h] + eref[h : h + 1, :])
        none = [jnp.zeros((8 - heads, rows), f32)]
        upto = lax.broadcasted_iota(jnp.int32, (rows, rows), 0) <= lax.broadcasted_iota(jnp.int32, (rows, rows), 1)
        run = dot(jnp.concatenate(logs + none, 0), jnp.where(upto, 1.0, 0.0), 1, 0, HIGHEST)
        lane = lax.broadcasted_iota(jnp.int32, (rows, ch), 1) // p

        def wide(cols):
            out = jnp.broadcast_to(cols[:, 0:1], (rows, ch))
            for h in range(1, heads):
                out = jnp.where(lane == h, cols[:, h : h + 1], out)
            return out

        cum_t[...] = run[:heads]
        cum[...] = wide(jnp.transpose(run))
        left[...] = wide(jnp.transpose(jnp.exp(run[:, rows - 1 :] - run)))
        step[...] = wide(jnp.transpose(jnp.concatenate(size + none, 0)))
        place = lax.broadcasted_iota(jnp.int32, (1, STATE), 1)
        ends = jnp.zeros((1, STATE), f32)
        for h in range(heads):
            ends = jnp.where(place == h, run[h : h + 1, rows - 1 :], ends)
        total[...] = ends
        row = lax.broadcasted_iota(jnp.int32, (8, STATE), 0)
        at[...] = jnp.where(row == 0, iz[0], jnp.where(row == 1, iy[0], tp[0]))

    wide = pltpu.VMEM((rows, ch), f32)
    return pl.pallas_call(
        body,
        out_shape=(
            wide, wide, wide, pltpu.VMEM((heads, rows), f32), pltpu.VMEM((1, STATE), f32),
            pltpu.VMEM((8, STATE), jnp.int32),
        ),
        in_specs=[*[SMEM] * 6, VMEM, VMEM, VMEM],
        out_specs=(VMEM,) * 6,
        compiler_params=SMALL, name="steps_of",
    )(*index, bias, rate_log, *held(own, step_proj, extra))


def local_states(normed, first, taps, step, left, total, copies):
    ext, _ = normed.shape
    rows, ch = step.shape

    def body(nref, wref, tref, sref, lref, logs, send, xs, w16, buf):
        buf[...] = dot(nref[...], wref[...], 1, 0).astype(bf16).astype(f32)
        at = HALO - SHORT + 1
        mix = sum(buf[at + i : at + i + rows, :] * tref[i : i + 1, :] for i in range(SHORT))
        act = jax.nn.silu(mix)
        x = act[:, :ch] * sref[...]
        w = act[:, ch:].astype(bf16)
        xs[...] = x.astype(bf16)
        w16[...] = w
        ends = dot((x * lref[...]).astype(bf16), w, 0, 0).astype(bf16)
        tail = log_rows(logs[...])
        for k in range(copies):
            send[k, :ch, :] = ends
            send[k, ch:, :] = tail

    return pl.pallas_call(
        body,
        out_shape=(sds((copies, ch + LOGS, STATE), bf16), pltpu.VMEM((rows, ch), bf16), pltpu.VMEM((rows, STATE), bf16)),
        in_specs=[VMEM] * 6,
        out_specs=(VMEM,) * 3,
        scratch_shapes=[pltpu.VMEM((ext, 2 * ch), f32)],
        compiler_params=SMALL, name="local_states",
    )(*held(normed, first, taps, step, left, total))


def spread_heads(c, heads, p):
    return jnp.concatenate([jnp.broadcast_to(c[:, h : h + 1], (p, STATE)) for h in range(heads)], 0)


def line_states(got, index, heads, p, copies):
    n, size, _ = got.shape
    ch = heads * p

    def body(at, ref, enter, before, send):
        zero = jnp.zeros((1, STATE), f32)
        acc_in, acc_all = zero, zero
        ent = jnp.zeros((ch, STATE), f32)
        tot = jnp.zeros((ch, STATE), f32)
        for k in reversed(range(n)):
            logs = jnp.sum(ref[k, ch:, :].astype(f32), axis=0, keepdims=True)
            inside = jnp.where(k < at[1:2, :], 1.0, 0.0)
            piece = ref[k, :ch, :].astype(f32)
            ent = ent + piece * spread_heads(inside * jnp.exp(acc_in), heads, p)
            tot = tot + piece * spread_heads(jnp.exp(acc_all), heads, p)
            acc_in = acc_in + inside * logs
            acc_all = acc_all + logs
        enter[...] = ent
        before[...] = jnp.broadcast_to(acc_in, (8, STATE))
        line, tail = tot.astype(bf16), log_rows(acc_all)
        for k in range(copies):
            send[k, :ch, :] = line
            send[k, ch:, :] = tail

    return pl.pallas_call(
        body,
        out_shape=(pltpu.VMEM((ch, STATE), f32), pltpu.VMEM((8, STATE), f32), sds((copies, size, STATE), bf16)),
        in_specs=[VMEM, VMEM],
        out_specs=(VMEM,) * 3,
        compiler_params=SMALL, name="line_states",
    )(*held(index, got))


def rows_local(normed, rest, ftaps, ltaps, xs, w16, cum, cum_t):
    ext, d = normed.shape
    rows, ch = xs.shape
    heads = cum_t.shape[0]
    p = ch // heads
    part, n = 64, 8
    kc = d // n

    def body(nref, wref, ftaps, ltaps, xs, w16, cum, cum_t, read16, zgate, mixed, inner, back, acc, glu, wall, sems):
        def fetch(i):
            at = slice(i * kc, (i + 1) * kc)
            return pltpu.make_async_copy(wref.at[at, : 4 * ch], wall.at[at, :], sems.at[0, i])

        def fetch_back(i):
            at = slice(i * kc, (i + 1) * kc)
            return pltpu.make_async_copy(wref.at[at, 4 * ch :], back.at[at, :], sems.at[1, i])

        for i in range(n):
            fetch(i).start()
        for i in range(n):
            fetch_back(i).start()
        for i in range(n):
            fetch(i).wait()
            at = slice(i * kc, (i + 1) * kc)
            term = dot(nref[:, at], wall[at, :], 1, 0)
            acc[...] = term if i == 0 else acc[...] + term
        glu[...] = acc[:, 2 * ch : 3 * ch].astype(bf16).astype(f32) * jax.nn.sigmoid(
            acc[:, 3 * ch :].astype(bf16).astype(f32)
        )
        acc[:, : 2 * ch] = acc[:, : 2 * ch].astype(bf16).astype(f32)
        s_at, l_at = HALO - SHORT + 1, HALO - WIDE + 1
        read = sum(acc[s_at + i : s_at + i + rows, :ch] * ftaps[i : i + 1, :] for i in range(SHORT))
        read = jax.nn.silu(read).astype(bf16)
        read16[...] = read
        zgate[...] = jax.nn.silu(acc[HALO:, ch : 2 * ch])
        scores = dot(read, w16[...], 1, 1)
        lower = lax.broadcasted_iota(jnp.int32, (rows, rows), 0) >= lax.broadcasted_iota(jnp.int32, (rows, rows), 1)
        lane = lax.broadcasted_iota(jnp.int32, (rows, ch), 1)
        y = jnp.zeros((rows, ch), f32)
        for h in range(heads):
            gap = jnp.where(lower, cum[:, h * p : h * p + 1] - cum_t[h : h + 1, :], 0.0)
            m = jnp.where(lower, jnp.exp(gap) * scores, 0.0).astype(bf16)
            x = jnp.where(lane // p == h, xs[...].astype(f32), 0.0).astype(bf16)
            y = y + dot(m, x, 1, 0)
        inner[...] = y
        for r in range(0, rows, part):
            mixed[r : r + part, :] = sum(
                glu[l_at + r + i : l_at + r + i + part, :] * ltaps[i : i + 1, :] for i in range(WIDE)
            )
        for i in range(n):
            fetch_back(i).wait()

    small = (ftaps, ltaps, xs, w16, cum, cum_t)
    return pl.pallas_call(
        body,
        out_shape=(
            pltpu.VMEM((rows, STATE), bf16), pltpu.VMEM((rows, ch), f32), pltpu.VMEM((rows, ch), f32),
            pltpu.VMEM((rows, ch), f32), pltpu.VMEM((d, 2 * ch), bf16),
        ),
        in_specs=[VMEM, pl.BlockSpec(memory_space=pltpu.HBM), *[VMEM] * len(small)],
        out_specs=(VMEM,) * 5,
        scratch_shapes=[
            pltpu.VMEM((ext, 4 * ch), f32), pltpu.VMEM((ext, ch), f32), pltpu.VMEM((d, 4 * ch), bf16),
            pltpu.SemaphoreType.DMA((2, n)),
        ],
        compiler_params=SMALL, name="rows_local",
    )(*held(normed), *fetched(rest), *held(*small))


def rows_done(got, enter, before, init, index, read16, zgate, mixed, inner, cum, gain, copies):
    rows, ch = mixed.shape
    n, _, _ = got.shape
    heads = init.shape[0]
    p = ch // heads

    def body(at, got, enter, before, init, read16, zgate, mixed, inner, cum, gain, sums, pre):
        acc_in = jnp.zeros((1, STATE), f32)
        start = enter[...]
        b = before[0:1, :]
        for j in reversed(range(n)):
            logs = jnp.sum(got[j, ch:, :].astype(f32), axis=0, keepdims=True)
            inside = jnp.where(j < at[0:1, :], 1.0, 0.0)
            start = start + got[j, :ch, :].astype(f32) * spread_heads(inside * jnp.exp(acc_in + b), heads, p)
            acc_in = acc_in + inside * logs
        start = start + init[...].reshape(ch, STATE) * spread_heads(jnp.exp(acc_in + b), heads, p)
        y = inner[...] + dot(read16[...], start.astype(bf16), 1, 1) * jnp.exp(cum[...])
        gated = y * zgate[...]
        mix = mixed[...]
        cols = [jnp.sum(v, axis=1, keepdims=True) for v in (mix, mix * mix, gated * gated)]
        found = jnp.transpose(jnp.concatenate([*cols, jnp.zeros((rows, 5), f32)], 1))
        for j in range(copies):
            sums[j] = found[:3]
        high = mix.astype(bf16)
        pre[:, :ch] = high
        pre[:, ch : 2 * ch] = (mix - high.astype(f32)).astype(bf16)
        pre[:, 2 * ch :] = (gated * gain[...]).astype(bf16)

    return pl.pallas_call(
        body,
        out_shape=(sds((copies, 3, rows), f32), pltpu.VMEM((rows, 3 * ch), bf16)),
        in_specs=[VMEM] * 11,
        out_specs=(VMEM, VMEM),
        compiler_params=SMALL, name="rows_done",
    )(*held(index, got, enter, before, init, read16, zgate, mixed, inner, cum, gain))


def output_rows(sums, both, gains, own, other, index, nf, nt):
    copies, _, rows = sums.shape
    ch = gains.shape[1]
    d = own.shape[0]
    piece = rows // (nf * nt)

    def body(at, sref, bref, gref, wa, wb, out, cols, act):
        tp = at[2, 0]
        s = sref[0]
        for j in range(1, copies):
            s = s + sref[j]
        cols[...] = jnp.transpose(jnp.concatenate([s, jnp.zeros((5, rows), f32)], 0))
        for i in range(nf):
            at_row = pl.multiple_of(i * (nt * piece) + tp * piece, piece)
            here = slice(i * piece, (i + 1) * piece)
            t = cols[pl.ds(at_row, piece), :]
            mean = t[:, 0:1] / C_CH
            rstd = lax.rsqrt(t[:, 1:2] / C_CH - mean * mean + EPS)
            scale = lax.rsqrt(t[:, 2:3] / D_INNER + EPS)
            for j in range(nt):
                src = tp if j == 0 else 1 - tp
                a = bref[pl.ds(pl.multiple_of(src * rows + at_row, piece), piece), :].astype(f32)
                mix = a[:, :ch] + a[:, ch : 2 * ch]
                conv = jax.nn.silu((mix - mean) * rstd * gref[pl.ds(src, 1), :])
                act[here, 2 * j * ch : (2 * j + 1) * ch] = conv.astype(bf16)
                act[here, (2 * j + 1) * ch : (2 * j + 2) * ch] = (a[:, 2 * ch :] * scale).astype(bf16)
        term = dot(act[:, : 2 * ch], wa[...], 1, 1) + dot(act[:, 2 * ch :], wb[...], 1, 1)
        out[...] = term.astype(bf16).reshape(nf, piece, d)

    return pl.pallas_call(
        body,
        out_shape=sds((nf, piece, d), bf16),
        in_specs=[VMEM] * 6,
        out_specs=VMEM,
        scratch_shapes=[pltpu.VMEM((rows, 8), f32), pltpu.VMEM((nf * piece, 4 * ch), bf16)],
        compiler_params=SMALL, name="output_rows",
    )(*held(index, sums, both, gains, own, other))


def per_device(
    tokens, norm_gain, conv_value, conv_gate, mixer_gate, state_input, write_projection, state_read,
    step_proj, step_bias, decay_log, decay_extra, input_taps, write_taps, fetch_taps, long_taps,
    conv_gain, state_gain, conv_output, state_output, initial_state,
):
    rows = tokens.shape[0]
    ch = conv_value.shape[1]
    heads = step_bias.shape[0]
    p = ch // heads
    nf, nt = lax.axis_size("fs"), lax.axis_size("tp")
    iz, iy, ix, tp = (lax.axis_index(a).astype(jnp.int32).reshape(1) for a in ("sp_0", "sp_1", "fs", "tp"))
    ny = lax.axis_size("sp_1")
    rest = lay_out((state_read, mixer_gate, conv_value, conv_gate, conv_output, state_output), ny)
    rest = lax.all_to_all(rest, "sp_1", 0, 0, tiled=True).reshape(-1, 6 * ch)
    rest = lax.all_gather(rest, "sp_0", axis=0, tiled=True)
    first = lay_out((state_input, write_projection), lax.axis_size(SP))
    first = lax.all_to_all(first, SP, 0, 0, tiled=True).reshape(-1, 2 * ch)
    n = lax.axis_size(SP)
    halo = lax.ppermute(tokens[rows - HALO :], SP, [(i, i + 1) for i in range(n - 1)])
    v = jnp.concatenate([halo, tokens], 0).astype(f32)
    normed = (v * lax.rsqrt(jnp.mean(v * v, axis=1, keepdims=True) + EPS) * norm_gain).astype(bf16)
    step, left, cum, cum_t, total, at = steps_of(
        normed, step_proj, decay_extra, step_bias, decay_log, (iz, iy, ix * nt + tp, tp), p
    )
    gains = lax.all_gather(conv_gain, "tp")
    taps = jnp.concatenate([input_taps, write_taps], 1)
    send, xs, w16 = local_states(normed, first, taps, step, left, total, ny)
    got = lax.all_to_all(send, "sp_1", 0, 0, tiled=True)
    enter, before, send = line_states(got, at, heads, p, lax.axis_size("sp_0"))
    got = lax.all_to_all(send, "sp_0", 0, 0, tiled=True)
    read16, zgate, mixed, inner, back = rows_local(normed, rest, fetch_taps, long_taps, xs, w16, cum, cum_t)
    back_other = lax.ppermute(back, "tp", [(i, nt - 1 - i) for i in range(nt)])
    sums, pre = rows_done(
        got, enter, before, initial_state, at, read16, zgate, mixed, inner, cum, state_gain[None], nf * nt
    )
    sums = lax.all_to_all(sums, FT, 0, 0, tiled=True)
    both = lax.all_gather(pre, "tp", axis=0, tiled=True)
    out = output_rows(sums, both, gains, back, back_other, at, nf, nt)
    pieces = lax.all_to_all(out, "fs", 0, 0, tiled=True)
    return jnp.sum(pieces.astype(f32), 0).astype(bf16)


def solution(mesh):
    torus = Mesh(
        mesh.devices.reshape(8, 8, mesh.shape["fs"], mesh.shape["tp"]), ("sp_0", "sp_1", "fs", "tp")
    )
    w = P(SP, FT)
    in_specs = (
        P(SP, None), P(), w, w, w, w, w, w, P(), P(FT), P(FT), P(FT, SP), P(None, FT), P(None, FT), P(None, FT),
        P(None, FT), P(FT), P(FT), w, w, P(FT, None, None),
    )

    return jax.shard_map(per_device, mesh=torus, in_specs=in_specs, out_specs=P((*SP, *FT), None), check_vma=False)
```

```python
import jax
import jax.numpy as jnp
from jax import lax
from jax.experimental import pallas as pl
from jax.experimental.pallas import tpu as pltpu
from jax.sharding import Mesh
from jax.sharding import PartitionSpec as P


C_CH = 1024
STATE = 128
D_INNER = 1024
WIDE = 31
SHORT = 4
HALO = 32
EPS = 1e-06
LOGS = 8
SP = ("sp_0", "sp_1")
FT = ("fs", "tp")
f32 = jnp.float32
bf16 = jnp.bfloat16
VMEM = pl.BlockSpec(memory_space=pltpu.VMEM)
SMEM = pl.BlockSpec(memory_space=pltpu.SMEM)
HIGHEST = lax.Precision.HIGHEST
SMALL = pltpu.CompilerParams(vmem_limit_bytes=12 * 2**20)
LARGE = pltpu.CompilerParams(vmem_limit_bytes=64 * 2**20 - 2**17)


def dot(a, b, ca, cb, precision=None):
    return lax.dot_general(a, b, (((ca,), (cb,)), ((), ())), precision=precision, preferred_element_type=f32)


def sds(shape, dtype):
    return jax.ShapeDtypeStruct(shape, dtype)


def held(*arrays):
    return tuple(pltpu.with_memory_space_constraint(a, pltpu.VMEM) for a in arrays)


def fetched(*arrays):
    return tuple(pltpu.with_memory_space_constraint(a, pltpu.HBM) for a in arrays)


def lay_out(shards, copies, params):
    rows, ch = shards[0].shape
    n = len(shards)

    def body(*refs):
        for i in range(n):
            w = refs[i][...]
            for k in range(copies):
                refs[n][k, :, i * ch : (i + 1) * ch] = w

    return pl.pallas_call(
        body, out_shape=sds((copies, rows, n * ch), bf16), in_specs=[VMEM] * n, out_specs=VMEM, compiler_params=params
    )(*fetched(*shards))


def log_rows(logs):
    hi = logs.astype(bf16).astype(f32)
    mid = (logs - hi).astype(bf16).astype(f32)
    lo = logs - hi - mid
    row = lax.broadcasted_iota(jnp.int32, (LOGS, STATE), 0)
    return jnp.where(row == 0, hi, jnp.where(row == 1, mid, jnp.where(row == 2, lo, 0.0))).astype(bf16)


def steps_of(own, step_proj, extra, bias, rate_log, index, p):
    rows = own.shape[0] - HALO
    heads = extra.shape[0]
    ch = heads * p
    every = step_proj.shape[1]

    def body(iz, iy, shard, tp, bref, rref, nref, wref, eref, step, left, cum, cum_t, total, at):
        raw = dot(wref[...], nref[HALO:, :], 0, 1)
        which = lax.broadcasted_iota(jnp.int32, (every, rows), 0)
        size, logs = [], []
        for h in range(heads):
            x = jnp.sum(jnp.where(which == shard[0] * heads + h, raw, 0.0), axis=0, keepdims=True) + bref[h]
            size.append(jnp.maximum(x, 0.0) + jnp.log1p(jnp.exp(-jnp.abs(x))))
            logs.append(-jnp.exp(jnp.full((1, rows), rref[h], f32)) * size[h] + eref[h : h + 1, :])
        none = [jnp.zeros((8 - heads, rows), f32)]
        upto = lax.broadcasted_iota(jnp.int32, (rows, rows), 0) <= lax.broadcasted_iota(jnp.int32, (rows, rows), 1)
        run = dot(jnp.concatenate(logs + none, 0), jnp.where(upto, 1.0, 0.0), 1, 0, HIGHEST)
        lane = lax.broadcasted_iota(jnp.int32, (rows, ch), 1) // p

        def wide(cols):
            out = jnp.broadcast_to(cols[:, 0:1], (rows, ch))
            for h in range(1, heads):
                out = jnp.where(lane == h, cols[:, h : h + 1], out)
            return out

        cum_t[...] = run[:heads]
        cum[...] = wide(jnp.transpose(run))
        left[...] = wide(jnp.transpose(jnp.exp(run[:, rows - 1 :] - run)))
        step[...] = wide(jnp.transpose(jnp.concatenate(size + none, 0)))
        place = lax.broadcasted_iota(jnp.int32, (1, STATE), 1)
        ends = jnp.zeros((1, STATE), f32)
        for h in range(heads):
            ends = jnp.where(place == h, run[h : h + 1, rows - 1 :], ends)
        total[...] = ends
        row = lax.broadcasted_iota(jnp.int32, (8, STATE), 0)
        at[...] = jnp.where(row == 0, iz[0], jnp.where(row == 1, iy[0], tp[0]))

    wide = pltpu.VMEM((rows, ch), f32)
    return pl.pallas_call(
        body,
        out_shape=(
            wide, wide, wide, pltpu.VMEM((heads, rows), f32), pltpu.VMEM((1, STATE), f32),
            pltpu.VMEM((8, STATE), jnp.int32),
        ),
        in_specs=[*[SMEM] * 6, VMEM, VMEM, VMEM],
        out_specs=(VMEM,) * 6,
        compiler_params=SMALL, name="steps_of",
    )(*index, bias, rate_log, *held(own, step_proj, extra))


def local_states(normed, first, taps, step, left, total, copies):
    ext, _ = normed.shape
    rows, ch = step.shape

    def body(nref, wref, tref, sref, lref, logs, send, xs, w16, buf):
        buf[...] = dot(nref[...], wref[...], 1, 0).astype(bf16).astype(f32)
        at = HALO - SHORT + 1
        mix = sum(buf[at + i : at + i + rows, :] * tref[i : i + 1, :] for i in range(SHORT))
        act = jax.nn.silu(mix)
        x = act[:, :ch] * sref[...]
        w = act[:, ch:].astype(bf16)
        xs[...] = x.astype(bf16)
        w16[...] = w
        ends = dot((x * lref[...]).astype(bf16), w, 0, 0).astype(bf16)
        tail = log_rows(logs[...])
        for k in range(copies):
            send[k, :ch, :] = ends
            send[k, ch:, :] = tail

    return pl.pallas_call(
        body,
        out_shape=(sds((copies, ch + LOGS, STATE), bf16), pltpu.VMEM((rows, ch), bf16), pltpu.VMEM((rows, STATE), bf16)),
        in_specs=[VMEM] * 6,
        out_specs=(VMEM,) * 3,
        scratch_shapes=[pltpu.VMEM((ext, 2 * ch), f32)],
        compiler_params=SMALL, name="local_states",
    )(*held(normed, first, taps, step, left, total))


def spread_heads(c, heads, p):
    return jnp.concatenate([jnp.broadcast_to(c[:, h : h + 1], (p, STATE)) for h in range(heads)], 0)


def line_states(got, index, heads, p, copies):
    n, size, _ = got.shape
    ch = heads * p

    def body(at, ref, enter, before, send):
        zero = jnp.zeros((1, STATE), f32)
        acc_in, acc_all = zero, zero
        ent = jnp.zeros((ch, STATE), f32)
        tot = jnp.zeros((ch, STATE), f32)
        for k in reversed(range(n)):
            logs = jnp.sum(ref[k, ch:, :].astype(f32), axis=0, keepdims=True)
            inside = jnp.where(k < at[1:2, :], 1.0, 0.0)
            piece = ref[k, :ch, :].astype(f32)
            ent = ent + piece * spread_heads(inside * jnp.exp(acc_in), heads, p)
            tot = tot + piece * spread_heads(jnp.exp(acc_all), heads, p)
            acc_in = acc_in + inside * logs
            acc_all = acc_all + logs
        enter[...] = ent
        before[...] = jnp.broadcast_to(acc_in, (8, STATE))
        line, tail = tot.astype(bf16), log_rows(acc_all)
        for k in range(copies):
            send[k, :ch, :] = line
            send[k, ch:, :] = tail

    return pl.pallas_call(
        body,
        out_shape=(pltpu.VMEM((ch, STATE), f32), pltpu.VMEM((8, STATE), f32), sds((copies, size, STATE), bf16)),
        in_specs=[VMEM, VMEM],
        out_specs=(VMEM,) * 3,
        compiler_params=SMALL, name="line_states",
    )(*held(index, got))


def rows_local(normed, rest, ftaps, ltaps, xs, w16, cum, cum_t):
    ext, d = normed.shape
    rows, ch = xs.shape
    heads = cum_t.shape[0]
    p = ch // heads
    part, n = 64, 8
    kc = d // n

    def body(nref, wref, ftaps, ltaps, xs, w16, cum, cum_t, read16, zgate, mixed, inner, back, acc, glu, wall, sems):
        def fetch(i):
            at = slice(i * kc, (i + 1) * kc)
            return pltpu.make_async_copy(wref.at[at, : 4 * ch], wall.at[at, :], sems.at[0, i])

        def fetch_back(i):
            at = slice(i * kc, (i + 1) * kc)
            return pltpu.make_async_copy(wref.at[at, 4 * ch :], back.at[at, :], sems.at[1, i])

        for i in range(n):
            fetch(i).start()
        for i in range(n):
            fetch_back(i).start()
        for i in range(n):
            fetch(i).wait()
            at = slice(i * kc, (i + 1) * kc)
            term = dot(nref[:, at], wall[at, :], 1, 0)
            acc[...] = term if i == 0 else acc[...] + term
        glu[...] = acc[:, 2 * ch : 3 * ch].astype(bf16).astype(f32) * jax.nn.sigmoid(
            acc[:, 3 * ch :].astype(bf16).astype(f32)
        )
        acc[:, : 2 * ch] = acc[:, : 2 * ch].astype(bf16).astype(f32)
        s_at, l_at = HALO - SHORT + 1, HALO - WIDE + 1
        read = sum(acc[s_at + i : s_at + i + rows, :ch] * ftaps[i : i + 1, :] for i in range(SHORT))
        read = jax.nn.silu(read).astype(bf16)
        read16[...] = read
        zgate[...] = jax.nn.silu(acc[HALO:, ch : 2 * ch])
        scores = dot(read, w16[...], 1, 1)
        lower = lax.broadcasted_iota(jnp.int32, (rows, rows), 0) >= lax.broadcasted_iota(jnp.int32, (rows, rows), 1)
        lane = lax.broadcasted_iota(jnp.int32, (rows, ch), 1)
        y = jnp.zeros((rows, ch), f32)
        for h in range(heads):
            gap = jnp.where(lower, cum[:, h * p : h * p + 1] - cum_t[h : h + 1, :], 0.0)
            m = jnp.where(lower, jnp.exp(gap) * scores, 0.0).astype(bf16)
            x = jnp.where(lane // p == h, xs[...].astype(f32), 0.0).astype(bf16)
            y = y + dot(m, x, 1, 0)
        inner[...] = y
        for r in range(0, rows, part):
            mixed[r : r + part, :] = sum(
                glu[l_at + r + i : l_at + r + i + part, :] * ltaps[i : i + 1, :] for i in range(WIDE)
            )
        for i in range(n):
            fetch_back(i).wait()

    small = (ftaps, ltaps, xs, w16, cum, cum_t)
    return pl.pallas_call(
        body,
        out_shape=(
            pltpu.VMEM((rows, STATE), bf16), pltpu.VMEM((rows, ch), f32), pltpu.VMEM((rows, ch), f32),
            pltpu.VMEM((rows, ch), f32), pltpu.VMEM((d, 2 * ch), bf16),
        ),
        in_specs=[VMEM, pl.BlockSpec(memory_space=pltpu.HBM), *[VMEM] * len(small)],
        out_specs=(VMEM,) * 5,
        scratch_shapes=[
            pltpu.VMEM((ext, 4 * ch), f32), pltpu.VMEM((ext, ch), f32), pltpu.VMEM((d, 4 * ch), bf16),
            pltpu.SemaphoreType.DMA((2, n)),
        ],
        compiler_params=SMALL, name="rows_local",
    )(*held(normed), *fetched(rest), *held(*small))


def rows_done(got, enter, before, init, index, read16, zgate, mixed, inner, cum, gain, copies):
    rows, ch = mixed.shape
    n, _, _ = got.shape
    heads = init.shape[0]
    p = ch // heads

    def body(at, got, enter, before, init, read16, zgate, mixed, inner, cum, gain, sums, pre):
        acc_in = jnp.zeros((1, STATE), f32)
        start = enter[...]
        b = before[0:1, :]
        for j in reversed(range(n)):
            logs = jnp.sum(got[j, ch:, :].astype(f32), axis=0, keepdims=True)
            inside = jnp.where(j < at[0:1, :], 1.0, 0.0)
            start = start + got[j, :ch, :].astype(f32) * spread_heads(inside * jnp.exp(acc_in + b), heads, p)
            acc_in = acc_in + inside * logs
        start = start + init[...].reshape(ch, STATE) * spread_heads(jnp.exp(acc_in + b), heads, p)
        y = inner[...] + dot(read16[...], start.astype(bf16), 1, 1) * jnp.exp(cum[...])
        gated = y * zgate[...]
        mix = mixed[...]
        cols = [jnp.sum(v, axis=1, keepdims=True) for v in (mix, mix * mix, gated * gated)]
        found = jnp.transpose(jnp.concatenate([*cols, jnp.zeros((rows, 5), f32)], 1))
        for j in range(copies):
            sums[j] = found[:3]
        high = mix.astype(bf16)
        pre[:, :ch] = high
        pre[:, ch : 2 * ch] = (mix - high.astype(f32)).astype(bf16)
        pre[:, 2 * ch :] = (gated * gain[...]).astype(bf16)

    return pl.pallas_call(
        body,
        out_shape=(sds((copies, 3, rows), f32), pltpu.VMEM((rows, 3 * ch), bf16)),
        in_specs=[VMEM] * 11,
        out_specs=(VMEM, VMEM),
        compiler_params=SMALL, name="rows_done",
    )(*held(index, got, enter, before, init, read16, zgate, mixed, inner, cum, gain))


def output_rows(sums, both, gains, own, other, index, nf, nt):
    copies, _, rows = sums.shape
    ch = gains.shape[1]
    d = own.shape[0]
    piece = rows // (nf * nt)

    def body(at, sref, bref, gref, wa, wb, out, cols, act):
        tp = at[2, 0]
        s = sref[0]
        for j in range(1, copies):
            s = s + sref[j]
        cols[...] = jnp.transpose(jnp.concatenate([s, jnp.zeros((5, rows), f32)], 0))
        for i in range(nf):
            at_row = pl.multiple_of(i * (nt * piece) + tp * piece, piece)
            here = slice(i * piece, (i + 1) * piece)
            t = cols[pl.ds(at_row, piece), :]
            mean = t[:, 0:1] / C_CH
            rstd = lax.rsqrt(t[:, 1:2] / C_CH - mean * mean + EPS)
            scale = lax.rsqrt(t[:, 2:3] / D_INNER + EPS)
            for j in range(nt):
                src = tp if j == 0 else 1 - tp
                a = bref[pl.ds(pl.multiple_of(src * rows + at_row, piece), piece), :].astype(f32)
                mix = a[:, :ch] + a[:, ch : 2 * ch]
                conv = jax.nn.silu((mix - mean) * rstd * gref[pl.ds(src, 1), :])
                act[here, 2 * j * ch : (2 * j + 1) * ch] = conv.astype(bf16)
                act[here, (2 * j + 1) * ch : (2 * j + 2) * ch] = (a[:, 2 * ch :] * scale).astype(bf16)
        term = dot(act[:, : 2 * ch], wa[...], 1, 1) + dot(act[:, 2 * ch :], wb[...], 1, 1)
        out[...] = term.astype(bf16).reshape(nf, piece, d)

    return pl.pallas_call(
        body,
        out_shape=sds((nf, piece, d), bf16),
        in_specs=[VMEM] * 6,
        out_specs=VMEM,
        scratch_shapes=[pltpu.VMEM((rows, 8), f32), pltpu.VMEM((nf * piece, 4 * ch), bf16)],
        compiler_params=SMALL, name="output_rows",
    )(*held(index, sums, both, gains, own, other))


def per_device(
    tokens, norm_gain, conv_value, conv_gate, mixer_gate, state_input, write_projection, state_read,
    step_proj, step_bias, decay_log, decay_extra, input_taps, write_taps, fetch_taps, long_taps,
    conv_gain, state_gain, conv_output, state_output, initial_state,
):
    rows = tokens.shape[0]
    ch = conv_value.shape[1]
    heads = step_bias.shape[0]
    p = ch // heads
    nf, nt = lax.axis_size("fs"), lax.axis_size("tp")
    iz, iy, ix, tp = (lax.axis_index(a).astype(jnp.int32).reshape(1) for a in ("sp_0", "sp_1", "fs", "tp"))
    ny = lax.axis_size("sp_1")
    rest = lay_out((state_read, mixer_gate, conv_value, conv_gate, conv_output, state_output), ny, SMALL)
    rest = lax.all_to_all(rest, "sp_1", 0, 0, tiled=True).reshape(-1, 6 * ch)
    rest = lax.all_gather(rest, "sp_0", axis=0, tiled=True)
    first = lay_out((state_input, write_projection), lax.axis_size(SP), LARGE)
    first = lax.all_to_all(first, SP, 0, 0, tiled=True).reshape(-1, 2 * ch)
    n = lax.axis_size(SP)
    halo = lax.ppermute(tokens[rows - HALO :], SP, [(i, i + 1) for i in range(n - 1)])
    v = jnp.concatenate([halo, tokens], 0).astype(f32)
    normed = (v * lax.rsqrt(jnp.mean(v * v, axis=1, keepdims=True) + EPS) * norm_gain).astype(bf16)
    step, left, cum, cum_t, total, at = steps_of(
        normed, step_proj, decay_extra, step_bias, decay_log, (iz, iy, ix * nt + tp, tp), p
    )
    gains = lax.all_gather(conv_gain, "tp")
    taps = jnp.concatenate([input_taps, write_taps], 1)
    send, xs, w16 = local_states(normed, first, taps, step, left, total, ny)
    got = lax.all_to_all(send, "sp_1", 0, 0, tiled=True)
    enter, before, send = line_states(got, at, heads, p, lax.axis_size("sp_0"))
    got = lax.all_to_all(send, "sp_0", 0, 0, tiled=True)
    read16, zgate, mixed, inner, back = rows_local(normed, rest, fetch_taps, long_taps, xs, w16, cum, cum_t)
    back_other = lax.ppermute(back, "tp", [(i, nt - 1 - i) for i in range(nt)])
    sums, pre = rows_done(
        got, enter, before, initial_state, at, read16, zgate, mixed, inner, cum, state_gain[None], nf * nt
    )
    sums = lax.all_to_all(sums, FT, 0, 0, tiled=True)
    both = lax.all_gather(pre, "tp", axis=0, tiled=True)
    out = output_rows(sums, both, gains, back, back_other, at, nf, nt)
    pieces = lax.all_to_all(out, "fs", 0, 0, tiled=True)
    return jnp.sum(pieces.astype(f32), 0).astype(bf16)


def solution(mesh):
    torus = Mesh(
        mesh.devices.reshape(8, 8, mesh.shape["fs"], mesh.shape["tp"]), ("sp_0", "sp_1", "fs", "tp")
    )
    w = P(SP, FT)
    in_specs = (
        P(SP, None), P(), w, w, w, w, w, w, P(), P(FT), P(FT), P(FT, SP), P(None, FT), P(None, FT), P(None, FT),
        P(None, FT), P(FT), P(FT), w, w, P(FT, None, None),
    )

    return jax.shard_map(per_device, mesh=torus, in_specs=in_specs, out_specs=P((*SP, *FT), None), check_vma=False)
```

```python
import jax
import jax.numpy as jnp
from jax import lax
from jax.experimental import pallas as pl
from jax.experimental.pallas import tpu as pltpu
from jax.sharding import Mesh
from jax.sharding import PartitionSpec as P


C_CH = 1024
STATE = 128
D_INNER = 1024
WIDE = 31
SHORT = 4
HALO = 32
EPS = 1e-06
LOGS = 8
SP = ("sp_0", "sp_1")
FT = ("fs", "tp")
f32 = jnp.float32
bf16 = jnp.bfloat16
VMEM = pl.BlockSpec(memory_space=pltpu.VMEM)
SMEM = pl.BlockSpec(memory_space=pltpu.SMEM)
HIGHEST = lax.Precision.HIGHEST
SMALL = pltpu.CompilerParams(vmem_limit_bytes=12 * 2**20)
LARGE = pltpu.CompilerParams(vmem_limit_bytes=64 * 2**20 - 2**17)


def dot(a, b, ca, cb, precision=None):
    return lax.dot_general(a, b, (((ca,), (cb,)), ((), ())), precision=precision, preferred_element_type=f32)


def sds(shape, dtype):
    return jax.ShapeDtypeStruct(shape, dtype)


def held(*arrays):
    return tuple(pltpu.with_memory_space_constraint(a, pltpu.VMEM) for a in arrays)


def fetched(*arrays):
    return tuple(pltpu.with_memory_space_constraint(a, pltpu.HBM) for a in arrays)


def lay_out(shards, copies, params):
    rows, ch = shards[0].shape
    n = len(shards)

    def body(*refs):
        for i in range(n):
            w = refs[i][...]
            for k in range(copies):
                refs[n][k, :, i * ch : (i + 1) * ch] = w

    return pl.pallas_call(
        body, out_shape=sds((copies, rows, n * ch), bf16), in_specs=[VMEM] * n, out_specs=VMEM, compiler_params=params
    )(*fetched(*shards))


def log_rows(logs):
    hi = logs.astype(bf16).astype(f32)
    mid = (logs - hi).astype(bf16).astype(f32)
    lo = logs - hi - mid
    row = lax.broadcasted_iota(jnp.int32, (LOGS, STATE), 0)
    return jnp.where(row == 0, hi, jnp.where(row == 1, mid, jnp.where(row == 2, lo, 0.0))).astype(bf16)


def steps_of(own, step_proj, extra, bias, rate_log, index, p):
    rows = own.shape[0] - HALO
    heads = extra.shape[0]
    ch = heads * p
    every = step_proj.shape[1]

    def body(iz, iy, shard, tp, bref, rref, nref, wref, eref, step, left, cum, cum_t, total, at):
        raw = dot(wref[...], nref[HALO:, :], 0, 1)
        which = lax.broadcasted_iota(jnp.int32, (every, rows), 0)
        size, logs = [], []
        for h in range(heads):
            x = jnp.sum(jnp.where(which == shard[0] * heads + h, raw, 0.0), axis=0, keepdims=True) + bref[h]
            size.append(jnp.maximum(x, 0.0) + jnp.log1p(jnp.exp(-jnp.abs(x))))
            logs.append(-jnp.exp(jnp.full((1, rows), rref[h], f32)) * size[h] + eref[h : h + 1, :])
        none = [jnp.zeros((8 - heads, rows), f32)]
        upto = lax.broadcasted_iota(jnp.int32, (rows, rows), 0) <= lax.broadcasted_iota(jnp.int32, (rows, rows), 1)
        run = dot(jnp.concatenate(logs + none, 0), jnp.where(upto, 1.0, 0.0), 1, 0, HIGHEST)
        lane = lax.broadcasted_iota(jnp.int32, (rows, ch), 1) // p

        def wide(cols):
            out = jnp.broadcast_to(cols[:, 0:1], (rows, ch))
            for h in range(1, heads):
                out = jnp.where(lane == h, cols[:, h : h + 1], out)
            return out

        cum_t[...] = run[:heads]
        cum[...] = wide(jnp.transpose(run))
        left[...] = wide(jnp.transpose(jnp.exp(run[:, rows - 1 :] - run)))
        step[...] = wide(jnp.transpose(jnp.concatenate(size + none, 0)))
        place = lax.broadcasted_iota(jnp.int32, (1, STATE), 1)
        ends = jnp.zeros((1, STATE), f32)
        for h in range(heads):
            ends = jnp.where(place == h, run[h : h + 1, rows - 1 :], ends)
        total[...] = ends
        row = lax.broadcasted_iota(jnp.int32, (8, STATE), 0)
        at[...] = jnp.where(row == 0, iz[0], jnp.where(row == 1, iy[0], tp[0]))

    wide = pltpu.VMEM((rows, ch), f32)
    return pl.pallas_call(
        body,
        out_shape=(
            wide, wide, wide, pltpu.VMEM((heads, rows), f32), pltpu.VMEM((1, STATE), f32),
            pltpu.VMEM((8, STATE), jnp.int32),
        ),
        in_specs=[*[SMEM] * 6, VMEM, VMEM, VMEM],
        out_specs=(VMEM,) * 6,
        compiler_params=SMALL, name="steps_of",
    )(*index, bias, rate_log, *held(own, step_proj, extra))


def local_states(normed, first, taps, step, left, total, copies):
    ext, _ = normed.shape
    rows, ch = step.shape

    def body(nref, wref, tref, sref, lref, logs, send, xs, w16, buf):
        buf[...] = dot(nref[...], wref[...], 1, 0).astype(bf16).astype(f32)
        at = HALO - SHORT + 1
        mix = sum(buf[at + i : at + i + rows, :] * tref[i : i + 1, :] for i in range(SHORT))
        act = jax.nn.silu(mix)
        x = act[:, :ch] * sref[...]
        w = act[:, ch:].astype(bf16)
        xs[...] = x.astype(bf16)
        w16[...] = w
        ends = dot((x * lref[...]).astype(bf16), w, 0, 0).astype(bf16)
        tail = log_rows(logs[...])
        for k in range(copies):
            send[k, :ch, :] = ends
            send[k, ch:, :] = tail

    return pl.pallas_call(
        body,
        out_shape=(sds((copies, ch + LOGS, STATE), bf16), pltpu.VMEM((rows, ch), bf16), pltpu.VMEM((rows, STATE), bf16)),
        in_specs=[VMEM] * 6,
        out_specs=(VMEM,) * 3,
        scratch_shapes=[pltpu.VMEM((ext, 2 * ch), f32)],
        compiler_params=SMALL, name="local_states",
    )(*held(normed, first, taps, step, left, total))


def spread_heads(c, heads, p):
    return jnp.concatenate([jnp.broadcast_to(c[:, h : h + 1], (p, STATE)) for h in range(heads)], 0)


def line_states(got, index, heads, p, copies):
    n, size, _ = got.shape
    ch = heads * p

    def body(at, ref, enter, before, send):
        zero = jnp.zeros((1, STATE), f32)
        acc_in, acc_all = zero, zero
        ent = jnp.zeros((ch, STATE), f32)
        tot = jnp.zeros((ch, STATE), f32)
        for k in reversed(range(n)):
            logs = jnp.sum(ref[k, ch:, :].astype(f32), axis=0, keepdims=True)
            inside = jnp.where(k < at[1:2, :], 1.0, 0.0)
            piece = ref[k, :ch, :].astype(f32)
            ent = ent + piece * spread_heads(inside * jnp.exp(acc_in), heads, p)
            tot = tot + piece * spread_heads(jnp.exp(acc_all), heads, p)
            acc_in = acc_in + inside * logs
            acc_all = acc_all + logs
        enter[...] = ent
        before[...] = jnp.broadcast_to(acc_in, (8, STATE))
        line, tail = tot.astype(bf16), log_rows(acc_all)
        for k in range(copies):
            send[k, :ch, :] = line
            send[k, ch:, :] = tail

    return pl.pallas_call(
        body,
        out_shape=(pltpu.VMEM((ch, STATE), f32), pltpu.VMEM((8, STATE), f32), sds((copies, size, STATE), bf16)),
        in_specs=[VMEM, VMEM],
        out_specs=(VMEM,) * 3,
        compiler_params=SMALL, name="line_states",
    )(*held(index, got))


def rows_local(normed, rest, ftaps, ltaps, xs, w16, cum, cum_t):
    ext, d = normed.shape
    rows, ch = xs.shape
    heads = cum_t.shape[0]
    p = ch // heads
    part, n = 64, 8
    kc = d // n

    def body(nref, wref, ftaps, ltaps, xs, w16, cum, cum_t, read16, zgate, mixed, inner, back, acc, glu, wall, sems):
        def fetch(i):
            at = slice(i * kc, (i + 1) * kc)
            return pltpu.make_async_copy(wref.at[at, : 4 * ch], wall.at[at, :], sems.at[0, i])

        def fetch_back(i):
            at = slice(i * kc, (i + 1) * kc)
            return pltpu.make_async_copy(wref.at[at, 4 * ch :], back.at[at, :], sems.at[1, i])

        for i in range(n):
            fetch(i).start()
        for i in range(n):
            fetch_back(i).start()
        for i in range(n):
            fetch(i).wait()
            at = slice(i * kc, (i + 1) * kc)
            term = dot(nref[:, at], wall[at, :], 1, 0)
            acc[...] = term if i == 0 else acc[...] + term
        glu[...] = acc[:, 2 * ch : 3 * ch].astype(bf16).astype(f32) * jax.nn.sigmoid(
            acc[:, 3 * ch :].astype(bf16).astype(f32)
        )
        acc[:, : 2 * ch] = acc[:, : 2 * ch].astype(bf16).astype(f32)
        s_at, l_at = HALO - SHORT + 1, HALO - WIDE + 1
        read = sum(acc[s_at + i : s_at + i + rows, :ch] * ftaps[i : i + 1, :] for i in range(SHORT))
        read = jax.nn.silu(read).astype(bf16)
        read16[...] = read
        zgate[...] = jax.nn.silu(acc[HALO:, ch : 2 * ch])
        scores = dot(read, w16[...], 1, 1)
        lower = lax.broadcasted_iota(jnp.int32, (rows, rows), 0) >= lax.broadcasted_iota(jnp.int32, (rows, rows), 1)
        lane = lax.broadcasted_iota(jnp.int32, (rows, ch), 1)
        y = jnp.zeros((rows, ch), f32)
        for h in range(heads):
            gap = jnp.where(lower, cum[:, h * p : h * p + 1] - cum_t[h : h + 1, :], 0.0)
            m = jnp.where(lower, jnp.exp(gap) * scores, 0.0).astype(bf16)
            x = jnp.where(lane // p == h, xs[...].astype(f32), 0.0).astype(bf16)
            y = y + dot(m, x, 1, 0)
        inner[...] = y
        for r in range(0, rows, part):
            mixed[r : r + part, :] = sum(
                glu[l_at + r + i : l_at + r + i + part, :] * ltaps[i : i + 1, :] for i in range(WIDE)
            )
        for i in range(n):
            fetch_back(i).wait()

    small = (ftaps, ltaps, xs, w16, cum, cum_t)
    return pl.pallas_call(
        body,
        out_shape=(
            pltpu.VMEM((rows, STATE), bf16), pltpu.VMEM((rows, ch), f32), pltpu.VMEM((rows, ch), f32),
            pltpu.VMEM((rows, ch), f32), pltpu.VMEM((d + 3 * rows // 4, 2 * ch), bf16),
        ),
        in_specs=[VMEM, pl.BlockSpec(memory_space=pltpu.HBM), *[VMEM] * len(small)],
        out_specs=(VMEM,) * 5,
        scratch_shapes=[
            pltpu.VMEM((ext, 4 * ch), f32), pltpu.VMEM((ext, ch), f32), pltpu.VMEM((d, 4 * ch), bf16),
            pltpu.SemaphoreType.DMA((2, n)),
        ],
        compiler_params=SMALL, name="rows_local",
    )(*held(normed), *fetched(rest), *held(*small))


def rows_done(got, enter, before, init, index, read16, zgate, mixed, inner, cum, gain, back, nf, nt):
    rows, ch = mixed.shape
    n, _, _ = got.shape
    heads = init.shape[0]
    p = ch // heads
    half, piece = rows // 2, rows // (nf * nt)
    d = back.shape[0] - 3 * rows // 4

    def body(at, got, enter, before, init, read16, zgate, mixed, inner, cum, gain, _, sums, pack, keep, last):
        acc_in = jnp.zeros((1, STATE), f32)
        start = enter[...]
        b = before[0:1, :]
        for j in reversed(range(n)):
            logs = jnp.sum(got[j, ch:, :].astype(f32), axis=0, keepdims=True)
            inside = jnp.where(j < at[0:1, :], 1.0, 0.0)
            start = start + got[j, :ch, :].astype(f32) * spread_heads(inside * jnp.exp(acc_in + b), heads, p)
            acc_in = acc_in + inside * logs
        start = start + init[...].reshape(ch, STATE) * spread_heads(jnp.exp(acc_in + b), heads, p)
        y = inner[...] + dot(read16[...], start.astype(bf16), 1, 1) * jnp.exp(cum[...])
        gated = y * zgate[...]
        mix = mixed[...]
        cols = [jnp.sum(v, axis=1, keepdims=True) for v in (mix, mix * mix, gated * gated)]
        found = jnp.transpose(jnp.concatenate([*cols, jnp.zeros((rows, 5), f32)], 1))
        for j in range(nf * nt):
            sums[j] = found[:3]
        last[...] = gated * gain[...]
        tp = at[2, 0]

        def values(start):
            rows_at = pl.ds(pl.multiple_of(start, piece), piece)
            high = mixed[rows_at, :].astype(bf16)
            return high, (mixed[rows_at, :] - high.astype(f32)).astype(bf16), last[rows_at, :].astype(bf16)

        for i in range(nf):
            here = slice(i * piece, (i + 1) * piece)
            for k, v in enumerate(values(i * (nt * piece) + tp * piece)):
                keep[here, k * ch : (k + 1) * ch] = v
            high, low, scaled = values(i * (nt * piece) + (1 - tp) * piece)
            pack[d + i * piece : d + (i + 1) * piece, :ch] = high
            pack[d + i * piece : d + (i + 1) * piece, ch:] = low
            right, up = divmod(i * piece, half // 2)
            pack[d + half + up : d + half + up + piece, right * ch : (right + 1) * ch] = scaled

    return pl.pallas_call(
        body,
        out_shape=(sds((nf * nt, 3, rows), f32), pltpu.VMEM(back.shape, bf16), pltpu.VMEM((half, 3 * ch), bf16)),
        in_specs=[VMEM] * 12,
        out_specs=(VMEM,) * 3,
        input_output_aliases={11: 1},
        scratch_shapes=[pltpu.VMEM((rows, ch), f32)],
        compiler_params=SMALL, name="rows_done",
    )(*held(index, got, enter, before, init, read16, zgate, mixed, inner, cum, gain, back))


def output_rows(sums, gains, keep, own, other, index, nf, nt):
    copies, _, rows = sums.shape
    ch = gains.shape[1]
    half = rows // 2
    d = own.shape[0] - 3 * rows // 4
    piece = rows // (nf * nt)

    def body(at, sref, gref, keep, own, other, out, cols, act):
        tp = at[2, 0]
        s = sref[0]
        for j in range(1, copies):
            s = s + sref[j]
        cols[...] = jnp.transpose(jnp.concatenate([s, jnp.zeros((5, rows), f32)], 0))
        for i in range(nf):
            at_row = pl.multiple_of(i * (nt * piece) + tp * piece, piece)
            here = slice(i * piece, (i + 1) * piece)
            t = cols[pl.ds(at_row, piece), :]
            mean = t[:, 0:1] / C_CH
            rstd = lax.rsqrt(t[:, 1:2] / C_CH - mean * mean + EPS)
            scale = lax.rsqrt(t[:, 2:3] / D_INNER + EPS)
            right, up = divmod(i * piece, half // 2)
            mine = [keep[here, k * ch : (k + 1) * ch] for k in range(3)]
            got = other[d + i * piece : d + (i + 1) * piece, :]
            last = other[d + half + up : d + half + up + piece, right * ch : (right + 1) * ch]
            for j, (high, low, gated) in enumerate((mine, (got[:, :ch], got[:, ch:], last))):
                src = tp if j == 0 else 1 - tp
                mix = high.astype(f32) + low.astype(f32)
                conv = jax.nn.silu((mix - mean) * rstd * gref[pl.ds(src, 1), :])
                act[here, 2 * j * ch : (2 * j + 1) * ch] = conv.astype(bf16)
                act[here, (2 * j + 1) * ch : (2 * j + 2) * ch] = (gated.astype(f32) * scale).astype(bf16)
        term = dot(act[:, : 2 * ch], own[:d, :], 1, 1) + dot(act[:, 2 * ch :], other[:d, :], 1, 1)
        out[...] = term.astype(bf16).reshape(nf, piece, d)

    return pl.pallas_call(
        body,
        out_shape=sds((nf, piece, d), bf16),
        in_specs=[VMEM] * 6,
        out_specs=VMEM,
        scratch_shapes=[pltpu.VMEM((rows, 8), f32), pltpu.VMEM((nf * piece, 4 * ch), bf16)],
        compiler_params=SMALL, name="output_rows",
    )(*held(index, sums, gains, keep, own, other))


def per_device(
    tokens, norm_gain, conv_value, conv_gate, mixer_gate, state_input, write_projection, state_read,
    step_proj, step_bias, decay_log, decay_extra, input_taps, write_taps, fetch_taps, long_taps,
    conv_gain, state_gain, conv_output, state_output, initial_state,
):
    rows = tokens.shape[0]
    ch = conv_value.shape[1]
    heads = step_bias.shape[0]
    p = ch // heads
    nf, nt = lax.axis_size("fs"), lax.axis_size("tp")
    iz, iy, ix, tp = (lax.axis_index(a).astype(jnp.int32).reshape(1) for a in ("sp_0", "sp_1", "fs", "tp"))
    ny = lax.axis_size("sp_1")
    rest = lay_out((state_read, mixer_gate, conv_value, conv_gate, conv_output, state_output), ny, SMALL)
    rest = lax.all_to_all(rest, "sp_1", 0, 0, tiled=True).reshape(-1, 6 * ch)
    rest = lax.all_gather(rest, "sp_0", axis=0, tiled=True)
    first = lay_out((state_input, write_projection), lax.axis_size(SP), LARGE)
    first = lax.all_to_all(first, SP, 0, 0, tiled=True).reshape(-1, 2 * ch)
    n = lax.axis_size(SP)
    halo = lax.ppermute(tokens[rows - HALO :], SP, [(i, i + 1) for i in range(n - 1)])
    v = jnp.concatenate([halo, tokens], 0).astype(f32)
    normed = (v * lax.rsqrt(jnp.mean(v * v, axis=1, keepdims=True) + EPS) * norm_gain).astype(bf16)
    step, left, cum, cum_t, total, at = steps_of(
        normed, step_proj, decay_extra, step_bias, decay_log, (iz, iy, ix * nt + tp, tp), p
    )
    gains = lax.all_gather(conv_gain, "tp")
    taps = jnp.concatenate([input_taps, write_taps], 1)
    send, xs, w16 = local_states(normed, first, taps, step, left, total, ny)
    got = lax.all_to_all(send, "sp_1", 0, 0, tiled=True)
    enter, before, send = line_states(got, at, heads, p, lax.axis_size("sp_0"))
    got = lax.all_to_all(send, "sp_0", 0, 0, tiled=True)
    read16, zgate, mixed, inner, back = rows_local(normed, rest, fetch_taps, long_taps, xs, w16, cum, cum_t)
    sums, pack, keep = rows_done(
        got, enter, before, initial_state, at, read16, zgate, mixed, inner, cum, state_gain[None], back, nf, nt
    )
    sums = lax.all_to_all(sums, FT, 0, 0, tiled=True)
    other = lax.ppermute(pack, "tp", [(i, nt - 1 - i) for i in range(nt)])
    out = output_rows(sums, gains, keep, pack, other, at, nf, nt)
    pieces = lax.all_to_all(out, "fs", 0, 0, tiled=True)
    return jnp.sum(pieces.astype(f32), 0).astype(bf16)


def solution(mesh):
    torus = Mesh(
        mesh.devices.reshape(8, 8, mesh.shape["fs"], mesh.shape["tp"]), ("sp_0", "sp_1", "fs", "tp")
    )
    w = P(SP, FT)
    in_specs = (
        P(SP, None), P(), w, w, w, w, w, w, P(), P(FT), P(FT), P(FT, SP), P(None, FT), P(None, FT), P(None, FT),
        P(None, FT), P(FT), P(FT), w, w, P(FT, None, None),
    )

    return jax.shard_map(per_device, mesh=torus, in_specs=in_specs, out_specs=P((*SP, *FT), None), check_vma=False)
```

```python
import jax
import jax.numpy as jnp
from jax import lax
from jax.experimental import pallas as pl
from jax.experimental.pallas import tpu as pltpu
from jax.sharding import Mesh
from jax.sharding import PartitionSpec as P


C_CH = 1024
STATE = 128
D_INNER = 1024
WIDE = 31
SHORT = 4
HALO = 32
EPS = 1e-06
LOGS = 8
SP = ("sp_0", "sp_1")
FT = ("fs", "tp")
f32 = jnp.float32
bf16 = jnp.bfloat16
VMEM = pl.BlockSpec(memory_space=pltpu.VMEM)
SMEM = pl.BlockSpec(memory_space=pltpu.SMEM)
HIGHEST = lax.Precision.HIGHEST
SMALL = pltpu.CompilerParams(vmem_limit_bytes=12 * 2**20)
LARGE = pltpu.CompilerParams(vmem_limit_bytes=64 * 2**20 - 2**17)


def dot(a, b, ca, cb, precision=None):
    return lax.dot_general(a, b, (((ca,), (cb,)), ((), ())), precision=precision, preferred_element_type=f32)


def sds(shape, dtype):
    return jax.ShapeDtypeStruct(shape, dtype)


def held(*arrays):
    return tuple(pltpu.with_memory_space_constraint(a, pltpu.VMEM) for a in arrays)


def fetched(*arrays):
    return tuple(pltpu.with_memory_space_constraint(a, pltpu.HBM) for a in arrays)


def lay_out(shards, copies, params):
    rows, ch = shards[0].shape
    n = len(shards)

    def body(*refs):
        for i in range(n):
            w = refs[i][...]
            for k in range(copies):
                refs[n][k, :, i * ch : (i + 1) * ch] = w

    return pl.pallas_call(
        body, out_shape=sds((copies, rows, n * ch), bf16), in_specs=[VMEM] * n, out_specs=VMEM, compiler_params=params
    )(*fetched(*shards))


def log_rows(logs):
    hi = logs.astype(bf16).astype(f32)
    mid = (logs - hi).astype(bf16).astype(f32)
    lo = logs - hi - mid
    row = lax.broadcasted_iota(jnp.int32, (LOGS, STATE), 0)
    return jnp.where(row == 0, hi, jnp.where(row == 1, mid, jnp.where(row == 2, lo, 0.0))).astype(bf16)


def steps_of(own, step_proj, extra, bias, rate_log, index, p):
    rows = own.shape[0] - HALO
    heads = extra.shape[0]
    ch = heads * p
    every = step_proj.shape[1]

    def body(iz, iy, shard, tp, bref, rref, nref, wref, eref, step, left, cum, cum_t, total, at):
        raw = dot(wref[...], nref[HALO:, :], 0, 1)
        which = lax.broadcasted_iota(jnp.int32, (every, rows), 0)
        size, logs = [], []
        for h in range(heads):
            x = jnp.sum(jnp.where(which == shard[0] * heads + h, raw, 0.0), axis=0, keepdims=True) + bref[h]
            size.append(jnp.maximum(x, 0.0) + jnp.log1p(jnp.exp(-jnp.abs(x))))
            logs.append(-jnp.exp(jnp.full((1, rows), rref[h], f32)) * size[h] + eref[h : h + 1, :])
        none = [jnp.zeros((8 - heads, rows), f32)]
        upto = lax.broadcasted_iota(jnp.int32, (rows, rows), 0) <= lax.broadcasted_iota(jnp.int32, (rows, rows), 1)
        run = dot(jnp.concatenate(logs + none, 0), jnp.where(upto, 1.0, 0.0), 1, 0, HIGHEST)
        lane = lax.broadcasted_iota(jnp.int32, (rows, ch), 1) // p

        def wide(cols):
            out = jnp.broadcast_to(cols[:, 0:1], (rows, ch))
            for h in range(1, heads):
                out = jnp.where(lane == h, cols[:, h : h + 1], out)
            return out

        cum_t[...] = run[:heads]
        cum[...] = wide(jnp.transpose(run))
        left[...] = wide(jnp.transpose(jnp.exp(run[:, rows - 1 :] - run)))
        step[...] = wide(jnp.transpose(jnp.concatenate(size + none, 0)))
        place = lax.broadcasted_iota(jnp.int32, (1, STATE), 1)
        ends = jnp.zeros((1, STATE), f32)
        for h in range(heads):
            ends = jnp.where(place == h, run[h : h + 1, rows - 1 :], ends)
        total[...] = ends
        row = lax.broadcasted_iota(jnp.int32, (8, STATE), 0)
        at[...] = jnp.where(row == 0, iz[0], jnp.where(row == 1, iy[0], tp[0]))

    wide = pltpu.VMEM((rows, ch), f32)
    return pl.pallas_call(
        body,
        out_shape=(
            wide, wide, wide, pltpu.VMEM((heads, rows), f32), pltpu.VMEM((1, STATE), f32),
            pltpu.VMEM((8, STATE), jnp.int32),
        ),
        in_specs=[*[SMEM] * 6, VMEM, VMEM, VMEM],
        out_specs=(VMEM,) * 6,
        compiler_params=SMALL, name="steps_of",
    )(*index, bias, rate_log, *held(own, step_proj, extra))


def local_states(normed, first, taps, step, left, total, copies):
    ext, _ = normed.shape
    rows, ch = step.shape

    def body(nref, wref, tref, sref, lref, logs, send, xs, w16, buf):
        w = jnp.concatenate([wref[:, z].reshape(-1, 2 * ch) for z in range(wref.shape[1])], 0)
        buf[...] = dot(nref[...], w, 1, 0).astype(bf16).astype(f32)
        at = HALO - SHORT + 1
        mix = sum(buf[at + i : at + i + rows, :] * tref[i : i + 1, :] for i in range(SHORT))
        act = jax.nn.silu(mix)
        x = act[:, :ch] * sref[...]
        w = act[:, ch:].astype(bf16)
        xs[...] = x.astype(bf16)
        w16[...] = w
        ends = dot((x * lref[...]).astype(bf16), w, 0, 0).astype(bf16)
        tail = log_rows(logs[...])
        for k in range(copies):
            send[k, :ch, :] = ends
            send[k, ch:, :] = tail

    return pl.pallas_call(
        body,
        out_shape=(sds((copies, ch + LOGS, STATE), bf16), pltpu.VMEM((rows, ch), bf16), pltpu.VMEM((rows, STATE), bf16)),
        in_specs=[VMEM] * 6,
        out_specs=(VMEM,) * 3,
        scratch_shapes=[pltpu.VMEM((ext, 2 * ch), f32)],
        compiler_params=SMALL, name="local_states",
    )(*held(normed, first, taps, step, left, total))


def spread_heads(c, heads, p):
    return jnp.concatenate([jnp.broadcast_to(c[:, h : h + 1], (p, STATE)) for h in range(heads)], 0)


def line_states(got, index, heads, p, copies):
    n, size, _ = got.shape
    ch = heads * p

    def body(at, ref, enter, before, send):
        zero = jnp.zeros((1, STATE), f32)
        acc_in, acc_all = zero, zero
        ent = jnp.zeros((ch, STATE), f32)
        tot = jnp.zeros((ch, STATE), f32)
        for k in reversed(range(n)):
            logs = jnp.sum(ref[k, ch:, :].astype(f32), axis=0, keepdims=True)
            inside = jnp.where(k < at[1:2, :], 1.0, 0.0)
            piece = ref[k, :ch, :].astype(f32)
            ent = ent + piece * spread_heads(inside * jnp.exp(acc_in), heads, p)
            tot = tot + piece * spread_heads(jnp.exp(acc_all), heads, p)
            acc_in = acc_in + inside * logs
            acc_all = acc_all + logs
        enter[...] = ent
        before[...] = jnp.broadcast_to(acc_in, (8, STATE))
        line, tail = tot.astype(bf16), log_rows(acc_all)
        for k in range(copies):
            send[k, :ch, :] = line
            send[k, ch:, :] = tail

    return pl.pallas_call(
        body,
        out_shape=(pltpu.VMEM((ch, STATE), f32), pltpu.VMEM((8, STATE), f32), sds((copies, size, STATE), bf16)),
        in_specs=[VMEM, VMEM],
        out_specs=(VMEM,) * 3,
        compiler_params=SMALL, name="line_states",
    )(*held(index, got))


def rows_local(normed, rest, ftaps, ltaps, xs, w16, cum, cum_t):
    ext, d = normed.shape
    rows, ch = xs.shape
    heads = cum_t.shape[0]
    p = ch // heads
    part, n = 64, 8
    kc = d // n

    def body(nref, wref, ftaps, ltaps, xs, w16, cum, cum_t, read16, zgate, mixed, inner, back, acc, glu, wall, sems):
        def fetch(i):
            at = slice(i * kc, (i + 1) * kc)
            return pltpu.make_async_copy(wref.at[at, : 4 * ch], wall.at[at, :], sems.at[0, i])

        def fetch_back(i):
            at = slice(i * kc, (i + 1) * kc)
            return pltpu.make_async_copy(wref.at[at, 4 * ch :], back.at[at, :], sems.at[1, i])

        for i in range(n):
            fetch(i).start()
        for i in range(n):
            fetch_back(i).start()
        for i in range(n):
            fetch(i).wait()
            at = slice(i * kc, (i + 1) * kc)
            term = dot(nref[:, at], wall[at, :], 1, 0)
            acc[...] = term if i == 0 else acc[...] + term
        glu[...] = acc[:, 2 * ch : 3 * ch].astype(bf16).astype(f32) * jax.nn.sigmoid(
            acc[:, 3 * ch :].astype(bf16).astype(f32)
        )
        acc[:, : 2 * ch] = acc[:, : 2 * ch].astype(bf16).astype(f32)
        s_at, l_at = HALO - SHORT + 1, HALO - WIDE + 1
        read = sum(acc[s_at + i : s_at + i + rows, :ch] * ftaps[i : i + 1, :] for i in range(SHORT))
        read = jax.nn.silu(read).astype(bf16)
        read16[...] = read
        zgate[...] = jax.nn.silu(acc[HALO:, ch : 2 * ch])
        scores = dot(read, w16[...], 1, 1)
        lower = lax.broadcasted_iota(jnp.int32, (rows, rows), 0) >= lax.broadcasted_iota(jnp.int32, (rows, rows), 1)
        lane = lax.broadcasted_iota(jnp.int32, (rows, ch), 1)
        y = jnp.zeros((rows, ch), f32)
        for h in range(heads):
            gap = jnp.where(lower, cum[:, h * p : h * p + 1] - cum_t[h : h + 1, :], 0.0)
            m = jnp.where(lower, jnp.exp(gap) * scores, 0.0).astype(bf16)
            x = jnp.where(lane // p == h, xs[...].astype(f32), 0.0).astype(bf16)
            y = y + dot(m, x, 1, 0)
        inner[...] = y
        for r in range(0, rows, part):
            mixed[r : r + part, :] = sum(
                glu[l_at + r + i : l_at + r + i + part, :] * ltaps[i : i + 1, :] for i in range(WIDE)
            )
        for i in range(n):
            fetch_back(i).wait()

    small = (ftaps, ltaps, xs, w16, cum, cum_t)
    return pl.pallas_call(
        body,
        out_shape=(
            pltpu.VMEM((rows, STATE), bf16), pltpu.VMEM((rows, ch), f32), pltpu.VMEM((rows, ch), f32),
            pltpu.VMEM((rows, ch), f32), pltpu.VMEM((d + 3 * rows // 4, 2 * ch), bf16),
        ),
        in_specs=[VMEM, pl.BlockSpec(memory_space=pltpu.HBM), *[VMEM] * len(small)],
        out_specs=(VMEM,) * 5,
        scratch_shapes=[
            pltpu.VMEM((ext, 4 * ch), f32), pltpu.VMEM((ext, ch), f32), pltpu.VMEM((d, 4 * ch), bf16),
            pltpu.SemaphoreType.DMA((2, n)),
        ],
        compiler_params=SMALL, name="rows_local",
    )(*held(normed), *fetched(rest), *held(*small))


def rows_done(got, enter, before, init, index, read16, zgate, mixed, inner, cum, gain, back, nf, nt):
    rows, ch = mixed.shape
    n, _, _ = got.shape
    heads = init.shape[0]
    p = ch // heads
    half, piece = rows // 2, rows // (nf * nt)
    d = back.shape[0] - 3 * rows // 4

    def body(at, got, enter, before, init, read16, zgate, mixed, inner, cum, gain, _, sums, pack, keep, last):
        acc_in = jnp.zeros((1, STATE), f32)
        start = enter[...]
        b = before[0:1, :]
        for j in reversed(range(n)):
            logs = jnp.sum(got[j, ch:, :].astype(f32), axis=0, keepdims=True)
            inside = jnp.where(j < at[0:1, :], 1.0, 0.0)
            start = start + got[j, :ch, :].astype(f32) * spread_heads(inside * jnp.exp(acc_in + b), heads, p)
            acc_in = acc_in + inside * logs
        start = start + init[...].reshape(ch, STATE) * spread_heads(jnp.exp(acc_in + b), heads, p)
        y = inner[...] + dot(read16[...], start.astype(bf16), 1, 1) * jnp.exp(cum[...])
        gated = y * zgate[...]
        mix = mixed[...]
        cols = [jnp.sum(v, axis=1, keepdims=True) for v in (mix, mix * mix, gated * gated)]
        found = jnp.transpose(jnp.concatenate([*cols, jnp.zeros((rows, 5), f32)], 1))
        for j in range(nf * nt):
            sums[j] = found[:3]
        last[...] = gated * gain[...]
        tp = at[2, 0]

        def values(start):
            rows_at = pl.ds(pl.multiple_of(start, piece), piece)
            high = mixed[rows_at, :].astype(bf16)
            return high, (mixed[rows_at, :] - high.astype(f32)).astype(bf16), last[rows_at, :].astype(bf16)

        for i in range(nf):
            here = slice(i * piece, (i + 1) * piece)
            for k, v in enumerate(values(i * (nt * piece) + tp * piece)):
                keep[here, k * ch : (k + 1) * ch] = v
            high, low, scaled = values(i * (nt * piece) + (1 - tp) * piece)
            pack[d + i * piece : d + (i + 1) * piece, :ch] = high
            pack[d + i * piece : d + (i + 1) * piece, ch:] = low
            right, up = divmod(i * piece, half // 2)
            pack[d + half + up : d + half + up + piece, right * ch : (right + 1) * ch] = scaled

    return pl.pallas_call(
        body,
        out_shape=(sds((nf * nt, 3, rows), f32), pltpu.VMEM(back.shape, bf16), pltpu.VMEM((half, 3 * ch), bf16)),
        in_specs=[VMEM] * 12,
        out_specs=(VMEM,) * 3,
        input_output_aliases={11: 1},
        scratch_shapes=[pltpu.VMEM((rows, ch), f32)],
        compiler_params=SMALL, name="rows_done",
    )(*held(index, got, enter, before, init, read16, zgate, mixed, inner, cum, gain, back))


def output_rows(sums, gains, keep, own, other, index, nf, nt):
    copies, _, rows = sums.shape
    ch = gains.shape[1]
    half = rows // 2
    d = own.shape[0] - 3 * rows // 4
    piece = rows // (nf * nt)

    def body(at, sref, gref, keep, own, other, out, cols, act):
        tp = at[2, 0]
        s = sref[0]
        for j in range(1, copies):
            s = s + sref[j]
        cols[...] = jnp.transpose(jnp.concatenate([s, jnp.zeros((5, rows), f32)], 0))
        for i in range(nf):
            at_row = pl.multiple_of(i * (nt * piece) + tp * piece, piece)
            here = slice(i * piece, (i + 1) * piece)
            t = cols[pl.ds(at_row, piece), :]
            mean = t[:, 0:1] / C_CH
            rstd = lax.rsqrt(t[:, 1:2] / C_CH - mean * mean + EPS)
            scale = lax.rsqrt(t[:, 2:3] / D_INNER + EPS)
            right, up = divmod(i * piece, half // 2)
            mine = [keep[here, k * ch : (k + 1) * ch] for k in range(3)]
            got = other[d + i * piece : d + (i + 1) * piece, :]
            last = other[d + half + up : d + half + up + piece, right * ch : (right + 1) * ch]
            for j, (high, low, gated) in enumerate((mine, (got[:, :ch], got[:, ch:], last))):
                src = tp if j == 0 else 1 - tp
                mix = high.astype(f32) + low.astype(f32)
                conv = jax.nn.silu((mix - mean) * rstd * gref[pl.ds(src, 1), :])
                act[here, 2 * j * ch : (2 * j + 1) * ch] = conv.astype(bf16)
                act[here, (2 * j + 1) * ch : (2 * j + 2) * ch] = (gated.astype(f32) * scale).astype(bf16)
        term = dot(act[:, : 2 * ch], own[:d, :], 1, 1) + dot(act[:, 2 * ch :], other[:d, :], 1, 1)
        out[...] = term.astype(bf16).reshape(nf, piece, d)

    return pl.pallas_call(
        body,
        out_shape=sds((nf, piece, d), bf16),
        in_specs=[VMEM] * 6,
        out_specs=VMEM,
        scratch_shapes=[pltpu.VMEM((rows, 8), f32), pltpu.VMEM((nf * piece, 4 * ch), bf16)],
        compiler_params=SMALL, name="output_rows",
    )(*held(index, sums, gains, keep, own, other))


def per_device(
    tokens, norm_gain, conv_value, conv_gate, mixer_gate, state_input, write_projection, state_read,
    step_proj, step_bias, decay_log, decay_extra, input_taps, write_taps, fetch_taps, long_taps,
    conv_gain, state_gain, conv_output, state_output, initial_state,
):
    rows = tokens.shape[0]
    ch = conv_value.shape[1]
    heads = step_bias.shape[0]
    p = ch // heads
    nf, nt = lax.axis_size("fs"), lax.axis_size("tp")
    iz, iy, ix, tp = (lax.axis_index(a).astype(jnp.int32).reshape(1) for a in ("sp_0", "sp_1", "fs", "tp"))
    ny = lax.axis_size("sp_1")
    rest = lay_out((state_read, mixer_gate, conv_value, conv_gate, conv_output, state_output), ny, SMALL)
    rest = lax.all_to_all(rest, "sp_1", 0, 0, tiled=True).reshape(-1, 6 * ch)
    rest = lax.all_gather(rest, "sp_0", axis=0, tiled=True)
    first = lay_out((state_input, write_projection), lax.axis_size(SP), LARGE)
    first = lax.all_to_all(first, SP[::-1], 0, 0, tiled=True).reshape(ny, -1, *first.shape[1:])
    n = lax.axis_size(SP)
    halo = lax.ppermute(tokens[rows - HALO :], SP, [(i, i + 1) for i in range(n - 1)])
    v = jnp.concatenate([halo, tokens], 0).astype(f32)
    normed = (v * lax.rsqrt(jnp.mean(v * v, axis=1, keepdims=True) + EPS) * norm_gain).astype(bf16)
    step, left, cum, cum_t, total, at = steps_of(
        normed, step_proj, decay_extra, step_bias, decay_log, (iz, iy, ix * nt + tp, tp), p
    )
    gains = lax.all_gather(conv_gain, "tp")
    taps = jnp.concatenate([input_taps, write_taps], 1)
    send, xs, w16 = local_states(normed, first, taps, step, left, total, ny)
    got = lax.all_to_all(send, "sp_1", 0, 0, tiled=True)
    enter, before, send = line_states(got, at, heads, p, lax.axis_size("sp_0"))
    got = lax.all_to_all(send, "sp_0", 0, 0, tiled=True)
    read16, zgate, mixed, inner, back = rows_local(normed, rest, fetch_taps, long_taps, xs, w16, cum, cum_t)
    sums, pack, keep = rows_done(
        got, enter, before, initial_state, at, read16, zgate, mixed, inner, cum, state_gain[None], back, nf, nt
    )
    sums = lax.all_to_all(sums, FT, 0, 0, tiled=True)
    other = lax.ppermute(pack, "tp", [(i, nt - 1 - i) for i in range(nt)])
    out = output_rows(sums, gains, keep, pack, other, at, nf, nt)
    pieces = lax.all_to_all(out, "fs", 0, 0, tiled=True)
    return jnp.sum(pieces.astype(f32), 0).astype(bf16)


def solution(mesh):
    torus = Mesh(
        mesh.devices.reshape(8, 8, mesh.shape["fs"], mesh.shape["tp"]), ("sp_0", "sp_1", "fs", "tp")
    )
    w = P(SP, FT)
    in_specs = (
        P(SP, None), P(), w, w, w, w, w, w, P(), P(FT), P(FT), P(FT, SP), P(None, FT), P(None, FT), P(None, FT),
        P(None, FT), P(FT), P(FT), w, w, P(FT, None, None),
    )

    return jax.shard_map(per_device, mesh=torus, in_specs=in_specs, out_specs=P((*SP, *FT), None), check_vma=False)
```

```python
import jax
import jax.numpy as jnp
from jax import lax
from jax.experimental import pallas as pl
from jax.experimental.pallas import tpu as pltpu
from jax.sharding import Mesh
from jax.sharding import PartitionSpec as P


C_CH = 1024
STATE = 128
D_INNER = 1024
WIDE = 31
SHORT = 4
HALO = 32
EPS = 1e-06
LOGS = 8
SP = ("sp_0", "sp_1")
FT = ("fs", "tp")
f32 = jnp.float32
bf16 = jnp.bfloat16
VMEM = pl.BlockSpec(memory_space=pltpu.VMEM)
SMEM = pl.BlockSpec(memory_space=pltpu.SMEM)
HIGHEST = lax.Precision.HIGHEST
SMALL = pltpu.CompilerParams(vmem_limit_bytes=12 * 2**20)
LARGE = pltpu.CompilerParams(vmem_limit_bytes=64 * 2**20 - 2**17)


def dot(a, b, ca, cb, precision=None):
    return lax.dot_general(a, b, (((ca,), (cb,)), ((), ())), precision=precision, preferred_element_type=f32)


def sds(shape, dtype):
    return jax.ShapeDtypeStruct(shape, dtype)


def held(*arrays):
    return tuple(pltpu.with_memory_space_constraint(a, pltpu.VMEM) for a in arrays)


def fetched(*arrays):
    return tuple(pltpu.with_memory_space_constraint(a, pltpu.HBM) for a in arrays)


def lay_out(shards, copies, params):
    rows, ch = shards[0].shape
    n = len(shards)

    def body(*refs):
        for i in range(n):
            w = refs[i][...]
            for k in range(copies):
                refs[n][k, :, i * ch : (i + 1) * ch] = w

    return pl.pallas_call(
        body, out_shape=sds((copies, rows, n * ch), bf16), in_specs=[VMEM] * n, out_specs=VMEM, compiler_params=params
    )(*fetched(*shards))


def log_rows(logs):
    hi = logs.astype(bf16).astype(f32)
    mid = (logs - hi).astype(bf16).astype(f32)
    lo = logs - hi - mid
    row = lax.broadcasted_iota(jnp.int32, (LOGS, STATE), 0)
    return jnp.where(row == 0, hi, jnp.where(row == 1, mid, jnp.where(row == 2, lo, 0.0))).astype(bf16)


def steps_of(own, step_proj, extra, bias, rate_log, index, p):
    rows = own.shape[0] - HALO
    heads = extra.shape[0]
    ch = heads * p
    every = step_proj.shape[1]

    def body(iz, iy, shard, tp, bref, rref, nref, wref, eref, step, left, cum, cum_t, total, at):
        raw = dot(wref[...], nref[HALO:, :], 0, 1)
        which = lax.broadcasted_iota(jnp.int32, (every, rows), 0)
        size, logs = [], []
        for h in range(heads):
            x = jnp.sum(jnp.where(which == shard[0] * heads + h, raw, 0.0), axis=0, keepdims=True) + bref[h]
            size.append(jnp.maximum(x, 0.0) + jnp.log1p(jnp.exp(-jnp.abs(x))))
            logs.append(-jnp.exp(jnp.full((1, rows), rref[h], f32)) * size[h] + eref[h : h + 1, :])
        none = [jnp.zeros((8 - heads, rows), f32)]
        upto = lax.broadcasted_iota(jnp.int32, (rows, rows), 0) <= lax.broadcasted_iota(jnp.int32, (rows, rows), 1)
        run = dot(jnp.concatenate(logs + none, 0), jnp.where(upto, 1.0, 0.0), 1, 0, HIGHEST)
        lane = lax.broadcasted_iota(jnp.int32, (rows, ch), 1) // p

        def wide(cols):
            out = jnp.broadcast_to(cols[:, 0:1], (rows, ch))
            for h in range(1, heads):
                out = jnp.where(lane == h, cols[:, h : h + 1], out)
            return out

        cum_t[...] = run[:heads]
        cum[...] = wide(jnp.transpose(run))
        left[...] = wide(jnp.transpose(jnp.exp(run[:, rows - 1 :] - run)))
        step[...] = wide(jnp.transpose(jnp.concatenate(size + none, 0)))
        place = lax.broadcasted_iota(jnp.int32, (1, STATE), 1)
        ends = jnp.zeros((1, STATE), f32)
        for h in range(heads):
            ends = jnp.where(place == h, run[h : h + 1, rows - 1 :], ends)
        total[...] = ends
        row = lax.broadcasted_iota(jnp.int32, (8, STATE), 0)
        at[...] = jnp.where(row == 0, iz[0], jnp.where(row == 1, iy[0], tp[0]))

    wide = pltpu.VMEM((rows, ch), f32)
    return pl.pallas_call(
        body,
        out_shape=(
            wide, wide, wide, pltpu.VMEM((heads, rows), f32), pltpu.VMEM((1, STATE), f32),
            pltpu.VMEM((8, STATE), jnp.int32),
        ),
        in_specs=[*[SMEM] * 6, VMEM, VMEM, VMEM],
        out_specs=(VMEM,) * 6,
        compiler_params=SMALL, name="steps_of",
    )(*index, bias, rate_log, *held(own, step_proj, extra))


def local_states(normed, first, taps, step, left, total, copies):
    ext, _ = normed.shape
    rows, ch = step.shape

    def body(nref, wref, tref, sref, lref, logs, send, xs, w16, buf):
        buf[...] = dot(nref[...], wref[...], 1, 0).astype(bf16).astype(f32)
        at = HALO - SHORT + 1
        mix = sum(buf[at + i : at + i + rows, :] * tref[i : i + 1, :] for i in range(SHORT))
        act = jax.nn.silu(mix)
        x = act[:, :ch] * sref[...]
        w = act[:, ch:].astype(bf16)
        xs[...] = x.astype(bf16)
        w16[...] = w
        ends = dot((x * lref[...]).astype(bf16), w, 0, 0).astype(bf16)
        tail = log_rows(logs[...])
        for k in range(copies):
            send[k, :ch, :] = ends
            send[k, ch:, :] = tail

    return pl.pallas_call(
        body,
        out_shape=(sds((copies, ch + LOGS, STATE), bf16), pltpu.VMEM((rows, ch), bf16), pltpu.VMEM((rows, STATE), bf16)),
        in_specs=[VMEM] * 6,
        out_specs=(VMEM,) * 3,
        scratch_shapes=[pltpu.VMEM((ext, 2 * ch), f32)],
        compiler_params=SMALL, name="local_states",
    )(*held(normed, first, taps, step, left, total))


def spread_heads(c, heads, p):
    return jnp.concatenate([jnp.broadcast_to(c[:, h : h + 1], (p, STATE)) for h in range(heads)], 0)


def line_states(got, index, heads, p, copies):
    n, size, _ = got.shape
    ch = heads * p

    def body(at, ref, enter, before, send):
        zero = jnp.zeros((1, STATE), f32)
        acc_in, acc_all = zero, zero
        ent = jnp.zeros((ch, STATE), f32)
        tot = jnp.zeros((ch, STATE), f32)
        for k in reversed(range(n)):
            logs = jnp.sum(ref[k, ch:, :].astype(f32), axis=0, keepdims=True)
            inside = jnp.where(k < at[1:2, :], 1.0, 0.0)
            piece = ref[k, :ch, :].astype(f32)
            ent = ent + piece * spread_heads(inside * jnp.exp(acc_in), heads, p)
            tot = tot + piece * spread_heads(jnp.exp(acc_all), heads, p)
            acc_in = acc_in + inside * logs
            acc_all = acc_all + logs
        enter[...] = ent
        before[...] = jnp.broadcast_to(acc_in, (8, STATE))
        line, tail = tot.astype(bf16), log_rows(acc_all)
        for k in range(copies):
            send[k, :ch, :] = line
            send[k, ch:, :] = tail

    return pl.pallas_call(
        body,
        out_shape=(pltpu.VMEM((ch, STATE), f32), pltpu.VMEM((8, STATE), f32), sds((copies, size, STATE), bf16)),
        in_specs=[VMEM, VMEM],
        out_specs=(VMEM,) * 3,
        compiler_params=SMALL, name="line_states",
    )(*held(index, got))


def rows_local(normed, rest, ftaps, ltaps, xs, w16, cum, cum_t):
    ext, d = normed.shape
    rows, ch = xs.shape
    heads = cum_t.shape[0]
    p = ch // heads
    part, n = 64, 8
    kc = d // n

    def body(nref, wref, ftaps, ltaps, xs, w16, cum, cum_t, read16, zgate, mixed, inner, back, acc, glu, wall, decay, owned, sems):
        def fetch(i):
            at = slice(i * kc, (i + 1) * kc)
            return pltpu.make_async_copy(wref.at[at, : 4 * ch], wall.at[at, :], sems.at[0, i])

        def fetch_back(i):
            at = slice(i * kc, (i + 1) * kc)
            return pltpu.make_async_copy(wref.at[at, 4 * ch :], back.at[at, :], sems.at[1, i])

        for i in range(n):
            fetch(i).start()
        for i in range(n):
            fetch_back(i).start()
        lower = lax.broadcasted_iota(jnp.int32, (rows, rows), 0) >= lax.broadcasted_iota(jnp.int32, (rows, rows), 1)
        lane = lax.broadcasted_iota(jnp.int32, (rows, ch), 1)
        for h in range(heads):
            gap = jnp.where(lower, cum[:, h * p : h * p + 1] - cum_t[h : h + 1, :], 0.0)
            decay[h] = jnp.exp(gap)
            owned[h] = jnp.where(lane // p == h, xs[...].astype(f32), 0.0).astype(bf16)
        for i in range(n):
            fetch(i).wait()
            at = slice(i * kc, (i + 1) * kc)
            term = dot(nref[:, at], wall[at, :], 1, 0)
            acc[...] = term if i == 0 else acc[...] + term
        glu[...] = acc[:, 2 * ch : 3 * ch].astype(bf16).astype(f32) * jax.nn.sigmoid(
            acc[:, 3 * ch :].astype(bf16).astype(f32)
        )
        acc[:, : 2 * ch] = acc[:, : 2 * ch].astype(bf16).astype(f32)
        s_at, l_at = HALO - SHORT + 1, HALO - WIDE + 1
        read = sum(acc[s_at + i : s_at + i + rows, :ch] * ftaps[i : i + 1, :] for i in range(SHORT))
        read = jax.nn.silu(read).astype(bf16)
        read16[...] = read
        zgate[...] = jax.nn.silu(acc[HALO:, ch : 2 * ch])
        scores = dot(read, w16[...], 1, 1)
        y = jnp.zeros((rows, ch), f32)
        for h in range(heads):
            m = jnp.where(lower, decay[h] * scores, 0.0).astype(bf16)
            y = y + dot(m, owned[h], 1, 0)
        inner[...] = y
        for r in range(0, rows, part):
            mixed[r : r + part, :] = sum(
                glu[l_at + r + i : l_at + r + i + part, :] * ltaps[i : i + 1, :] for i in range(WIDE)
            )
        for i in range(n):
            fetch_back(i).wait()

    small = (ftaps, ltaps, xs, w16, cum, cum_t)
    return pl.pallas_call(
        body,
        out_shape=(
            pltpu.VMEM((rows, STATE), bf16), pltpu.VMEM((rows, ch), f32), pltpu.VMEM((rows, ch), f32),
            pltpu.VMEM((rows, ch), f32), pltpu.VMEM((d + 3 * rows // 4, 2 * ch), bf16),
        ),
        in_specs=[VMEM, pl.BlockSpec(memory_space=pltpu.HBM), *[VMEM] * len(small)],
        out_specs=(VMEM,) * 5,
        scratch_shapes=[
            pltpu.VMEM((ext, 4 * ch), f32), pltpu.VMEM((ext, ch), f32), pltpu.VMEM((d, 4 * ch), bf16),
            pltpu.VMEM((heads, rows, rows), f32), pltpu.VMEM((heads, rows, ch), bf16), pltpu.SemaphoreType.DMA((2, n)),
        ],
        compiler_params=SMALL, name="rows_local",
    )(*held(normed), *fetched(rest), *held(*small))


def rows_done(got, enter, before, init, index, read16, zgate, mixed, inner, cum, gain, back, nf, nt):
    rows, ch = mixed.shape
    n, _, _ = got.shape
    heads = init.shape[0]
    p = ch // heads
    half, piece = rows // 2, rows // (nf * nt)
    d = back.shape[0] - 3 * rows // 4

    def body(at, got, enter, before, init, read16, zgate, mixed, inner, cum, gain, _, sums, pack, keep, last):
        acc_in = jnp.zeros((1, STATE), f32)
        start = enter[...]
        b = before[0:1, :]
        for j in reversed(range(n)):
            logs = jnp.sum(got[j, ch:, :].astype(f32), axis=0, keepdims=True)
            inside = jnp.where(j < at[0:1, :], 1.0, 0.0)
            start = start + got[j, :ch, :].astype(f32) * spread_heads(inside * jnp.exp(acc_in + b), heads, p)
            acc_in = acc_in + inside * logs
        start = start + init[...].reshape(ch, STATE) * spread_heads(jnp.exp(acc_in + b), heads, p)
        y = inner[...] + dot(read16[...], start.astype(bf16), 1, 1) * jnp.exp(cum[...])
        gated = y * zgate[...]
        mix = mixed[...]
        cols = [jnp.sum(v, axis=1, keepdims=True) for v in (mix, mix * mix, gated * gated)]
        found = jnp.transpose(jnp.concatenate([*cols, jnp.zeros((rows, 5), f32)], 1))
        for j in range(nf * nt):
            sums[j] = found[:3]
        last[...] = gated * gain[...]
        tp = at[2, 0]

        def values(start):
            rows_at = pl.ds(pl.multiple_of(start, piece), piece)
            high = mixed[rows_at, :].astype(bf16)
            return high, (mixed[rows_at, :] - high.astype(f32)).astype(bf16), last[rows_at, :].astype(bf16)

        for i in range(nf):
            here = slice(i * piece, (i + 1) * piece)
            for k, v in enumerate(values(i * (nt * piece) + tp * piece)):
                keep[here, k * ch : (k + 1) * ch] = v
            high, low, scaled = values(i * (nt * piece) + (1 - tp) * piece)
            pack[d + i * piece : d + (i + 1) * piece, :ch] = high
            pack[d + i * piece : d + (i + 1) * piece, ch:] = low
            right, up = divmod(i * piece, half // 2)
            pack[d + half + up : d + half + up + piece, right * ch : (right + 1) * ch] = scaled

    return pl.pallas_call(
        body,
        out_shape=(sds((nf * nt, 3, rows), f32), pltpu.VMEM(back.shape, bf16), pltpu.VMEM((half, 3 * ch), bf16)),
        in_specs=[VMEM] * 12,
        out_specs=(VMEM,) * 3,
        input_output_aliases={11: 1},
        scratch_shapes=[pltpu.VMEM((rows, ch), f32)],
        compiler_params=SMALL, name="rows_done",
    )(*held(index, got, enter, before, init, read16, zgate, mixed, inner, cum, gain, back))


def output_rows(sums, gains, keep, own, other, index, nf, nt):
    copies, _, rows = sums.shape
    ch = gains.shape[1]
    half = rows // 2
    d = own.shape[0] - 3 * rows // 4
    piece = rows // (nf * nt)

    def body(at, sref, gref, keep, own, other, out, cols, act):
        tp = at[2, 0]
        s = sref[0]
        for j in range(1, copies):
            s = s + sref[j]
        cols[...] = jnp.transpose(jnp.concatenate([s, jnp.zeros((5, rows), f32)], 0))
        for i in range(nf):
            at_row = pl.multiple_of(i * (nt * piece) + tp * piece, piece)
            here = slice(i * piece, (i + 1) * piece)
            t = cols[pl.ds(at_row, piece), :]
            mean = t[:, 0:1] / C_CH
            rstd = lax.rsqrt(t[:, 1:2] / C_CH - mean * mean + EPS)
            scale = lax.rsqrt(t[:, 2:3] / D_INNER + EPS)
            right, up = divmod(i * piece, half // 2)
            mine = [keep[here, k * ch : (k + 1) * ch] for k in range(3)]
            got = other[d + i * piece : d + (i + 1) * piece, :]
            last = other[d + half + up : d + half + up + piece, right * ch : (right + 1) * ch]
            for j, (high, low, gated) in enumerate((mine, (got[:, :ch], got[:, ch:], last))):
                src = tp if j == 0 else 1 - tp
                mix = high.astype(f32) + low.astype(f32)
                conv = jax.nn.silu((mix - mean) * rstd * gref[pl.ds(src, 1), :])
                act[here, 2 * j * ch : (2 * j + 1) * ch] = conv.astype(bf16)
                act[here, (2 * j + 1) * ch : (2 * j + 2) * ch] = (gated.astype(f32) * scale).astype(bf16)
        term = dot(act[:, : 2 * ch], own[:d, :], 1, 1) + dot(act[:, 2 * ch :], other[:d, :], 1, 1)
        out[...] = term.astype(bf16).reshape(nf, piece, d)

    return pl.pallas_call(
        body,
        out_shape=sds((nf, piece, d), bf16),
        in_specs=[VMEM] * 6,
        out_specs=VMEM,
        scratch_shapes=[pltpu.VMEM((rows, 8), f32), pltpu.VMEM((nf * piece, 4 * ch), bf16)],
        compiler_params=SMALL, name="output_rows",
    )(*held(index, sums, gains, keep, own, other))


def per_device(
    tokens, norm_gain, conv_value, conv_gate, mixer_gate, state_input, write_projection, state_read,
    step_proj, step_bias, decay_log, decay_extra, input_taps, write_taps, fetch_taps, long_taps,
    conv_gain, state_gain, conv_output, state_output, initial_state,
):
    rows = tokens.shape[0]
    ch = conv_value.shape[1]
    heads = step_bias.shape[0]
    p = ch // heads
    nf, nt = lax.axis_size("fs"), lax.axis_size("tp")
    iz, iy, ix, tp = (lax.axis_index(a).astype(jnp.int32).reshape(1) for a in ("sp_0", "sp_1", "fs", "tp"))
    ny = lax.axis_size("sp_1")
    rest = lay_out((state_read, mixer_gate, conv_value, conv_gate, conv_output, state_output), ny, SMALL)
    rest = lax.all_to_all(rest, "sp_1", 0, 0, tiled=True).reshape(-1, 6 * ch)
    rest = lax.all_gather(rest, "sp_0", axis=0, tiled=True)
    first = lay_out((state_input, write_projection), lax.axis_size(SP), LARGE)
    first = lax.all_to_all(first, SP, 0, 0, tiled=True).reshape(-1, 2 * ch)
    n = lax.axis_size(SP)
    halo = lax.ppermute(tokens[rows - HALO :], SP, [(i, i + 1) for i in range(n - 1)])
    v = jnp.concatenate([halo, tokens], 0).astype(f32)
    normed = (v * lax.rsqrt(jnp.mean(v * v, axis=1, keepdims=True) + EPS) * norm_gain).astype(bf16)
    step, left, cum, cum_t, total, at = steps_of(
        normed, step_proj, decay_extra, step_bias, decay_log, (iz, iy, ix * nt + tp, tp), p
    )
    gains = lax.all_gather(conv_gain, "tp")
    taps = jnp.concatenate([input_taps, write_taps], 1)
    send, xs, w16 = local_states(normed, first, taps, step, left, total, ny)
    got = lax.all_to_all(send, "sp_1", 0, 0, tiled=True)
    enter, before, send = line_states(got, at, heads, p, lax.axis_size("sp_0"))
    got = lax.all_to_all(send, "sp_0", 0, 0, tiled=True)
    read16, zgate, mixed, inner, back = rows_local(normed, rest, fetch_taps, long_taps, xs, w16, cum, cum_t)
    sums, pack, keep = rows_done(
        got, enter, before, initial_state, at, read16, zgate, mixed, inner, cum, state_gain[None], back, nf, nt
    )
    sums = lax.all_to_all(sums, FT, 0, 0, tiled=True)
    other = lax.ppermute(pack, "tp", [(i, nt - 1 - i) for i in range(nt)])
    out = output_rows(sums, gains, keep, pack, other, at, nf, nt)
    pieces = lax.all_to_all(out, "fs", 0, 0, tiled=True)
    return jnp.sum(pieces.astype(f32), 0).astype(bf16)


def solution(mesh):
    torus = Mesh(
        mesh.devices.reshape(8, 8, mesh.shape["fs"], mesh.shape["tp"]), ("sp_0", "sp_1", "fs", "tp")
    )
    w = P(SP, FT)
    in_specs = (
        P(SP, None), P(), w, w, w, w, w, w, P(), P(FT), P(FT), P(FT, SP), P(None, FT), P(None, FT), P(None, FT),
        P(None, FT), P(FT), P(FT), w, w, P(FT, None, None),
    )

    return jax.shard_map(per_device, mesh=torus, in_specs=in_specs, out_specs=P((*SP, *FT), None), check_vma=False)
```
